128 devices in a mesh: rep: 2 (over x_hi), fs: 16 (over y, x_lo, core), tp: 4 (over z).
Axes of the slice: x: 4 (x_hi: 2, x_lo: 2; x = x_hi * 2 + x_lo), y: 4, z: 4, core: 2. Of those that a mesh axis runs over, the one named last changes fastest.
Arguments:
- tokens: bfloat16 [16384, 2048], P(('rep', 'fs', 'tp')), may hold values from -3 to 3
- mixer_output: bfloat16 [16384, 2048], P(('rep', 'fs', 'tp')), may hold values from -6 to 6
- early_norm: float32 [2048], replicated, may hold values from 0.75 to 1.25
- early_gate: bfloat16 [2048, 5120], P('fs', 'tp'), may hold values from -0.125 to 0.125
- early_value: bfloat16 [2048, 5120], P('fs', 'tp'), may hold values from -0.125 to 0.125
- early_down: bfloat16 [5120, 2048], P('tp', 'fs'), may hold values from -0.078125 to 0.078125
- early_post: float32 [2048], replicated, may hold values from 0.75 to 1.25
- mixer_gain: float32 [2048], replicated, may hold values from 0.75 to 1.25
- later_norm: float32 [2048], replicated, may hold values from 0.75 to 1.25
- later_gate: bfloat16 [2048, 5120], P('fs', 'tp'), may hold values from -0.125 to 0.125
- later_value: bfloat16 [2048, 5120], P('fs', 'tp'), may hold values from -0.125 to 0.125
- later_down: bfloat16 [5120, 2048], P('tp', 'fs'), may hold values from -0.078125 to 0.078125
- later_post: float32 [2048], replicated, may hold values from 0.75 to 1.25
Outputs:
- layer_out: bfloat16 [16384, 2048], P(('rep', 'fs', 'tp'))
The draws below stay inside these ranges and needn't reach their ends.
All inputs are finite; a program needn't handle non-finite values.
Results may differ from the reference program's by a relative error of at most 0.015.
Values may be sent and summed in bfloat16 or wider, within the bound.
A program may use at most 128 MiB of HBM per device.

```python
import jax
import jax.numpy as jnp
from jax import lax

D = 2048
FF = 5120
TOKENS = 16384


def steps_of(rng, extent, split, low, top_value):
    def one(position, parts):
        draws = jax.random.uniform(jax.random.fold_in(jax.random.fold_in(rng, 6), position), (parts,), jnp.float32, low / len(split), top_value / len(split))
        return jnp.repeat(jnp.exp(draws), extent[position] // parts).reshape((-1,) + (1,) * (len(extent) - position - 1))

    loudness = one(*split[0])
    for cut in split[1:]:
        loudness = loudness * one(*cut)
    return loudness


def scatter_about(stream_key, dims, scale, bound, cuts=(), dtype=jnp.bfloat16):
    array = jax.random.normal(stream_key, dims, jnp.float32) * scale
    if len(cuts) > 0:
        array = steps_of(stream_key, dims, cuts, -0.22, 0.18) * array
    return jnp.clip(array, min=-bound, max=bound).astype(dtype)


def setup_inputs(seed: int = 0) -> dict:
    keys = jax.random.split(jax.random.key(seed), 14)
    return {
        "tokens": scatter_about(keys[0], (TOKENS, D), 0.5, 3.0, ((0, 128),)),
        "mixer_output": scatter_about(keys[1], (TOKENS, D), 1.0, 6.0, ((0, 128),)),
        "early_norm": jnp.clip(1.0 + 0.05 * jax.random.normal(keys[2], (D,), jnp.float32), 0.75, 1.25),
        "early_gate": scatter_about(keys[3], (D, FF), D ** -0.5, 0.125, ((0, 16), (1, 4))),
        "early_value": scatter_about(keys[4], (D, FF), D ** -0.5, 0.125, ((0, 16), (1, 4))),
        "early_down": scatter_about(keys[5], (FF, D), FF ** -0.5, 0.078125, ((0, 4), (1, 16))),
        "early_post": jnp.clip(1.0 + 0.05 * jax.random.normal(keys[6], (D,), jnp.float32), 0.75, 1.25),
        "mixer_gain": jnp.clip(1.0 + 0.05 * jax.random.normal(keys[7], (D,), jnp.float32), 0.75, 1.25),
        "later_norm": jnp.clip(1.0 + 0.05 * jax.random.normal(keys[8], (D,), jnp.float32), 0.75, 1.25),
        "later_gate": scatter_about(keys[9], (D, FF), D ** -0.5, 0.125, ((0, 16), (1, 4))),
        "later_value": scatter_about(keys[10], (D, FF), D ** -0.5, 0.125, ((0, 16), (1, 4))),
        "later_down": scatter_about(keys[11], (FF, D), FF ** -0.5, 0.078125, ((0, 4), (1, 16))),
        "later_post": jnp.clip(1.0 + 0.05 * jax.random.normal(keys[12], (D,), jnp.float32), 0.75, 1.25),
    }


epsilon = 1e-06

def rms_scale(values, gain):
    values = values.astype(jnp.float32)
    scale = lax.rsqrt(lax.optimization_barrier(jnp.mean(values * values, axis=-1, keepdims=True)) + epsilon)
    return values * scale * gain

def half_branch(normed, w_gate, w_value, w_down):
    gate_sum = jnp.dot(normed, w_gate, preferred_element_type=jnp.float32)
    value_sum = jnp.dot(normed, w_value, preferred_element_type=jnp.float32)
    hidden = (jax.nn.silu(gate_sum) * value_sum).astype(jnp.bfloat16)
    return jnp.dot(hidden, w_down, preferred_element_type=jnp.float32)

def reference(tokens, mixer_output, early_norm, early_gate, early_value, early_down, early_post, mixer_gain, later_norm, later_gate, later_value, later_down, later_post):
    early_in = rms_scale(tokens, early_norm).astype(jnp.bfloat16)
    early_branch = half_branch(early_in, early_gate, early_value, early_down)
    mixed = tokens.astype(jnp.float32) + 0.5 * rms_scale(early_branch, early_post) + rms_scale(mixer_output, mixer_gain)
    mixed = mixed.astype(jnp.bfloat16)
    later_in = rms_scale(mixed, later_norm).astype(jnp.bfloat16)
    later_branch = half_branch(later_in, later_gate, later_value, later_down)
    layer_out = mixed.astype(jnp.float32) + 0.5 * rms_scale(later_branch, later_post)
    return layer_out.astype(jnp.bfloat16)
```

```python
import functools

import jax
import jax.numpy as jnp
from jax import lax
from jax.experimental import pallas as pl
from jax.experimental.pallas import tpu as pltpu
from jax.sharding import PartitionSpec as P

MESH = pl.DeviceIdType.MESH
EPS = 1e-06
BF = jnp.bfloat16
F32 = jnp.float32


def kernel(
    tok, mix, en, eg, ev, ed, ep, mg, ln, lg, lv, ld, lp,
    out,
    gbuf, vbuf, dbuf, xbuf, acc, hbuf, tokv, mixv, mixed, gains,
    rs1, rr1, rs2, rr2, keep, br, pbuf,
    loc_sem, w_send, w_recv, p_send, p_recv, ag_send, ag_recv, rs_send, rs_recv,
):
    rep = lax.axis_index("rep")
    fs = lax.axis_index("fs")
    z = lax.axis_index("tp")
    c = lax.rem(fs, 2)
    xl = lax.rem(fs // 2, 2)
    y = fs // 4
    x = rep * 2 + xl

    def mod4(v):
        return lax.rem(v + 8, 4)

    def dev(dx=0, dy=0, dz=0, dc=0):
        nx = mod4(x + dx)
        ny = mod4(y + dy)
        nc = c if dc == 0 else 1 - c
        return (nx // 2, (ny * 2 + lax.rem(nx, 2)) * 2 + nc, mod4(z + dz))

    y_dev = {1: dev(dy=1), -1: dev(dy=-1)}
    x_dev = {1: dev(dx=1), -1: dev(dx=-1)}
    z_dev = {1: dev(dz=1), -1: dev(dz=-1)}
    partner = dev(dc=1)
    everyone = [y_dev[1], y_dev[-1], x_dev[1], x_dev[-1], z_dev[1], z_dev[-1], partner]
    zp, zm, zo = mod4(z + 1), mod4(z - 1), mod4(z + 2)

    def blk_of(dy, dp):
        return mod4(y + dy) * 2 + (xl if dp == 0 else 1 - xl)

    blocks = {(dy, dp): blk_of(dy, dp) for dy in (0, 1, -1, 2) for dp in (0, 1)}

    def unit(r, content, core):
        dy, dp, st, s = content
        blk = blocks[(dy, dp)]
        layer = r // 2
        if r % 2 == 0:
            buf = gbuf if st == 0 else vbuf
            row = pl.multiple_of(blk * 256 + core * 128 + s * 64, 64)
            return buf.at[layer, pl.ds(row, 64), :]
        return dbuf.at[layer, blk, core, pl.ds(st * 640 + s * 320, 320), :]

    def unit_id(content):
        dy, dp, st, s = content
        return (((dy % 4) * 2 + dp) * 2 + st) * 2 + s

    sent = []

    def send(src, dst, send_sem, recv_sem, target):
        copy = pltpu.make_async_remote_copy(src, dst, send_sem, recv_sem, device_id=target, device_id_type=MESH)
        copy.start()
        sent.append(copy)

    def await_copy(dst, send_sem, recv_sem, source):
        pltpu.make_async_remote_copy(dst, dst, send_sem, recv_sem, device_id=source, device_id_type=MESH).wait_recv()

    def tee(sign):
        return 0 if sign > 0 else 1

    def y_recv_content(sign, k):
        t = tee(sign)
        return [(-sign, 0, t, 0), (-sign, 0, t, 1), (2, 0, t, 0), (2, 0, t, 1),
                (-sign, 0, 1 - t, 0), (-sign, 0, 1 - t, 1), (-sign, 1, t, 1)][k]

    def y_send_content(sign, k):
        t = tee(sign)
        return [(0, 0, t, 0), (0, 0, t, 1), (-sign, 0, t, 0), (-sign, 0, t, 1),
                (0, 0, 1 - t, 0), (0, 0, 1 - t, 1), (0, 1, t, 1)][k]

    def x_content(sign, k, dp):
        t = tee(sign)
        return [(0, dp, t, 0), (0, dp, t, 1), (-sign, dp, t, 0), (2, dp, t, 0), (2, dp, t, 1),
                (sign, dp, t, 0), (sign, dp, t, 1)][k]

    have = set()
    partner_have = set()

    def send_y(r, sign, k):
        content = y_send_content(sign, k)
        assert (r, content) in have
        ref = unit(r, content, c)
        send(ref, ref, w_send.at[r, tee(sign), k], w_recv.at[r, tee(sign), k], y_dev[sign])

    def send_x(r, sign, k):
        content = x_content(sign, k, 0)
        assert (r, content) in have
        ref = unit(r, content, c)
        send(ref, ref, w_send.at[r, 2 + tee(sign), k], w_recv.at[r, 2 + tee(sign), k], x_dev[sign])

    def send_partner(r, content):
        ref = unit(r, content, c)
        i = unit_id(content)
        send(ref, ref, p_send.at[r, i], p_recv.at[r, i], partner)

    def need(r, content):
        assert (r, content) in have, (r, content)
        if (r, content) not in partner_have:
            partner_have.add((r, content))
            i = unit_id(content)
            await_copy(unit(r, content, 1 - c), p_send.at[r, i], p_recv.at[r, i], partner)

    def own_y(r):
        wait_local(r)
        for sign in (1, -1):
            send_y(r, sign, 0)
            send_y(r, sign, 1)

    def own_x(r):
        for sign in (1, -1):
            send_x(r, sign, 0)
            send_x(r, sign, 1)

    def own_partner(r):
        for st in (0, 1):
            for s in (0, 1):
                send_partner(r, (0, 0, st, s))

    def y_event(r, j):
        for sign in (1, -1):
            content = y_recv_content(sign, j)
            await_copy(unit(r, content, c), w_send.at[r, tee(sign), j], w_recv.at[r, tee(sign), j], y_dev[-sign])
            have.add((r, content))
            if j == 0:
                send_x(r, sign, 2)
                send_y(r, sign, 2)
            elif j == 1:
                send_y(r, sign, 3)
                send_y(r, sign, 4)
                send_y(r, sign, 5)
            elif j == 2:
                send_x(r, sign, 3)
            elif j == 3:
                send_x(r, sign, 4)
            elif j == 4:
                send_x(r, -sign, 5)
            elif j == 5:
                send_x(r, -sign, 6)
        if r < 3 and j == 3:
            own_y(r + 1)
        if r < 3 and j == 5:
            own_x(r + 1)
        for sign in (1, -1):
            send_partner(r, y_recv_content(sign, j))
        if r < 3 and j == 3:
            own_partner(r + 1)

    def x_event(r, j):
        for sign in (1, -1):
            content = x_content(sign, j, 1)
            lane = 2 + tee(sign)
            await_copy(unit(r, content, c), w_send.at[r, lane, j], w_recv.at[r, lane, j], x_dev[-sign])
            have.add((r, content))
            if j == 1:
                send_y(r, sign, 6)
            send_partner(r, content)

    own = pl.multiple_of(blocks[(0, 0)] * 256 + c * 128, 128)
    weights = {
        0: [(eg, gbuf.at[0, pl.ds(own, 128), :]), (ev, vbuf.at[0, pl.ds(own, 128), :])],
        1: [(ed, dbuf.at[0, blocks[(0, 0)], c])],
        2: [(lg, gbuf.at[1, pl.ds(own, 128), :]), (lv, vbuf.at[1, pl.ds(own, 128), :])],
        3: [(ld, dbuf.at[1, blocks[(0, 0)], c])],
    }
    local = {}
    count = 0
    small = [(tok, tokv)] + [(g, gains.at[i]) for i, g in enumerate((en, ep, mg, ln, lp))] + [(mix, mixv)]
    for name, pairs in [(0, weights[0]), ("small", small), (1, weights[1]), (2, weights[2]), (3, weights[3])]:
        local[name] = []
        for src, dst in pairs:
            copy = pltpu.make_async_copy(src, dst, loc_sem.at[count])
            copy.start()
            local[name].append(copy)
            count += 1

    def wait_local(name):
        for copy in local[name]:
            copy.wait()
        if name != "small":
            for st in (0, 1):
                for s in (0, 1):
                    have.add((name, (0, 0, st, s)))

    barrier = pltpu.get_barrier_semaphore()
    for other in everyone:
        pl.semaphore_signal(barrier, inc=1, device_id=other, device_id_type=MESH)
    pl.semaphore_wait(barrier, len(everyone))

    def x_rows(layer, h, zz, u, n=16):
        row = pl.multiple_of(h * 256 + zz * 64 + u * 16, 16)
        return xbuf.at[layer, pl.ds(row, n), :]

    def ag_send_own(layer, h):
        for u in range(4):
            for sign in (1, -1):
                v = u if sign > 0 else (u + 2) % 4
                ref = x_rows(layer, h, z, v)
                send(ref, ref, ag_send.at[layer, h, tee(sign), v], ag_recv.at[layer, h, tee(sign), v], z_dev[sign])

    def ag_wait_own(layer, h, sign, u):
        zz = zm if sign > 0 else zp
        await_copy(x_rows(layer, h, zz, u), ag_send.at[layer, h, tee(sign), u], ag_recv.at[layer, h, tee(sign), u], z_dev[-sign])

    def ag_forward(layer, h, u):
        for sign in (1, -1):
            v = u if sign > 0 else u + 2
            ag_wait_own(layer, h, sign, v)
            zz = zm if sign > 0 else zp
            ref = x_rows(layer, h, zz, v)
            i = 4 + u
            send(ref, ref, ag_send.at[layer, h, tee(sign), i], ag_recv.at[layer, h, tee(sign), i], z_dev[sign])

    def ag_finish(layer, h):
        for sign in (1, -1):
            for u in (0, 1):
                v = u + 2 if sign > 0 else u
                ag_wait_own(layer, h, sign, v)
        for sign in (1, -1):
            for u in (0, 1):
                v = u if sign > 0 else u + 2
                i = 4 + u
                await_copy(x_rows(layer, h, zo, v), ag_send.at[layer, h, tee(sign), i], ag_recv.at[layer, h, tee(sign), i], z_dev[-sign])

    def rms(v, gain):
        return v * lax.rsqrt(jnp.mean(v * v, axis=-1, keepdims=True) + EPS) * gain

    def early_norm(h):
        def body(i, carry):
            rows = pl.ds(pl.multiple_of(h * 64 + i * 16, 16), 16)
            v = rms(tokv[rows, :].astype(F32), gains[0])
            x_rows(0, h, z, i)[...] = v.astype(BF)
            return carry

        lax.fori_loop(0, 4, body, 0)

    started = set()

    def gemm(st, dy, dp):
        for s in (0, 1):
            need(0, (dy, dp, st, s))
        first = st not in started
        started.add(st)
        base = pl.multiple_of(blocks[(dy, dp)] * 256, 256)
        w = gbuf if st == 0 else vbuf

        def body(n, carry):
            cols = pl.ds(pl.multiple_of(n * 256, 256), 256)
            part = jnp.dot(xbuf[0, :, pl.ds(base, 256)], w[0, pl.ds(base, 256), cols], preferred_element_type=F32)
            if first:
                acc[st, :, cols] = part
            else:
                acc[st, :, cols] += part
            return carry

        lax.fori_loop(0, 5, body, 0)

    def silu_mul(g, v):
        return (g * (1.0 / (1.0 + jnp.exp(-g))) * v).astype(BF)

    def hidden_early(h):
        def body(i, carry):
            rows = pl.ds(pl.multiple_of(h * 256 + i * 16, 16), 16)
            hbuf[rows, :] = silu_mul(acc[0, rows, :], acc[1, rows, :])
            return carry

        lax.fori_loop(0, 16, body, 0)

    def hidden_later(h, n):
        if (h, n) == (0, 0):
            for dy in (0, 1, -1, 2):
                for dp in (0, 1):
                    for st in (0, 1):
                        for s in (0, 1):
                            need(2, (dy, dp, st, s))
        rows = slice(h * 256, h * 256 + 256)
        cols = slice(n * 256, n * 256 + 256)
        xs = xbuf[1, rows, :]
        g = jnp.dot(xs, gbuf[1, :, cols], preferred_element_type=F32)
        v = jnp.dot(xs, vbuf[1, :, cols], preferred_element_type=F32)
        hbuf[rows, cols] = silu_mul(g, v)

    order = (0, 2, -1, 1)

    def rs_refs(kind, layer, h, j, lane):
        return kind.at[layer, h, j, lane]

    def down(layer, h, dy):
        r = 2 * layer + 1
        for dp in (0, 1):
            for st in (0, 1):
                for s in (0, 1):
                    need(r, (dy, dp, st, s))
        j = order.index(dy)
        yy = mod4(y + dy)

        def body(e, carry):
            w = jnp.concatenate([dbuf[layer, yy * 2 + e, 0], dbuf[layer, yy * 2 + e, 1]], axis=1)
            pbuf[:, pl.ds(pl.multiple_of(e * 256, 256), 256)] = jnp.dot(
                hbuf[h * 256 : h * 256 + 256, :], w, preferred_element_type=F32
            )
            return carry

        lax.fori_loop(0, 2, body, 0)

        def rows(zz, half):
            return pl.ds(pl.multiple_of(zz * 64 + half * 32, 32), 32)

        rs1[layer, h, j, 0, 0:32, :] = pbuf[rows(zo, 0), :].astype(BF)
        rs1[layer, h, j, 0, 32:64, :] = pbuf[rows(zp, 1), :].astype(BF)
        rs1[layer, h, j, 1, 0:32, :] = pbuf[rows(zm, 0), :].astype(BF)
        rs1[layer, h, j, 1, 32:64, :] = pbuf[rows(zo, 1), :].astype(BF)
        keep[h, j, 0] = pbuf[rows(zp, 0), :]
        keep[h, j, 1] = pbuf[rows(zm, 1), :]
        cols = pl.ds(pl.multiple_of(yy * 512, 512), 512)
        br[h * 64 : h * 64 + 64, cols] = pbuf[pl.ds(pl.multiple_of(z * 64, 64), 64), :]
        for sign in (1, -1):
            lane = tee(sign)
            send(rs1.at[layer, h, j, lane], rr1.at[layer, h, j, lane],
                 rs_send.at[layer, h, j, lane], rs_recv.at[layer, h, j, lane], z_dev[sign])

    def combine(layer, h, dy):
        j = order.index(dy)
        for sign in (1, -1):
            lane = tee(sign)
            await_copy(rr1.at[layer, h, j, lane], rs_send.at[layer, h, j, lane], rs_recv.at[layer, h, j, lane], z_dev[-sign])
            half = slice(0, 32) if sign > 0 else slice(32, 64)
            rs2[layer, h, j, lane] = (rr1[layer, h, j, lane, half, :].astype(F32) + keep[h, j, lane]).astype(BF)
            send(rs2.at[layer, h, j, lane], rr2.at[layer, h, j, lane],
                 rs_send.at[layer, h, j, 2 + lane], rs_recv.at[layer, h, j, 2 + lane], z_dev[sign])

    def own_sum(layer, h, dy):
        j = order.index(dy)
        for sign in (1, -1):
            lane = tee(sign)
            await_copy(rr2.at[layer, h, j, lane], rs_send.at[layer, h, j, 2 + lane], rs_recv.at[layer, h, j, 2 + lane], z_dev[-sign])
        cols = pl.ds(pl.multiple_of(mod4(y + dy) * 512, 512), 512)
        a = slice(h * 64, h * 64 + 32)
        b = slice(h * 64 + 32, h * 64 + 64)
        br[a, cols] += rr2[layer, h, j, 0].astype(F32) + rr1[layer, h, j, 1, 0:32, :].astype(F32)
        br[b, cols] += rr2[layer, h, j, 1].astype(F32) + rr1[layer, h, j, 0, 32:64, :].astype(F32)

    def finish(layer, h):
        for dy in order:
            own_sum(layer, h, dy)

        def body(i, carry):
            rows = pl.ds(pl.multiple_of(h * 64 + i * 16, 16), 16)
            branch = br[rows, :]
            if layer == 0:
                m = tokv[rows, :].astype(F32) + 0.5 * rms(branch, gains[1]) + rms(mixv[rows, :].astype(F32), gains[2])
                m = m.astype(BF)
                mixed[rows, :] = m
                x_rows(1, h, z, i)[...] = rms(m.astype(F32), gains[3]).astype(BF)
            else:
                out[rows, :] = (mixed[rows, :].astype(F32) + 0.5 * rms(branch, gains[4])).astype(BF)
            return carry

        lax.fori_loop(0, 4, body, 0)
        if layer == 0:
            ag_send_own(1, h)

    own_start = True
    wait_local(0)
    for sign in (1, -1):
        send_y(0, sign, 0)
        send_x(0, sign, 0)
        send_y(0, sign, 1)
        send_x(0, sign, 1)
    own_partner(0)
    wait_local("small")
    for h in (0, 1):
        early_norm(h)
        ag_send_own(0, h)

    events = []

    def at(time, fn, *args):
        events.append((time, len(events), fn, args))

    starts = (0.0, 24.6, 36.9, 61.5)
    steps = (3.5, 1.76, 3.5, 1.76)
    for r in range(4):
        for j in range(7):
            at(2.5 + starts[r] + steps[r] * (j + 1), y_event, r, j)
            at(4.5 + starts[r] + steps[r] * (j + 1), x_event, r, j)
    at(6.1, ag_forward, 0, 0, 0)
    at(6.1, ag_forward, 0, 0, 1)
    at(11.5, ag_forward, 0, 1, 0)
    at(11.5, ag_forward, 0, 1, 1)
    at(18.9, ag_finish, 0, 0)
    at(18.9, ag_finish, 0, 1)
    for time, tasks in (
        (19.0, ((0, 0, 0), (1, 0, 0), (0, 0, 1), (1, 0, 1))),
        (20.5, ((0, -1, 0), (1, 1, 0), (0, 2, 0), (1, 2, 0))),
        (22.3, ((0, 2, 1), (1, 2, 1))),
        (24.0, ((0, 1, 0), (1, -1, 0))),
        (27.2, ((0, -1, 1), (1, 1, 1))),
        (29.2, ((0, 1, 1), (1, -1, 1))),
    ):
        for task in tasks:
            at(time, gemm, *task)
    at(30.0, hidden_early, 0)
    at(31.5, hidden_early, 1)
    for time, fn, h, dy in (
        (32.7, down, 0, 0), (33.5, down, 1, 0), (36.5, combine, 0, 0), (37.5, combine, 1, 0),
        (38.0, down, 0, 2), (38.8, down, 1, 2), (41.5, down, 0, -1), (42.0, down, 0, 1), (42.5, combine, 0, 2),
        (43.0, down, 1, -1), (43.2, combine, 1, 2), (45.0, combine, 0, -1), (45.2, down, 1, 1),
        (46.5, combine, 0, 1), (48.0, combine, 1, -1), (49.5, combine, 1, 1),
    ):
        at(time, fn, 0, h, dy)
    at(49.7, finish, 0, 0)
    at(52.5, ag_forward, 1, 0, 0)
    at(53.5, finish, 0, 1)
    at(54.0, ag_forward, 1, 0, 1)
    at(58.0, ag_forward, 1, 1, 0)
    at(59.5, ag_forward, 1, 1, 1)
    at(62.0, ag_finish, 1, 0)
    for n in range(5):
        at(66.1 + 0.7 * n, hidden_later, 0, n)
    at(69.6, ag_finish, 1, 1)
    for n in range(5):
        at(70.5 + 0.7 * n, hidden_later, 1, n)
    for time, fn, h, dy in (
        (70.0, down, 0, 0), (74.0, down, 1, 0), (74.5, combine, 0, 0), (75.0, down, 0, 2), (75.5, down, 1, 2),
        (77.0, combine, 1, 0), (78.5, down, 0, -1), (78.8, down, 0, 1), (79.0, combine, 0, 2), (79.2, down, 1, -1),
        (79.4, combine, 1, 2), (79.6, down, 1, 1), (81.0, combine, 0, -1), (82.0, combine, 0, 1),
        (83.0, combine, 1, -1), (84.0, combine, 1, 1),
    ):
        at(time, fn, 1, h, dy)
    at(86.0, finish, 1, 0)
    at(88.0, finish, 1, 1)
    for _, _, fn, args in sorted(events, key=lambda e: e[:2]):
        fn(*args)

    for r in range(4):
        for dy in (0, 1, -1, 2):
            for dp in (0, 1):
                for st in (0, 1):
                    for s in (0, 1):
                        need(r, (dy, dp, st, s))
    for copy in sent:
        copy.wait_send()


def on_device(tokens, mixer_output, en, eg, ev, ed, ep, mg, ln, lg, lv, ld, lp):
    gains = [g.reshape(1, 2048) for g in (en, ep, mg, ln, lp)]
    en, ep, mg, ln, lp = gains
    return pl.pallas_call(
        kernel,
        out_shape=jax.ShapeDtypeStruct((128, 2048), BF),
        in_specs=[pl.BlockSpec(memory_space=pl.ANY)] * 13,
        out_specs=pl.BlockSpec(memory_space=pltpu.VMEM),
        scratch_shapes=[
            pltpu.VMEM((2, 2048, 1280), BF),
            pltpu.VMEM((2, 2048, 1280), BF),
            pltpu.VMEM((2, 8, 2, 1280, 128), BF),
            pltpu.VMEM((2, 512, 2048), BF),
            pltpu.VMEM((2, 512, 1280), F32),
            pltpu.VMEM((512, 1280), BF),
            pltpu.VMEM((128, 2048), BF),
            pltpu.VMEM((128, 2048), BF),
            pltpu.VMEM((128, 2048), BF),
            pltpu.VMEM((5, 1, 2048), F32),
            pltpu.VMEM((2, 2, 4, 2, 64, 512), BF),
            pltpu.VMEM((2, 2, 4, 2, 64, 512), BF),
            pltpu.VMEM((2, 2, 4, 2, 32, 512), BF),
            pltpu.VMEM((2, 2, 4, 2, 32, 512), BF),
            pltpu.VMEM((2, 4, 2, 32, 512), F32),
            pltpu.VMEM((128, 2048), F32),
            pltpu.VMEM((256, 512), F32),
            pltpu.SemaphoreType.DMA((16,)),
            pltpu.SemaphoreType.DMA((4, 4, 7)),
            pltpu.SemaphoreType.DMA((4, 4, 7)),
            pltpu.SemaphoreType.DMA((4, 32)),
            pltpu.SemaphoreType.DMA((4, 32)),
            pltpu.SemaphoreType.DMA((2, 2, 2, 6)),
            pltpu.SemaphoreType.DMA((2, 2, 2, 6)),
            pltpu.SemaphoreType.DMA((2, 2, 4, 4)),
            pltpu.SemaphoreType.DMA((2, 2, 4, 4)),
        ],
        compiler_params=pltpu.CompilerParams(
            collective_id=0, has_side_effects=True, vmem_limit_bytes=67_000_000
        ),
    )(tokens, mixer_output, en, eg, ev, ed, ep, mg, ln, lg, lv, ld, lp)


def solution(mesh):
    placed = (
        P(("rep", "fs", "tp"), None),
        P(("rep", "fs", "tp"), None),
        P(),
        P("fs", "tp"),
        P("fs", "tp"),
        P("tp", "fs"),
        P(),
        P(),
        P(),
        P("fs", "tp"),
        P("fs", "tp"),
        P("tp", "fs"),
        P(),
    )
    return jax.shard_map(
        on_device,
        mesh=mesh,
        in_specs=placed,
        out_specs=P(("rep", "fs", "tp"), None),
        check_vma=False,
    )
```

```python
import functools

import jax
import jax.numpy as jnp
from jax import lax
from jax.experimental import pallas as pl
from jax.experimental.pallas import tpu as pltpu
from jax.sharding import PartitionSpec as P

MESH = pl.DeviceIdType.MESH
EPS = 1e-06
BF = jnp.bfloat16
F32 = jnp.float32


ORDER = (
    ("en", 0), ("en", 1), ("ao", 0, 0, 0), ("ao", 0, 0, 1), ("ao", 0, 0, 2), ("ao", 0, 0, 3), ("ao", 0, 1, 0),
    ("af", 0, 0, 0), ("y", 0, 0), ("x", 0, 0), ("af", 0, 0, 1), ("ao", 0, 1, 1), ("y", 0, 1), ("x", 0, 1),
    ("ao", 0, 1, 2), ("af", 0, 1, 0), ("ao", 0, 1, 3), ("y", 0, 2), ("x", 0, 2), ("ae", 0, 0), ("af", 0, 1, 1),
    ("y", 0, 3), ("x", 0, 3), ("y", 0, 4), ("x", 0, 4), ("ae", 0, 1), ("g1", 0, 0), ("g1", 1, 0), ("g1", 0, 1),
    ("g1", 1, 1), ("g1", 0, 2), ("g1", 1, 2), ("y", 0, 5), ("x", 0, 5), ("g1", 0, 3), ("g1", 1, 3), ("g1", 0, 4),
    ("g1", 1, 4), ("y", 0, 6), ("x", 0, 6), ("g2", 0, 0), ("g2", 1, 0), ("g2", 0, 1), ("g2", 1, 1), ("g2", 0, 2),
    ("g2", 1, 2), ("y", 1, 0), ("x", 1, 0), ("g2", 0, 3), ("g2", 1, 3), ("g2", 0, 4), ("g2", 1, 4), ("y", 1, 1),
    ("x", 1, 1), ("he", 0, 0), ("he", 0, 1), ("he", 0, 2), ("he", 0, 3), ("he", 0, 4), ("d", 0, 0, (0, 0)),
    ("he", 1, 0), ("y", 1, 2), ("x", 1, 2), ("he", 1, 1), ("d", 0, 0, (0, 1)), ("he", 1, 2), ("he", 1, 3),
    ("he", 1, 4), ("y", 1, 3), ("x", 1, 3), ("d", 0, 1, (0, 0)), ("d", 0, 1, (0, 1)), ("c", 0, 0, (0, 0)),
    ("y", 1, 4), ("c", 0, 0, (0, 1)), ("x", 1, 4), ("d", 0, 0, (2, 0)), ("d", 0, 1, (2, 0)), ("c", 0, 1, (0, 0)),
    ("y", 1, 5), ("x", 1, 5), ("c", 0, 1, (0, 1)), ("y", 1, 6), ("c", 0, 0, (2, 0)), ("x", 1, 6),
    ("c", 0, 1, (2, 0)), ("d", 0, 0, (-1, 0)), ("d", 0, 0, (1, 0)), ("d", 0, 0, (2, 1)), ("d", 0, 1, (-1, 0)),
    ("d", 0, 0, (-1, 1)), ("y", 2, 0), ("d", 0, 0, (1, 1)), ("x", 2, 0), ("d", 0, 1, (1, 0)), ("c", 0, 0, (-1, 0)),
    ("c", 0, 0, (1, 0)), ("d", 0, 1, (2, 1)), ("c", 0, 0, (2, 1)), ("c", 0, 1, (-1, 0)), ("y", 2, 1),
    ("d", 0, 1, (-1, 1)), ("x", 2, 1), ("c", 0, 0, (-1, 1)), ("c", 0, 0, (1, 1)), ("d", 0, 1, (1, 1)),
    ("c", 0, 1, (1, 0)), ("c", 0, 1, (2, 1)), ("y", 2, 2), ("x", 2, 2), ("c", 0, 1, (-1, 1)), ("f", 0, 0),
    ("c", 0, 1, (1, 1)), ("ao", 1, 0, 0), ("ao", 1, 0, 1), ("ao", 1, 0, 2), ("y", 2, 3), ("x", 2, 3),
    ("ao", 1, 0, 3), ("f", 0, 1), ("ao", 1, 1, 0), ("af", 1, 0, 0), ("y", 2, 4), ("x", 2, 4), ("af", 1, 0, 1),
    ("ao", 1, 1, 1), ("y", 2, 5), ("x", 2, 5), ("ao", 1, 1, 2), ("af", 1, 1, 0), ("y", 2, 6), ("ao", 1, 1, 3),
    ("x", 2, 6), ("ae", 1, 0), ("y", 3, 0), ("x", 3, 0), ("af", 1, 1, 1), ("y", 3, 1), ("hl", 0, 0), ("x", 3, 1),
    ("hl", 0, 1), ("hl", 0, 2), ("y", 3, 2), ("x", 3, 2), ("hl", 0, 3), ("hl", 0, 4), ("y", 3, 3), ("x", 3, 3),
    ("d", 1, 0, (0, 0)), ("ae", 1, 1), ("d", 1, 0, (0, 1)), ("hl", 1, 0), ("y", 3, 4), ("hl", 1, 1), ("x", 3, 4),
    ("d", 1, 0, (2, 0)), ("hl", 1, 2), ("y", 3, 5), ("c", 1, 0, (0, 0)), ("hl", 1, 3), ("x", 3, 5),
    ("c", 1, 0, (0, 1)), ("hl", 1, 4), ("y", 3, 6), ("d", 1, 1, (0, 0)), ("x", 3, 6), ("c", 1, 0, (2, 0)),
    ("d", 1, 0, (-1, 0)), ("d", 1, 0, (1, 0)), ("d", 1, 0, (2, 1)), ("d", 1, 1, (0, 1)), ("d", 1, 0, (-1, 1)),
    ("c", 1, 1, (0, 0)), ("d", 1, 0, (1, 1)), ("c", 1, 0, (-1, 0)), ("d", 1, 1, (2, 0)), ("c", 1, 0, (1, 0)),
    ("c", 1, 0, (2, 1)), ("d", 1, 1, (-1, 0)), ("c", 1, 1, (0, 1)), ("c", 1, 0, (-1, 1)), ("d", 1, 1, (1, 0)),
    ("c", 1, 0, (1, 1)), ("d", 1, 1, (2, 1)), ("c", 1, 1, (2, 0)), ("d", 1, 1, (-1, 1)), ("d", 1, 1, (1, 1)),
    ("c", 1, 1, (-1, 0)), ("c", 1, 1, (1, 0)), ("f", 1, 0), ("c", 1, 1, (2, 1)), ("c", 1, 1, (-1, 1)),
    ("c", 1, 1, (1, 1)), ("f", 1, 1),
)


def kernel(
    tok, mix, en, eg, ev, ed, ep, mg, ln, lg, lv, ld, lp,
    out,
    gbuf, vbuf, dbuf, xbuf, acc, hbuf, tokv, mixv, mixed, gains,
    rs1, rr1, rs2, rr2, keep, br, pbuf,
    loc_sem, w_send, w_recv, p_send, p_recv, ag_send, ag_recv, rs_send, rs1_recv, rs2_recv,
):
    rep = lax.axis_index("rep")
    fs = lax.axis_index("fs")
    z = lax.axis_index("tp")
    c = lax.rem(fs, 2)
    xl = lax.rem(fs // 2, 2)
    y = fs // 4
    x = rep * 2 + xl

    def mod4(v):
        return lax.rem(v + 8, 4)

    def dev(dx=0, dy=0, dz=0, dc=0):
        nx = mod4(x + dx)
        ny = mod4(y + dy)
        nc = c if dc == 0 else 1 - c
        return (nx // 2, (ny * 2 + lax.rem(nx, 2)) * 2 + nc, mod4(z + dz))

    y_dev = {1: dev(dy=1), -1: dev(dy=-1)}
    x_dev = {1: dev(dx=1), -1: dev(dx=-1)}
    z_dev = {1: dev(dz=1), -1: dev(dz=-1)}
    partner = dev(dc=1)
    everyone = [y_dev[1], y_dev[-1], x_dev[1], x_dev[-1], z_dev[1], z_dev[-1], partner]
    zp, zm, zo = mod4(z + 1), mod4(z - 1), mod4(z + 2)

    def blk_of(dy, dp):
        return mod4(y + dy) * 2 + (xl if dp == 0 else 1 - xl)

    blocks = {(dy, dp): blk_of(dy, dp) for dy in (0, 1, -1, 2) for dp in (0, 1)}

    def unit(r, content, core):
        dy, dp, st, s = content
        blk = blocks[(dy, dp)]
        layer = r // 2
        if r % 2 == 0:
            buf = gbuf if st == 0 else vbuf
            row = pl.multiple_of(blk * 256 + core * 128 + s * 64, 64)
            return buf.at[layer, pl.ds(row, 64), :]
        return dbuf.at[layer, blk, core, pl.ds(st * 640 + s * 320, 320), :]

    def unit_id(content):
        dy, dp, st, s = content
        return (((dy % 4) * 2 + dp) * 2 + st) * 2 + s

    def send(src, dst, send_sem, recv_sem, target):
        pltpu.make_async_remote_copy(src, dst, send_sem, recv_sem, device_id=target, device_id_type=MESH).start()

    def await_bytes(ref, sem):
        pltpu.make_async_copy(ref, ref, sem).wait()

    def units(r, n):
        return gbuf.at[0, pl.ds(0, n * (64 if r % 2 == 0 else 32)), :]

    def tee(sign):
        return 0 if sign > 0 else 1

    def y_recv_content(sign, k):
        t = tee(sign)
        return [(-sign, 0, t, 0), (-sign, 0, t, 1), (2, 0, t, 0), (2, 0, t, 1),
                (-sign, 0, 1 - t, 0), (-sign, 0, 1 - t, 1), (-sign, 1, 1 - t, 1)][k]

    def y_send_content(sign, k):
        t = tee(sign)
        return [(0, 0, t, 0), (0, 0, t, 1), (-sign, 0, t, 0), (-sign, 0, t, 1),
                (0, 0, 1 - t, 0), (0, 0, 1 - t, 1), (0, 1, 1 - t, 1)][k]

    def x_content(sign, k, dp):
        t = tee(sign)
        return [(0, dp, t, 0), (0, dp, t, 1), (-sign, dp, t, 0), (-sign, dp, t, 1), (2, dp, t, 0),
                (2, dp, t, 1), (sign, dp, t, 0)][k]

    have = set()
    partner_have = set()

    def group_of(r, content):
        dy, dp, st, s = content
        if r == 2:
            return 19
        if r == 0:
            last = 1 if st == 0 else -1
            return 0 if dy in (0, -last) else (1 if dy == 2 else 2)
        return 3 + (r // 2) * 8 + (dy % 4) * 2 + dp

    def send_y(r, sign, k):
        content = y_send_content(sign, k)
        assert (r, content) in have
        ref = unit(r, content, c)
        send(ref, ref, w_send.at[r], w_recv.at[r, 0, k], y_dev[sign])

    def send_x(r, sign, k):
        content = x_content(sign, k, 0)
        assert (r, content) in have
        ref = unit(r, content, c)
        send(ref, ref, w_send.at[r], w_recv.at[r, 1, k], x_dev[sign])

    def send_partner(r, content):
        ref = unit(r, content, c)
        send(ref, ref, p_send.at[r], p_recv.at[group_of(r, content)], partner)

    every = [(dy, dp, st, s) for dy in (0, 1, -1, 2) for dp in (0, 1) for st in (0, 1) for s in (0, 1)]

    def need(r, group):
        members = [content for content in every if group_of(r, content) == group]
        assert all((r, content) in have for content in members), (r, group)
        if group not in partner_have:
            partner_have.add(group)
            await_bytes(units(r, len(members)), p_recv.at[group])

    def own_y(r):
        wait_local(r)
        for sign in (1, -1):
            send_y(r, sign, 0)
            send_y(r, sign, 1)

    def own_x(r):
        for sign in (1, -1):
            send_x(r, sign, 0)
            send_x(r, sign, 1)

    def own_partner(r):
        for st in (0, 1):
            for s in (0, 1):
                send_partner(r, (0, 0, st, s))

    def y_event(r, j):
        await_bytes(units(r, 2), w_recv.at[r, 0, j])
        for sign in (1, -1):
            have.add((r, y_recv_content(sign, j)))
        for sign in (1, -1):
            if j == 0:
                send_x(r, sign, 2)
                send_y(r, sign, 2)
            elif j == 1:
                send_x(r, sign, 3)
                send_y(r, sign, 3)
                send_y(r, sign, 4)
                send_y(r, sign, 5)
            elif j == 2:
                send_x(r, sign, 4)
            elif j == 3:
                send_x(r, sign, 5)
            elif j == 4:
                send_x(r, -sign, 6)
        if r < 3 and j == 3:
            own_y(r + 1)
        if r < 3 and j == 5:
            own_x(r + 1)
        for sign in (1, -1):
            send_partner(r, y_recv_content(sign, j))
        if r < 3 and j == 3:
            own_partner(r + 1)

    def x_event(r, j):
        await_bytes(units(r, 2), w_recv.at[r, 1, j])
        for sign in (1, -1):
            have.add((r, x_content(sign, j, 1)))
        for sign in (1, -1):
            if j == 1:
                send_y(r, sign, 6)
            send_partner(r, x_content(sign, j, 1))

    own = pl.multiple_of(blocks[(0, 0)] * 256 + c * 128, 128)
    weights = {
        0: [(eg, gbuf.at[0, pl.ds(own, 128), :]), (ev, vbuf.at[0, pl.ds(own, 128), :])],
        1: [(ed, dbuf.at[0, blocks[(0, 0)], c])],
        2: [(lg, gbuf.at[1, pl.ds(own, 128), :]), (lv, vbuf.at[1, pl.ds(own, 128), :])],
        3: [(ld, dbuf.at[1, blocks[(0, 0)], c])],
    }
    norms = [(g, gains.at[i]) for i, g in enumerate((en, ep, mg, ln, lp))]
    for i, pairs in enumerate((weights[0], [(tok, tokv)], norms, weights[1], weights[2], weights[3], [(mix, mixv)])):
        for src, dst in pairs:
            pltpu.make_async_copy(src, dst, loc_sem.at[i]).start()

    def wait_local(r):
        await_bytes(units(r, 4), loc_sem.at[(0, 3, 4, 5)[r]])
        for st in (0, 1):
            for s in (0, 1):
                have.add((r, (0, 0, st, s)))

    barrier = pltpu.get_barrier_semaphore()
    for other in everyone:
        pl.semaphore_signal(barrier, inc=1, device_id=other, device_id_type=MESH)
    pl.semaphore_wait(barrier, len(everyone))

    def x_rows(layer, h, zz, u, n=16):
        row = pl.multiple_of(h * 256 + zz * 64 + u * 16, 16)
        return xbuf.at[layer, pl.ds(row, n), :]

    def ag_own(layer, h, u):
        for sign in (1, -1):
            v = u if sign > 0 else (u + 2) % 4
            ref = x_rows(layer, h, z, v)
            send(ref, ref, ag_send.at[layer], ag_recv.at[layer, h, min(u, 2)], z_dev[sign])

    def ag_forward(layer, h, u):
        await_bytes(xbuf.at[0, pl.ds(0, 32), :], ag_recv.at[layer, h, u])
        for sign in (1, -1):
            v = u if sign > 0 else u + 2
            ref = x_rows(layer, h, zm if sign > 0 else zp, v)
            send(ref, ref, ag_send.at[layer], ag_recv.at[layer, h, 2], z_dev[sign])

    def ag_finish(layer, h):
        await_bytes(xbuf.at[0, pl.ds(0, 128), :], ag_recv.at[layer, h, 2])

    def rms(v, gain):
        return v * lax.rsqrt(jnp.mean(v * v, axis=-1, keepdims=True) + EPS) * gain

    def early_norm(h):
        def body(i, carry):
            rows = pl.ds(pl.multiple_of(h * 64 + i * 16, 16), 16)
            v = rms(tokv[rows, :].astype(F32), gains[0])
            x_rows(0, h, z, i)[...] = v.astype(BF)
            return carry

        lax.fori_loop(0, 4, body, 0)

    def dot_rows(st, rows, dy, cols):
        base = pl.multiple_of(mod4(y + dy) * 512, 512)
        w = gbuf if st == 0 else vbuf
        return jnp.dot(xbuf[0, rows, pl.ds(base, 512)], w[0, pl.ds(base, 512), cols], preferred_element_type=F32)

    whole = slice(0, 512)

    def tile(n):
        return slice(n * 256, n * 256 + 256)

    def gemm1(st, n):
        need(0, 0)
        acc[st, :, tile(n)] = dot_rows(st, whole, 0, tile(n)) + dot_rows(st, whole, -1 if st == 0 else 1, tile(n))

    def gemm2(st, n):
        need(0, 1)
        acc[st, :, tile(n)] += dot_rows(st, whole, 2, tile(n))

    def silu_mul(g, v):
        return (g * (1.0 / (1.0 + jnp.exp(-g))) * v).astype(BF)

    def hidden_early(h, n):
        need(0, 2)
        rows = slice(h * 256, h * 256 + 256)
        g = acc[0, rows, tile(n)] + dot_rows(0, rows, 1, tile(n))
        v = acc[1, rows, tile(n)] + dot_rows(1, rows, -1, tile(n))
        hbuf[rows, tile(n)] = silu_mul(g, v)

    def hidden_later(h, n):
        need(2, 19)
        rows = slice(h * 256, h * 256 + 256)
        cols = slice(n * 256, n * 256 + 256)
        xs = xbuf[1, rows, :]
        g = jnp.dot(xs, gbuf[1, :, cols], preferred_element_type=F32)
        v = jnp.dot(xs, vbuf[1, :, cols], preferred_element_type=F32)
        hbuf[rows, cols] = silu_mul(g, v)

    chunks = ((0, 0), (0, 1), (2, 0), (-1, 0), (1, 0), (2, 1), (-1, 1), (1, 1))

    def down(layer, h, chunk):
        r = 2 * layer + 1
        dy, dp = chunk
        need(r, group_of(r, (dy, dp, 0, 0)))
        j = chunks.index(chunk)
        blk = blocks[chunk]
        w = jnp.concatenate([dbuf[layer, blk, 0], dbuf[layer, blk, 1]], axis=1)
        pbuf[...] = jnp.dot(hbuf[h * 256 : h * 256 + 256, :], w, preferred_element_type=F32)

        def rows(zz, half):
            return pl.ds(pl.multiple_of(zz * 64 + half * 32, 32), 32)

        rs1[layer, h, j, 0, 0:32, :] = pbuf[rows(zo, 0), :].astype(BF)
        rs1[layer, h, j, 0, 32:64, :] = pbuf[rows(zp, 1), :].astype(BF)
        rs1[layer, h, j, 1, 0:32, :] = pbuf[rows(zm, 0), :].astype(BF)
        rs1[layer, h, j, 1, 32:64, :] = pbuf[rows(zo, 1), :].astype(BF)
        keep[h, j, 0] = pbuf[rows(zp, 0), :]
        keep[h, j, 1] = pbuf[rows(zm, 1), :]
        cols = pl.ds(pl.multiple_of(blk * 256, 256), 256)
        br[h * 64 : h * 64 + 64, cols] = pbuf[pl.ds(pl.multiple_of(z * 64, 64), 64), :]
        for sign in (1, -1):
            lane = tee(sign)
            send(rs1.at[layer, h, j, lane], rr1.at[layer, h, j, lane], rs_send.at[0], rs1_recv.at[layer, h, j], z_dev[sign])

    def combine(layer, h, chunk):
        j = chunks.index(chunk)
        await_bytes(rr1.at[layer, h, j], rs1_recv.at[layer, h, j])
        for sign in (1, -1):
            lane = tee(sign)
            half = slice(0, 32) if sign > 0 else slice(32, 64)
            rs2[layer, h, j, lane] = (rr1[layer, h, j, lane, half, :].astype(F32) + keep[h, j, lane]).astype(BF)
        for sign in (1, -1):
            lane = tee(sign)
            send(rs2.at[layer, h, j, lane], rr2.at[layer, h, j, lane], rs_send.at[1], rs2_recv.at[layer, h], z_dev[sign])

    def finish(layer, h):
        await_bytes(rr2.at[layer, h], rs2_recv.at[layer, h])
        a = slice(h * 64, h * 64 + 32)
        b = slice(h * 64 + 32, h * 64 + 64)
        for j, chunk in enumerate(chunks):
            cols = pl.ds(pl.multiple_of(blocks[chunk] * 256, 256), 256)
            br[a, cols] += rr2[layer, h, j, 0].astype(F32) + rr1[layer, h, j, 1, 0:32, :].astype(F32)
            br[b, cols] += rr2[layer, h, j, 1].astype(F32) + rr1[layer, h, j, 0, 32:64, :].astype(F32)

        def body(i, carry):
            rows = pl.ds(pl.multiple_of(h * 64 + i * 16, 16), 16)
            branch = br[rows, :]
            if layer == 0:
                m = tokv[rows, :].astype(F32) + 0.5 * rms(branch, gains[1]) + rms(mixv[rows, :].astype(F32), gains[2])
                m = m.astype(BF)
                mixed[rows, :] = m
                x_rows(1, h, z, i)[...] = rms(m.astype(F32), gains[3]).astype(BF)
            else:
                out[rows, :] = (mixed[rows, :].astype(F32) + 0.5 * rms(branch, gains[4])).astype(BF)
            return carry

        lax.fori_loop(0, 4, body, 0)

    wait_local(0)
    for sign in (1, -1):
        send_y(0, sign, 0)
        send_x(0, sign, 0)
        send_y(0, sign, 1)
        send_x(0, sign, 1)
    own_partner(0)
    await_bytes(tokv, loc_sem.at[1])
    await_bytes(gains, loc_sem.at[2])
    await_bytes(mixv, loc_sem.at[6])
    tasks = dict(
        y=y_event, x=x_event, en=early_norm, ao=ag_own, af=ag_forward, ae=ag_finish, g1=gemm1, g2=gemm2,
        he=hidden_early, hl=hidden_later, d=down, c=combine, f=finish,
    )
    for name, *args in ORDER:
        fn = tasks[name]
        fn(*args)

    for r in range(4):
        await_bytes(units(r, 28), w_send.at[r])
        await_bytes(units(r, 32), p_send.at[r])
    for layer in (0, 1):
        await_bytes(xbuf.at[0, pl.ds(0, 384), :], ag_send.at[layer])
    await_bytes(rs1, rs_send.at[0])
    await_bytes(rs2, rs_send.at[1])


def on_device(tokens, mixer_output, en, eg, ev, ed, ep, mg, ln, lg, lv, ld, lp):
    gains = [g.reshape(1, 2048) for g in (en, ep, mg, ln, lp)]
    en, ep, mg, ln, lp = gains
    return pl.pallas_call(
        kernel,
        out_shape=jax.ShapeDtypeStruct((128, 2048), BF),
        in_specs=[pl.BlockSpec(memory_space=pl.ANY)] * 13,
        out_specs=pl.BlockSpec(memory_space=pltpu.VMEM),
        scratch_shapes=[
            pltpu.VMEM((2, 2048, 1280), BF),
            pltpu.VMEM((2, 2048, 1280), BF),
            pltpu.VMEM((2, 8, 2, 1280, 128), BF),
            pltpu.VMEM((2, 512, 2048), BF),
            pltpu.VMEM((2, 512, 1280), F32),
            pltpu.VMEM((512, 1280), BF),
            pltpu.VMEM((128, 2048), BF),
            pltpu.VMEM((128, 2048), BF),
            pltpu.VMEM((128, 2048), BF),
            pltpu.VMEM((5, 1, 2048), F32),
            pltpu.VMEM((2, 2, 8, 2, 64, 256), BF),
            pltpu.VMEM((2, 2, 8, 2, 64, 256), BF),
            pltpu.VMEM((2, 2, 8, 2, 32, 256), BF),
            pltpu.VMEM((2, 2, 8, 2, 32, 256), BF),
            pltpu.VMEM((2, 8, 2, 32, 256), F32),
            pltpu.VMEM((128, 2048), F32),
            pltpu.VMEM((256, 256), F32),
            pltpu.SemaphoreType.DMA((7,)),
            pltpu.SemaphoreType.DMA((4,)),
            pltpu.SemaphoreType.DMA((4, 2, 7)),
            pltpu.SemaphoreType.DMA((4,)),
            pltpu.SemaphoreType.DMA((20,)),
            pltpu.SemaphoreType.DMA((2,)),
            pltpu.SemaphoreType.DMA((2, 2, 3)),
            pltpu.SemaphoreType.DMA((2,)),
            pltpu.SemaphoreType.DMA((2, 2, 8)),
            pltpu.SemaphoreType.DMA((2, 2)),
        ],
        compiler_params=pltpu.CompilerParams(
            collective_id=0, has_side_effects=True, vmem_limit_bytes=67_000_000
        ),
    )(tokens, mixer_output, en, eg, ev, ed, ep, mg, ln, lg, lv, ld, lp)


def solution(mesh):
    placed = (
        P(("rep", "fs", "tp"), None),
        P(("rep", "fs", "tp"), None),
        P(),
        P("fs", "tp"),
        P("fs", "tp"),
        P("tp", "fs"),
        P(),
        P(),
        P(),
        P("fs", "tp"),
        P("fs", "tp"),
        P("tp", "fs"),
        P(),
    )
    return jax.shard_map(
        on_device,
        mesh=mesh,
        in_specs=placed,
        out_specs=P(("rep", "fs", "tp"), None),
        check_vma=False,
    )
```

```python
import functools

import jax
import jax.numpy as jnp
from jax import lax
from jax.experimental import pallas as pl
from jax.experimental.pallas import tpu as pltpu
from jax.sharding import PartitionSpec as P

MESH = pl.DeviceIdType.MESH
EPS = 1e-06
BF = jnp.bfloat16
F32 = jnp.float32


ORDER = (
    ("en", 0), ("en", 1), ("ao", 0, 1, 0), ("ao", 0, 1, 1), ("ao", 0, 1, 2), ("ao", 0, 1, 3), ("ao", 0, 0, 0),
    ("ao", 0, 0, 1), ("af", 0, 1, 0), ("y", 0, 0), ("x", 0, 0), ("af", 0, 1, 1), ("ao", 0, 0, 2), ("y", 0, 1),
    ("x", 0, 1), ("ao", 0, 0, 3), ("af", 0, 0, 0), ("af", 0, 0, 1), ("y", 0, 2), ("x", 0, 2), ("ae", 0, 1),
    ("y", 0, 3), ("x", 0, 3), ("y", 0, 4), ("x", 0, 4), ("ae", 0, 0), ("g1", 0, 1), ("g1", 0, 4), ("g1", 1, 4),
    ("g1", 1, 2), ("y", 0, 5), ("x", 0, 5), ("g1", 0, 3), ("g1", 0, 0), ("g1", 1, 1), ("g1", 0, 2), ("g1", 1, 3),
    ("g1", 1, 0), ("y", 0, 6), ("x", 0, 6), ("y", 1, 0), ("x", 1, 0), ("y", 1, 1), ("x", 1, 1), ("he", 1, 2),
    ("he", 0, 4), ("he", 0, 0), ("y", 1, 2), ("he", 0, 2), ("he", 0, 1), ("x", 1, 2), ("he", 1, 4), ("y", 1, 3),
    ("he", 1, 0), ("he", 0, 3), ("d", 0, 0, (0, 0)), ("x", 1, 3), ("d", 0, 0, (0, 1)), ("y", 1, 4), ("he", 1, 3),
    ("he", 1, 1), ("d", 0, 1, (0, 0)), ("x", 1, 4), ("y", 1, 5), ("d", 0, 1, (0, 1)), ("x", 1, 5),
    ("c", 0, 0, (0, 0)), ("y", 1, 6), ("d", 0, 0, (2, 0)), ("c", 0, 0, (0, 1)), ("d", 0, 1, (2, 0)), ("x", 1, 6),
    ("d", 0, 0, (1, 0)), ("d", 0, 0, (-1, 0)), ("c", 0, 1, (0, 1)), ("d", 0, 0, (1, 1)), ("d", 0, 0, (-1, 1)),
    ("d", 0, 0, (2, 1)), ("y", 2, 0), ("c", 0, 0, (2, 0)), ("c", 0, 1, (0, 0)), ("x", 2, 0), ("d", 0, 1, (2, 1)),
    ("c", 0, 1, (2, 0)), ("c", 0, 0, (1, 0)), ("d", 0, 1, (-1, 1)), ("y", 2, 1), ("c", 0, 0, (-1, 0)),
    ("d", 0, 1, (-1, 0)), ("c", 0, 0, (1, 1)), ("x", 2, 1), ("c", 0, 0, (-1, 1)), ("d", 0, 1, (1, 1)),
    ("c", 0, 0, (2, 1)), ("d", 0, 1, (1, 0)), ("y", 2, 2), ("c", 0, 1, (2, 1)), ("x", 2, 2), ("c", 0, 1, (-1, 1)),
    ("c", 0, 1, (-1, 0)), ("y", 2, 3), ("c", 0, 1, (1, 1)), ("f", 0, 0), ("x", 2, 3), ("ao", 1, 0, 0),
    ("ao", 1, 0, 1), ("ao", 1, 0, 2), ("c", 0, 1, (1, 0)), ("ao", 1, 0, 3), ("y", 2, 4), ("x", 2, 4),
    ("af", 1, 0, 0), ("y", 2, 5), ("af", 1, 0, 1), ("x", 2, 5), ("f", 0, 1), ("ao", 1, 1, 0), ("ao", 1, 1, 1),
    ("ao", 1, 1, 2), ("y", 2, 6), ("ao", 1, 1, 3), ("x", 2, 6), ("y", 3, 0), ("ae", 1, 0), ("x", 3, 0),
    ("y", 3, 1), ("af", 1, 1, 0), ("hl", 0, 4), ("hl", 0, 2), ("x", 3, 1), ("y", 3, 2), ("af", 1, 1, 1),
    ("hl", 0, 1), ("hl", 0, 0), ("x", 3, 2), ("y", 3, 3), ("hl", 0, 3), ("d", 1, 0, (0, 0)), ("x", 3, 3),
    ("d", 1, 0, (0, 1)), ("y", 3, 4), ("x", 3, 4), ("y", 3, 5), ("ae", 1, 1), ("hl", 1, 4), ("d", 1, 0, (2, 0)),
    ("x", 3, 5), ("y", 3, 6), ("hl", 1, 2), ("c", 1, 0, (0, 1)), ("d", 1, 0, (1, 0)), ("x", 3, 6),
    ("d", 1, 0, (-1, 0)), ("c", 1, 0, (0, 0)), ("hl", 1, 0), ("d", 1, 0, (-1, 1)), ("d", 1, 0, (1, 1)),
    ("c", 1, 0, (2, 0)), ("hl", 1, 1), ("d", 1, 0, (2, 1)), ("c", 1, 0, (1, 0)), ("hl", 1, 3),
    ("c", 1, 0, (-1, 0)), ("d", 1, 1, (2, 1)), ("d", 1, 1, (-1, 1)), ("d", 1, 1, (1, 0)), ("d", 1, 1, (0, 1)),
    ("d", 1, 1, (2, 0)), ("d", 1, 1, (0, 0)), ("d", 1, 1, (1, 1)), ("d", 1, 1, (-1, 0)), ("c", 1, 1, (2, 1)),
    ("c", 1, 0, (-1, 1)), ("c", 1, 0, (2, 1)), ("c", 1, 0, (1, 1)), ("c", 1, 1, (-1, 1)), ("c", 1, 1, (1, 0)),
    ("c", 1, 1, (0, 1)), ("c", 1, 1, (2, 0)), ("c", 1, 1, (0, 0)), ("c", 1, 1, (1, 1)), ("c", 1, 1, (-1, 0)),
    ("f", 1, 0), ("f", 1, 1),
)
OWN_Y_AT = 3
OWN_X_AT = 4


def kernel(
    tok, mix, en, eg, ev, ed, ep, mg, ln, lg, lv, ld, lp,
    out,
    gbuf, vbuf, dbuf, xbuf, acc, hbuf, tokv, mixv, mixed, gains,
    rs1, rr1, rs2, rr2, keep, br, pbuf,
    loc_sem, w_send, w_recv, p_send, p_recv, ag_send, ag_recv, rs_send, rs1_recv, rs2_recv,
):
    rep = lax.axis_index("rep")
    fs = lax.axis_index("fs")
    z = lax.axis_index("tp")
    c = lax.rem(fs, 2)
    xl = lax.rem(fs // 2, 2)
    y = fs // 4
    x = rep * 2 + xl

    def mod4(v):
        return lax.rem(v + 8, 4)

    def dev(dx=0, dy=0, dz=0, dc=0):
        nx = mod4(x + dx)
        ny = mod4(y + dy)
        nc = c if dc == 0 else 1 - c
        return (nx // 2, (ny * 2 + lax.rem(nx, 2)) * 2 + nc, mod4(z + dz))

    y_dev = {1: dev(dy=1), -1: dev(dy=-1)}
    x_dev = {1: dev(dx=1), -1: dev(dx=-1)}
    z_dev = {1: dev(dz=1), -1: dev(dz=-1)}
    partner = dev(dc=1)
    everyone = [y_dev[1], y_dev[-1], x_dev[1], x_dev[-1], z_dev[1], z_dev[-1], partner]
    zp, zm, zo = mod4(z + 1), mod4(z - 1), mod4(z + 2)

    def blk_of(dy, dp):
        return mod4(y + dy) * 2 + (xl if dp == 0 else 1 - xl)

    blocks = {(dy, dp): blk_of(dy, dp) for dy in (0, 1, -1, 2) for dp in (0, 1)}

    def unit(r, content, core):
        dy, dp, st, s = content
        blk = blocks[(dy, dp)]
        layer = r // 2
        if r % 2 == 0:
            buf = gbuf if st == 0 else vbuf
            row = pl.multiple_of(blk * 256 + core * 128 + s * 64, 64)
            return buf.at[layer, pl.ds(row, 64), :]
        return dbuf.at[layer, blk, core, pl.ds(st * 640 + s * 320, 320), :]

    def unit_id(content):
        dy, dp, st, s = content
        return (((dy % 4) * 2 + dp) * 2 + st) * 2 + s

    def send(src, dst, send_sem, recv_sem, target):
        pltpu.make_async_remote_copy(src, dst, send_sem, recv_sem, device_id=target, device_id_type=MESH).start()

    def await_bytes(ref, sem):
        pltpu.make_async_copy(ref, ref, sem).wait()

    def units(r, n):
        return gbuf.at[0, pl.ds(0, n * (64 if r % 2 == 0 else 32)), :]

    def tee(sign):
        return 0 if sign > 0 else 1

    def y_recv_content(sign, k):
        t = tee(sign)
        return [(-sign, 0, t, 0), (-sign, 0, t, 1), (-sign, 0, 1 - t, 0), (2, 0, t, 0), (2, 0, t, 1),
                (-sign, 0, 1 - t, 1), (-sign, 1, 1 - t, 1)][k]

    def y_send_content(sign, k):
        t = tee(sign)
        return [(0, 0, t, 0), (0, 0, t, 1), (0, 0, 1 - t, 0), (-sign, 0, t, 0), (-sign, 0, t, 1),
                (0, 0, 1 - t, 1), (0, 1, 1 - t, 1)][k]

    def x_content(sign, k, dp):
        t = tee(sign)
        return [(0, dp, t, 0), (0, dp, t, 1), (-sign, dp, t, 0), (-sign, dp, t, 1), (sign, dp, t, 0),
                (2, dp, t, 0), (2, dp, t, 1)][k]

    have = set()
    partner_have = set()

    def group_of(r, content):
        dy, dp, st, s = content
        if r == 2:
            return 18
        if r == 0:
            return 0 if dy in (0, -1 if st == 0 else 1) else 1
        return 2 + (r // 2) * 8 + (dy % 4) * 2 + dp

    def send_y(r, sign, k):
        content = y_send_content(sign, k)
        assert (r, content) in have
        ref = unit(r, content, c)
        send(ref, ref, w_send.at[r], w_recv.at[r, 0, k], y_dev[sign])

    def send_x(r, sign, k):
        content = x_content(sign, k, 0)
        assert (r, content) in have
        ref = unit(r, content, c)
        send(ref, ref, w_send.at[r], w_recv.at[r, 1, k], x_dev[sign])

    def send_partner(r, content):
        ref = unit(r, content, c)
        send(ref, ref, p_send.at[r], p_recv.at[group_of(r, content)], partner)

    every = [(dy, dp, st, s) for dy in (0, 1, -1, 2) for dp in (0, 1) for st in (0, 1) for s in (0, 1)]

    def need(r, group):
        members = [content for content in every if group_of(r, content) == group]
        assert all((r, content) in have for content in members), (r, group)
        if group not in partner_have:
            partner_have.add(group)
            await_bytes(units(r, len(members)), p_recv.at[group])

    def own_y(r):
        wait_local(r)
        for sign in (1, -1):
            for k in (0, 1, 2):
                send_y(r, sign, k)

    def own_x(r):
        for sign in (1, -1):
            send_x(r, sign, 0)
            send_x(r, sign, 1)

    def own_partner(r):
        for st in (0, 1):
            for s in (0, 1):
                send_partner(r, (0, 0, st, s))

    def y_event(r, j):
        await_bytes(units(r, 2), w_recv.at[r, 0, j])
        for sign in (1, -1):
            have.add((r, y_recv_content(sign, j)))
        for sign in (1, -1):
            if j == 0:
                send_x(r, sign, 2)
                send_y(r, sign, 3)
            elif j == 1:
                send_x(r, sign, 3)
                send_y(r, sign, 4)
                send_y(r, sign, 5)
            elif j == 2:
                send_x(r, -sign, 4)
            elif j == 3:
                send_x(r, sign, 5)
            elif j == 4:
                send_x(r, sign, 6)
        if r < 3 and j == OWN_Y_AT:
            own_y(r + 1)
        if r < 3 and j == OWN_X_AT:
            own_x(r + 1)
        for sign in (1, -1):
            send_partner(r, y_recv_content(sign, j))
        if r < 3 and j == OWN_Y_AT:
            own_partner(r + 1)

    def x_event(r, j):
        await_bytes(units(r, 2), w_recv.at[r, 1, j])
        for sign in (1, -1):
            have.add((r, x_content(sign, j, 1)))
        for sign in (1, -1):
            if j == 1:
                send_y(r, sign, 6)
            send_partner(r, x_content(sign, j, 1))

    own = pl.multiple_of(blocks[(0, 0)] * 256 + c * 128, 128)
    weights = {
        0: [(eg, gbuf.at[0, pl.ds(own, 128), :]), (ev, vbuf.at[0, pl.ds(own, 128), :])],
        1: [(ed, dbuf.at[0, blocks[(0, 0)], c])],
        2: [(lg, gbuf.at[1, pl.ds(own, 128), :]), (lv, vbuf.at[1, pl.ds(own, 128), :])],
        3: [(ld, dbuf.at[1, blocks[(0, 0)], c])],
    }
    norms = [(g, gains.at[i]) for i, g in enumerate((en, ep, mg, ln, lp))]
    for i, pairs in enumerate((weights[0], [(tok, tokv)], norms, weights[1], weights[2], weights[3], [(mix, mixv)])):
        for src, dst in pairs:
            pltpu.make_async_copy(src, dst, loc_sem.at[i]).start()

    def wait_local(r):
        await_bytes(units(r, 4), loc_sem.at[(0, 3, 4, 5)[r]])
        for st in (0, 1):
            for s in (0, 1):
                have.add((r, (0, 0, st, s)))

    barrier = pltpu.get_barrier_semaphore()
    for other in everyone:
        pl.semaphore_signal(barrier, inc=1, device_id=other, device_id_type=MESH)
    pl.semaphore_wait(barrier, len(everyone))

    def x_rows(layer, h, zz, u, n=16):
        row = pl.multiple_of(h * 256 + zz * 64 + u * 16, 16)
        return xbuf.at[layer, pl.ds(row, n), :]

    def ag_own(layer, h, u):
        for sign in (1, -1):
            v = u if sign > 0 else (u + 2) % 4
            ref = x_rows(layer, h, z, v)
            send(ref, ref, ag_send.at[layer], ag_recv.at[layer, h, min(u, 2)], z_dev[sign])

    def ag_forward(layer, h, u):
        await_bytes(xbuf.at[0, pl.ds(0, 32), :], ag_recv.at[layer, h, u])
        for sign in (1, -1):
            v = u if sign > 0 else u + 2
            ref = x_rows(layer, h, zm if sign > 0 else zp, v)
            send(ref, ref, ag_send.at[layer], ag_recv.at[layer, h, 2], z_dev[sign])

    def ag_finish(layer, h):
        await_bytes(xbuf.at[0, pl.ds(0, 128), :], ag_recv.at[layer, h, 2])

    def rms(v, gain):
        return v * lax.rsqrt(jnp.mean(v * v, axis=-1, keepdims=True) + EPS) * gain

    def early_norm(h):
        def body(i, carry):
            rows = pl.ds(pl.multiple_of(h * 64 + i * 16, 16), 16)
            v = rms(tokv[rows, :].astype(F32), gains[0])
            x_rows(0, h, z, i)[...] = v.astype(BF)
            return carry

        lax.fori_loop(0, 4, body, 0)

    def dot_rows(st, rows, dy, cols):
        base = pl.multiple_of(mod4(y + dy) * 512, 512)
        w = gbuf if st == 0 else vbuf
        return jnp.dot(xbuf[0, rows, pl.ds(base, 512)], w[0, pl.ds(base, 512), cols], preferred_element_type=F32)

    whole = slice(0, 512)

    def tile(n):
        return slice(n * 256, n * 256 + 256)

    def gemm1(st, n):
        need(0, 0)
        acc[st, :, tile(n)] = dot_rows(st, whole, 0, tile(n)) + dot_rows(st, whole, -1 if st == 0 else 1, tile(n))

    def silu_mul(g, v):
        return (g * (1.0 / (1.0 + jnp.exp(-g))) * v).astype(BF)

    def hidden_early(h, n):
        need(0, 1)
        rows = slice(h * 256, h * 256 + 256)
        g = acc[0, rows, tile(n)] + dot_rows(0, rows, 2, tile(n)) + dot_rows(0, rows, 1, tile(n))
        v = acc[1, rows, tile(n)] + dot_rows(1, rows, 2, tile(n)) + dot_rows(1, rows, -1, tile(n))
        hbuf[rows, tile(n)] = silu_mul(g, v)

    def hidden_later(h, n):
        need(2, 18)
        rows = slice(h * 256, h * 256 + 256)
        cols = slice(n * 256, n * 256 + 256)
        xs = xbuf[1, rows, :]
        g = jnp.dot(xs, gbuf[1, :, cols], preferred_element_type=F32)
        v = jnp.dot(xs, vbuf[1, :, cols], preferred_element_type=F32)
        hbuf[rows, cols] = silu_mul(g, v)

    chunks = ((0, 0), (0, 1), (2, 0), (-1, 0), (1, 0), (2, 1), (-1, 1), (1, 1))

    def down(layer, h, chunk):
        r = 2 * layer + 1
        dy, dp = chunk
        need(r, group_of(r, (dy, dp, 0, 0)))
        j = chunks.index(chunk)
        blk = blocks[chunk]
        w = jnp.concatenate([dbuf[layer, blk, 0], dbuf[layer, blk, 1]], axis=1)
        pbuf[...] = jnp.dot(hbuf[h * 256 : h * 256 + 256, :], w, preferred_element_type=F32)

        def rows(zz, half):
            return pl.ds(pl.multiple_of(zz * 64 + half * 32, 32), 32)

        rs1[layer, h, j, 0, 0:32, :] = pbuf[rows(zo, 0), :].astype(BF)
        rs1[layer, h, j, 0, 32:64, :] = pbuf[rows(zp, 1), :].astype(BF)
        rs1[layer, h, j, 1, 0:32, :] = pbuf[rows(zm, 0), :].astype(BF)
        rs1[layer, h, j, 1, 32:64, :] = pbuf[rows(zo, 1), :].astype(BF)
        keep[h, j, 0] = pbuf[rows(zp, 0), :]
        keep[h, j, 1] = pbuf[rows(zm, 1), :]
        cols = pl.ds(pl.multiple_of(blk * 256, 256), 256)
        br[h * 64 : h * 64 + 64, cols] = pbuf[pl.ds(pl.multiple_of(z * 64, 64), 64), :]
        for sign in (1, -1):
            lane = tee(sign)
            send(rs1.at[layer, h, j, lane], rr1.at[layer, h, j, lane], rs_send.at[0], rs1_recv.at[layer, h, j], z_dev[sign])

    def combine(layer, h, chunk):
        j = chunks.index(chunk)
        await_bytes(rr1.at[layer, h, j], rs1_recv.at[layer, h, j])
        for sign in (1, -1):
            lane = tee(sign)
            half = slice(0, 32) if sign > 0 else slice(32, 64)
            rs2[layer, h, j, lane] = (rr1[layer, h, j, lane, half, :].astype(F32) + keep[h, j, lane]).astype(BF)
        for sign in (1, -1):
            lane = tee(sign)
            send(rs2.at[layer, h, j, lane], rr2.at[layer, h, j, lane], rs_send.at[1], rs2_recv.at[layer, h], z_dev[sign])

    def finish(layer, h):
        await_bytes(rr2.at[layer, h], rs2_recv.at[layer, h])
        a = slice(h * 64, h * 64 + 32)
        b = slice(h * 64 + 32, h * 64 + 64)
        for j, chunk in enumerate(chunks):
            cols = pl.ds(pl.multiple_of(blocks[chunk] * 256, 256), 256)
            br[a, cols] += rr2[layer, h, j, 0].astype(F32) + rr1[layer, h, j, 1, 0:32, :].astype(F32)
            br[b, cols] += rr2[layer, h, j, 1].astype(F32) + rr1[layer, h, j, 0, 32:64, :].astype(F32)

        def body(i, carry):
            rows = pl.ds(pl.multiple_of(h * 64 + i * 16, 16), 16)
            branch = br[rows, :]
            if layer == 0:
                m = tokv[rows, :].astype(F32) + 0.5 * rms(branch, gains[1]) + rms(mixv[rows, :].astype(F32), gains[2])
                m = m.astype(BF)
                mixed[rows, :] = m
                x_rows(1, h, z, i)[...] = rms(m.astype(F32), gains[3]).astype(BF)
            else:
                out[rows, :] = (mixed[rows, :].astype(F32) + 0.5 * rms(branch, gains[4])).astype(BF)
            return carry

        lax.fori_loop(0, 4, body, 0)

    wait_local(0)
    for sign in (1, -1):
        send_y(0, sign, 0)
        send_x(0, sign, 0)
        send_y(0, sign, 1)
        send_x(0, sign, 1)
        send_y(0, sign, 2)
    own_partner(0)
    await_bytes(tokv, loc_sem.at[1])
    await_bytes(gains, loc_sem.at[2])
    await_bytes(mixv, loc_sem.at[6])
    tasks = dict(
        y=y_event, x=x_event, en=early_norm, ao=ag_own, af=ag_forward, ae=ag_finish, g1=gemm1,
        he=hidden_early, hl=hidden_later, d=down, c=combine, f=finish,
    )
    for name, *args in ORDER:
        fn = tasks[name]
        fn(*args)

    for r in range(4):
        await_bytes(units(r, 28), w_send.at[r])
        await_bytes(units(r, 32), p_send.at[r])
    for layer in (0, 1):
        await_bytes(xbuf.at[0, pl.ds(0, 384), :], ag_send.at[layer])
    await_bytes(rs1, rs_send.at[0])
    await_bytes(rs2, rs_send.at[1])


def on_device(tokens, mixer_output, en, eg, ev, ed, ep, mg, ln, lg, lv, ld, lp):
    gains = [g.reshape(1, 2048) for g in (en, ep, mg, ln, lp)]
    en, ep, mg, ln, lp = gains
    return pl.pallas_call(
        kernel,
        out_shape=jax.ShapeDtypeStruct((128, 2048), BF),
        in_specs=[pl.BlockSpec(memory_space=pl.ANY)] * 13,
        out_specs=pl.BlockSpec(memory_space=pltpu.VMEM),
        scratch_shapes=[
            pltpu.VMEM((2, 2048, 1280), BF),
            pltpu.VMEM((2, 2048, 1280), BF),
            pltpu.VMEM((2, 8, 2, 1280, 128), BF),
            pltpu.VMEM((2, 512, 2048), BF),
            pltpu.VMEM((2, 512, 1280), F32),
            pltpu.VMEM((512, 1280), BF),
            pltpu.VMEM((128, 2048), BF),
            pltpu.VMEM((128, 2048), BF),
            pltpu.VMEM((128, 2048), BF),
            pltpu.VMEM((5, 1, 2048), F32),
            pltpu.VMEM((2, 2, 8, 2, 64, 256), BF),
            pltpu.VMEM((2, 2, 8, 2, 64, 256), BF),
            pltpu.VMEM((2, 2, 8, 2, 32, 256), BF),
            pltpu.VMEM((2, 2, 8, 2, 32, 256), BF),
            pltpu.VMEM((2, 8, 2, 32, 256), F32),
            pltpu.VMEM((128, 2048), F32),
            pltpu.VMEM((256, 256), F32),
            pltpu.SemaphoreType.DMA((7,)),
            pltpu.SemaphoreType.DMA((4,)),
            pltpu.SemaphoreType.DMA((4, 2, 7)),
            pltpu.SemaphoreType.DMA((4,)),
            pltpu.SemaphoreType.DMA((19,)),
            pltpu.SemaphoreType.DMA((2,)),
            pltpu.SemaphoreType.DMA((2, 2, 3)),
            pltpu.SemaphoreType.DMA((2,)),
            pltpu.SemaphoreType.DMA((2, 2, 8)),
            pltpu.SemaphoreType.DMA((2, 2)),
        ],
        compiler_params=pltpu.CompilerParams(
            collective_id=0, has_side_effects=True, vmem_limit_bytes=67_000_000
        ),
    )(tokens, mixer_output, en, eg, ev, ed, ep, mg, ln, lg, lv, ld, lp)


def solution(mesh):
    placed = (
        P(("rep", "fs", "tp"), None),
        P(("rep", "fs", "tp"), None),
        P(),
        P("fs", "tp"),
        P("fs", "tp"),
        P("tp", "fs"),
        P(),
        P(),
        P(),
        P("fs", "tp"),
        P("fs", "tp"),
        P("tp", "fs"),
        P(),
    )
    return jax.shard_map(
        on_device,
        mesh=mesh,
        in_specs=placed,
        out_specs=P(("rep", "fs", "tp"), None),
        check_vma=False,
    )
```

```python
import functools

import jax
import jax.numpy as jnp
from jax import lax
from jax.experimental import pallas as pl
from jax.experimental.pallas import tpu as pltpu
from jax.sharding import PartitionSpec as P

MESH = pl.DeviceIdType.MESH
EPS = 1e-06
BF = jnp.bfloat16
F32 = jnp.float32


ORDER = (
    ("en", 0), ("ao", 0, 0, 0), ("ao", 0, 0, 1), ("ao", 0, 0, 2), ("en", 1), ("ao", 0, 1, 0), ("ao", 0, 1, 1),
    ("af", 0, 0, 0), ("ao", 0, 0, 3), ("af", 0, 0, 1), ("y", 0, 0), ("x", 0, 0), ("ao", 0, 1, 2), ("af", 0, 1, 0),
    ("y", 0, 1), ("x", 0, 1), ("af", 0, 1, 1), ("ao", 0, 1, 3), ("y", 0, 2), ("x", 0, 2), ("ae", 0, 0),
    ("y", 0, 3), ("x", 0, 3), ("ae", 0, 1), ("g1", 0, 1), ("y", 0, 4), ("x", 0, 4), ("g1", 1, 2), ("g1", 1, 3),
    ("g1", 0, 2), ("g1", 0, 3), ("g1", 1, 4), ("g1", 0, 0), ("g1", 0, 4), ("g1", 1, 0), ("y", 0, 5), ("x", 0, 5),
    ("g1", 1, 1), ("y", 0, 6), ("x", 0, 6), ("y", 1, 0), ("x", 1, 0), ("he", 1, 0), ("he", 0, 2), ("he", 1, 4),
    ("y", 1, 1), ("x", 1, 1), ("he", 0, 0), ("he", 0, 1), ("he", 0, 4), ("he", 0, 3), ("d", 0, 0, (0, 0)),
    ("y", 1, 2), ("d", 0, 0, (0, 1)), ("he", 1, 1), ("he", 1, 3), ("x", 1, 2), ("he", 1, 2), ("d", 0, 1, (0, 0)),
    ("y", 1, 3), ("d", 0, 1, (0, 1)), ("x", 1, 3), ("y", 1, 4), ("d", 0, 1, (1, 0)), ("d", 0, 1, (-1, 0)),
    ("c", 0, 0, (0, 0)), ("d", 0, 0, (-1, 0)), ("x", 1, 4), ("d", 0, 0, (1, 0)), ("y", 1, 5), ("c", 0, 0, (0, 1)),
    ("c", 0, 1, (0, 0)), ("c", 0, 1, (0, 1)), ("x", 1, 5), ("d", 0, 0, (2, 0)), ("d", 0, 1, (2, 0)), ("y", 1, 6),
    ("c", 0, 1, (1, 0)), ("c", 0, 1, (-1, 0)), ("d", 0, 0, (1, 1)), ("d", 0, 0, (-1, 1)), ("x", 1, 6),
    ("d", 0, 1, (-1, 1)), ("c", 0, 0, (-1, 0)), ("d", 0, 1, (1, 1)), ("c", 0, 0, (1, 0)), ("d", 0, 1, (2, 1)),
    ("y", 2, 0), ("d", 0, 0, (2, 1)), ("c", 0, 0, (2, 0)), ("x", 2, 0), ("c", 0, 1, (2, 0)), ("c", 0, 0, (1, 1)),
    ("y", 2, 1), ("c", 0, 0, (-1, 1)), ("c", 0, 1, (-1, 1)), ("x", 2, 1), ("c", 0, 1, (1, 1)), ("c", 0, 1, (2, 1)),
    ("y", 2, 2), ("c", 0, 0, (2, 1)), ("x", 2, 2), ("f", 0, 1), ("f", 0, 0), ("ao", 1, 0, 0), ("ao", 1, 0, 1),
    ("y", 2, 3), ("ao", 1, 0, 2), ("x", 2, 3), ("ao", 1, 0, 3), ("y", 2, 4), ("x", 2, 4), ("af", 1, 0, 0),
    ("af", 1, 0, 1), ("y", 2, 5), ("x", 2, 5), ("ao", 1, 1, 0), ("ao", 1, 1, 1), ("y", 2, 6), ("x", 2, 6),
    ("ao", 1, 1, 2), ("ae", 1, 0), ("gl", 0, 4), ("y", 3, 0), ("gl", 0, 0), ("gl", 0, 2), ("ao", 1, 1, 3),
    ("gl", 0, 1), ("af", 1, 1, 0), ("x", 3, 0), ("hl", 0, 1), ("y", 3, 1), ("hl", 0, 2), ("hl", 0, 4),
    ("gl", 0, 3), ("x", 3, 1), ("af", 1, 1, 1), ("hl", 0, 3), ("hl", 0, 0), ("y", 3, 2), ("d", 1, 0, (0, 0)),
    ("d", 1, 0, (0, 1)), ("x", 3, 2), ("y", 3, 3), ("x", 3, 3), ("d", 1, 0, (1, 0)), ("y", 3, 4),
    ("d", 1, 0, (-1, 0)), ("ae", 1, 1), ("gl", 1, 4), ("x", 3, 4), ("gl", 1, 0), ("c", 1, 0, (0, 0)), ("y", 3, 5),
    ("hl", 1, 0), ("gl", 1, 1), ("hl", 1, 1), ("x", 3, 5), ("c", 1, 0, (0, 1)), ("gl", 1, 2), ("c", 1, 0, (1, 0)),
    ("d", 1, 0, (2, 0)), ("y", 3, 6), ("hl", 1, 2), ("c", 1, 0, (-1, 0)), ("x", 3, 6), ("d", 1, 0, (-1, 1)),
    ("d", 1, 0, (1, 1)), ("hl", 1, 4), ("gl", 1, 3), ("d", 1, 0, (2, 1)), ("hl", 1, 3), ("d", 1, 1, (2, 1)),
    ("d", 1, 1, (2, 0)), ("c", 1, 0, (2, 0)), ("d", 1, 1, (-1, 1)), ("d", 1, 1, (0, 0)), ("d", 1, 1, (1, 0)),
    ("c", 1, 0, (-1, 1)), ("d", 1, 1, (0, 1)), ("d", 1, 1, (-1, 0)), ("d", 1, 1, (1, 1)), ("c", 1, 0, (2, 1)),
    ("c", 1, 0, (1, 1)), ("c", 1, 1, (2, 1)), ("c", 1, 1, (2, 0)), ("c", 1, 1, (-1, 1)), ("c", 1, 1, (0, 0)),
    ("c", 1, 1, (1, 0)), ("c", 1, 1, (0, 1)), ("c", 1, 1, (-1, 0)), ("c", 1, 1, (1, 1)), ("f", 1, 0), ("f", 1, 1),
)
OWN_Y_AT = 4
OWN_X_AT = 5


def kernel(
    tok, mix, en, eg, ev, ed, ep, mg, ln, lg, lv, ld, lp,
    out,
    gbuf, vbuf, dbuf, xbuf, acc, hbuf, tokv, mixv, mixed, gains,
    rs1, rr1, rs2, rr2, keep, br, pbuf,
    loc_sem, w_send, w_recv, p_send, p_recv, ag_send, ag_recv, rs_send, rs1_recv, rs2_recv,
):
    rep = lax.axis_index("rep")
    fs = lax.axis_index("fs")
    z = lax.axis_index("tp")
    c = lax.rem(fs, 2)
    xl = lax.rem(fs // 2, 2)
    y = fs // 4
    x = rep * 2 + xl

    def mod4(v):
        return lax.rem(v + 8, 4)

    def dev(dx=0, dy=0, dz=0, dc=0):
        nx = mod4(x + dx)
        ny = mod4(y + dy)
        nc = c if dc == 0 else 1 - c
        return (nx // 2, (ny * 2 + lax.rem(nx, 2)) * 2 + nc, mod4(z + dz))

    y_dev = {1: dev(dy=1), -1: dev(dy=-1)}
    x_dev = {1: dev(dx=1), -1: dev(dx=-1)}
    z_dev = {1: dev(dz=1), -1: dev(dz=-1)}
    partner = dev(dc=1)
    everyone = [y_dev[1], y_dev[-1], x_dev[1], x_dev[-1], z_dev[1], z_dev[-1], partner]
    zp, zm, zo = mod4(z + 1), mod4(z - 1), mod4(z + 2)

    def blk_of(dy, dp):
        return mod4(y + dy) * 2 + (xl if dp == 0 else 1 - xl)

    blocks = {(dy, dp): blk_of(dy, dp) for dy in (0, 1, -1, 2) for dp in (0, 1)}

    def unit(r, content, core):
        dy, dp, st, s = content
        blk = blocks[(dy, dp)]
        layer = r // 2
        if r % 2 == 0:
            buf = gbuf if st == 0 else vbuf
            row = pl.multiple_of(blk * 256 + core * 128 + s * 64, 64)
            return buf.at[layer, pl.ds(row, 64), :]
        return dbuf.at[layer, blk, core, pl.ds(st * 640 + s * 320, 320), :]

    def unit_id(content):
        dy, dp, st, s = content
        return (((dy % 4) * 2 + dp) * 2 + st) * 2 + s

    def send(src, dst, send_sem, recv_sem, target):
        pltpu.make_async_remote_copy(src, dst, send_sem, recv_sem, device_id=target, device_id_type=MESH).start()

    def await_bytes(ref, sem):
        pltpu.make_async_copy(ref, ref, sem).wait()

    def units(r, n):
        return gbuf.at[0, pl.ds(0, n * (64 if r % 2 == 0 else 32)), :]

    def tee(sign):
        return 0 if sign > 0 else 1

    def y_recv_content(sign, k):
        t = tee(sign)
        return [(-sign, 0, t, 0), (-sign, 0, t, 1), (-sign, 0, 1 - t, 0), (-sign, 0, 1 - t, 1), (2, 0, t, 0),
                (2, 0, t, 1), (2, 1, t, 1)][k]

    def y_send_content(sign, k):
        t = tee(sign)
        return [(0, 0, t, 0), (0, 0, t, 1), (0, 0, 1 - t, 0), (0, 0, 1 - t, 1), (-sign, 0, t, 0),
                (-sign, 0, t, 1), (-sign, 1, t, 1)][k]

    def x_content(sign, k, dp):
        t = tee(sign)
        return [(0, dp, t, 0), (0, dp, t, 1), (-sign, dp, t, 0), (-sign, dp, t, 1), (sign, dp, t, 0),
                (sign, dp, t, 1), (2, dp, t, 0)][k]

    have = set()
    partner_have = set()

    def group_of(r, content):
        dy, dp, st, s = content
        if r % 2 == 0:
            return r * 9 + (0 if dy in (0, -1 if st == 0 else 1) else 1)
        return 2 + (r // 2) * 8 + (dy % 4) * 2 + dp

    def send_y(r, sign, k):
        content = y_send_content(sign, k)
        assert (r, content) in have
        ref = unit(r, content, c)
        send(ref, ref, w_send.at[r], w_recv.at[r, 0, k], y_dev[sign])

    def send_x(r, sign, k):
        content = x_content(sign, k, 0)
        assert (r, content) in have
        ref = unit(r, content, c)
        send(ref, ref, w_send.at[r], w_recv.at[r, 1, k], x_dev[sign])

    def send_partner(r, content):
        ref = unit(r, content, c)
        send(ref, ref, p_send.at[r], p_recv.at[group_of(r, content)], partner)

    every = [(dy, dp, st, s) for dy in (0, 1, -1, 2) for dp in (0, 1) for st in (0, 1) for s in (0, 1)]

    def need(r, group):
        members = [content for content in every if group_of(r, content) == group]
        assert all((r, content) in have for content in members), (r, group)
        if group not in partner_have:
            partner_have.add(group)
            await_bytes(units(r, len(members)), p_recv.at[group])

    def own_y(r):
        wait_local(r)
        for sign in (1, -1):
            for k in (0, 1, 2, 3):
                send_y(r, sign, k)

    def own_x(r):
        for sign in (1, -1):
            send_x(r, sign, 0)
            send_x(r, sign, 1)

    def own_partner(r):
        for st in (0, 1):
            for s in (0, 1):
                send_partner(r, (0, 0, st, s))

    def y_event(r, j):
        await_bytes(units(r, 2), w_recv.at[r, 0, j])
        for sign in (1, -1):
            have.add((r, y_recv_content(sign, j)))
        for sign in (1, -1):
            if j in (2, 3):
                send_x(r, -sign, j + 2)
            elif j < 5:
                send_x(r, sign, j + 2)
            if j < 2:
                send_y(r, sign, j + 4)
        if r < 3 and j == OWN_Y_AT:
            own_y(r + 1)
        if r < 3 and j == OWN_X_AT:
            own_x(r + 1)
        for sign in (1, -1):
            send_partner(r, y_recv_content(sign, j))
        if r < 3 and j == OWN_Y_AT:
            own_partner(r + 1)

    def x_event(r, j):
        await_bytes(units(r, 2), w_recv.at[r, 1, j])
        for sign in (1, -1):
            have.add((r, x_content(sign, j, 1)))
        for sign in (1, -1):
            if j == 3:
                send_y(r, sign, 6)
            send_partner(r, x_content(sign, j, 1))

    own = pl.multiple_of(blocks[(0, 0)] * 256 + c * 128, 128)
    weights = {
        0: [(eg, gbuf.at[0, pl.ds(own, 128), :]), (ev, vbuf.at[0, pl.ds(own, 128), :])],
        1: [(ed, dbuf.at[0, blocks[(0, 0)], c])],
        2: [(lg, gbuf.at[1, pl.ds(own, 128), :]), (lv, vbuf.at[1, pl.ds(own, 128), :])],
        3: [(ld, dbuf.at[1, blocks[(0, 0)], c])],
    }
    norms = [(g, gains.at[i]) for i, g in enumerate((en, ep, mg, ln, lp))]
    for i, pairs in enumerate((weights[0], [(tok, tokv)], norms, weights[1], weights[2], weights[3], [(mix, mixv)])):
        for src, dst in pairs:
            pltpu.make_async_copy(src, dst, loc_sem.at[i]).start()

    def wait_local(r):
        await_bytes(units(r, 4), loc_sem.at[(0, 3, 4, 5)[r]])
        for st in (0, 1):
            for s in (0, 1):
                have.add((r, (0, 0, st, s)))

    barrier = pltpu.get_barrier_semaphore()
    for other in everyone:
        pl.semaphore_signal(barrier, inc=1, device_id=other, device_id_type=MESH)
    pl.semaphore_wait(barrier, len(everyone))

    def x_rows(layer, h, zz, u, n=16):
        row = pl.multiple_of(h * 256 + zz * 64 + u * 16, 16)
        return xbuf.at[layer, pl.ds(row, n), :]

    def ag_own(layer, h, u):
        for sign in (1, -1):
            v = u if sign > 0 else (u + 2) % 4
            ref = x_rows(layer, h, z, v)
            send(ref, ref, ag_send.at[layer], ag_recv.at[layer, h, min(u, 2)], z_dev[sign])

    def ag_forward(layer, h, u):
        await_bytes(xbuf.at[0, pl.ds(0, 32), :], ag_recv.at[layer, h, u])
        for sign in (1, -1):
            v = u if sign > 0 else u + 2
            ref = x_rows(layer, h, zm if sign > 0 else zp, v)
            send(ref, ref, ag_send.at[layer], ag_recv.at[layer, h, 2], z_dev[sign])

    def ag_finish(layer, h):
        await_bytes(xbuf.at[0, pl.ds(0, 128), :], ag_recv.at[layer, h, 2])

    def rms(v, gain):
        return v * lax.rsqrt(jnp.mean(v * v, axis=-1, keepdims=True) + EPS) * gain

    def early_norm(h):
        def body(i, carry):
            rows = pl.ds(pl.multiple_of(h * 64 + i * 16, 16), 16)
            v = rms(tokv[rows, :].astype(F32), gains[0])
            x_rows(0, h, z, i)[...] = v.astype(BF)
            return carry

        lax.fori_loop(0, 4, body, 0)

    def dot_rows(st, rows, dy, cols, layer=0):
        base = pl.multiple_of(mod4(y + dy) * 512, 512)
        w = gbuf if st == 0 else vbuf
        return jnp.dot(xbuf[layer, rows, pl.ds(base, 512)], w[layer, pl.ds(base, 512), cols], preferred_element_type=F32)

    whole = slice(0, 512)

    def tile(n):
        return slice(n * 256, n * 256 + 256)

    def gemm1(st, n):
        need(0, 0)
        acc[st, :, tile(n)] = dot_rows(st, whole, 0, tile(n)) + dot_rows(st, whole, -1 if st == 0 else 1, tile(n))

    def silu_mul(g, v):
        return (g * (1.0 / (1.0 + jnp.exp(-g))) * v).astype(BF)

    def gemm1_later(h, n):
        need(2, 18)
        rows = slice(h * 256, h * 256 + 256)
        for st in (0, 1):
            acc[st, rows, tile(n)] = dot_rows(st, rows, 0, tile(n), 1) + dot_rows(st, rows, -1 if st == 0 else 1, tile(n), 1)

    def hidden(layer, h, n):
        need(2 * layer, 18 * layer + 1)
        rows = slice(h * 256, h * 256 + 256)
        g = acc[0, rows, tile(n)] + dot_rows(0, rows, 2, tile(n), layer) + dot_rows(0, rows, 1, tile(n), layer)
        v = acc[1, rows, tile(n)] + dot_rows(1, rows, 2, tile(n), layer) + dot_rows(1, rows, -1, tile(n), layer)
        hbuf[rows, tile(n)] = silu_mul(g, v)

    def hidden_early(h, n):
        hidden(0, h, n)

    def hidden_later(h, n):
        hidden(1, h, n)

    chunks = ((0, 0), (0, 1), (-1, 0), (1, 0), (2, 0), (-1, 1), (1, 1), (2, 1))

    def down(layer, h, chunk):
        r = 2 * layer + 1
        dy, dp = chunk
        need(r, group_of(r, (dy, dp, 0, 0)))
        j = chunks.index(chunk)
        blk = blocks[chunk]
        w = jnp.concatenate([dbuf[layer, blk, 0], dbuf[layer, blk, 1]], axis=1)
        pbuf[...] = jnp.dot(hbuf[h * 256 : h * 256 + 256, :], w, preferred_element_type=F32)

        def rows(zz, half):
            return pl.ds(pl.multiple_of(zz * 64 + half * 32, 32), 32)

        rs1[layer, h, j, 0, 0:32, :] = pbuf[rows(zo, 0), :].astype(BF)
        rs1[layer, h, j, 0, 32:64, :] = pbuf[rows(zp, 1), :].astype(BF)
        rs1[layer, h, j, 1, 0:32, :] = pbuf[rows(zm, 0), :].astype(BF)
        rs1[layer, h, j, 1, 32:64, :] = pbuf[rows(zo, 1), :].astype(BF)
        keep[h, j, 0] = pbuf[rows(zp, 0), :]
        keep[h, j, 1] = pbuf[rows(zm, 1), :]
        cols = pl.ds(pl.multiple_of(blk * 256, 256), 256)
        br[h * 64 : h * 64 + 64, cols] = pbuf[pl.ds(pl.multiple_of(z * 64, 64), 64), :]
        for sign in (1, -1):
            lane = tee(sign)
            send(rs1.at[layer, h, j, lane], rr1.at[layer, h, j, lane], rs_send.at[0], rs1_recv.at[layer, h, j], z_dev[sign])

    def combine(layer, h, chunk):
        j = chunks.index(chunk)
        await_bytes(rr1.at[layer, h, j], rs1_recv.at[layer, h, j])
        for sign in (1, -1):
            lane = tee(sign)
            half = slice(0, 32) if sign > 0 else slice(32, 64)
            rs2[layer, h, j, lane] = (rr1[layer, h, j, lane, half, :].astype(F32) + keep[h, j, lane]).astype(BF)
        for sign in (1, -1):
            lane = tee(sign)
            send(rs2.at[layer, h, j, lane], rr2.at[layer, h, j, lane], rs_send.at[1], rs2_recv.at[layer, h], z_dev[sign])

    def finish(layer, h):
        await_bytes(rr2.at[layer, h], rs2_recv.at[layer, h])
        a = slice(h * 64, h * 64 + 32)
        b = slice(h * 64 + 32, h * 64 + 64)
        for j, chunk in enumerate(chunks):
            cols = pl.ds(pl.multiple_of(blocks[chunk] * 256, 256), 256)
            br[a, cols] += rr2[layer, h, j, 0].astype(F32) + rr1[layer, h, j, 1, 0:32, :].astype(F32)
            br[b, cols] += rr2[layer, h, j, 1].astype(F32) + rr1[layer, h, j, 0, 32:64, :].astype(F32)

        def body(i, carry):
            rows = pl.ds(pl.multiple_of(h * 64 + i * 16, 16), 16)
            branch = br[rows, :]
            if layer == 0:
                m = tokv[rows, :].astype(F32) + 0.5 * rms(branch, gains[1]) + rms(mixv[rows, :].astype(F32), gains[2])
                m = m.astype(BF)
                mixed[rows, :] = m
                x_rows(1, h, z, i)[...] = rms(m.astype(F32), gains[3]).astype(BF)
            else:
                out[rows, :] = (mixed[rows, :].astype(F32) + 0.5 * rms(branch, gains[4])).astype(BF)
            return carry

        lax.fori_loop(0, 4, body, 0)

    wait_local(0)
    for sign in (1, -1):
        send_y(0, sign, 0)
        send_x(0, sign, 0)
        send_y(0, sign, 1)
        send_x(0, sign, 1)
        send_y(0, sign, 2)
        send_y(0, sign, 3)
    own_partner(0)
    await_bytes(tokv, loc_sem.at[1])
    await_bytes(gains, loc_sem.at[2])
    await_bytes(mixv, loc_sem.at[6])
    tasks = dict(
        y=y_event, x=x_event, en=early_norm, ao=ag_own, af=ag_forward, ae=ag_finish, g1=gemm1, gl=gemm1_later,
        he=hidden_early, hl=hidden_later, d=down, c=combine, f=finish,
    )
    for name, *args in ORDER:
        fn = tasks[name]
        fn(*args)

    for r in range(4):
        await_bytes(units(r, 28), w_send.at[r])
        await_bytes(units(r, 32), p_send.at[r])
    for layer in (0, 1):
        await_bytes(xbuf.at[0, pl.ds(0, 384), :], ag_send.at[layer])
    await_bytes(rs1, rs_send.at[0])
    await_bytes(rs2, rs_send.at[1])


def on_device(tokens, mixer_output, en, eg, ev, ed, ep, mg, ln, lg, lv, ld, lp):
    gains = [g.reshape(1, 2048) for g in (en, ep, mg, ln, lp)]
    en, ep, mg, ln, lp = gains
    return pl.pallas_call(
        kernel,
        out_shape=jax.ShapeDtypeStruct((128, 2048), BF),
        in_specs=[pl.BlockSpec(memory_space=pl.ANY)] * 13,
        out_specs=pl.BlockSpec(memory_space=pltpu.VMEM),
        scratch_shapes=[
            pltpu.VMEM((2, 2048, 1280), BF),
            pltpu.VMEM((2, 2048, 1280), BF),
            pltpu.VMEM((2, 8, 2, 1280, 128), BF),
            pltpu.VMEM((2, 512, 2048), BF),
            pltpu.VMEM((2, 512, 1280), F32),
            pltpu.VMEM((512, 1280), BF),
            pltpu.VMEM((128, 2048), BF),
            pltpu.VMEM((128, 2048), BF),
            pltpu.VMEM((128, 2048), BF),
            pltpu.VMEM((5, 1, 2048), F32),
            pltpu.VMEM((2, 2, 8, 2, 64, 256), BF),
            pltpu.VMEM((2, 2, 8, 2, 64, 256), BF),
            pltpu.VMEM((2, 2, 8, 2, 32, 256), BF),
            pltpu.VMEM((2, 2, 8, 2, 32, 256), BF),
            pltpu.VMEM((2, 8, 2, 32, 256), F32),
            pltpu.VMEM((128, 2048), F32),
            pltpu.VMEM((256, 256), F32),
            pltpu.SemaphoreType.DMA((7,)),
            pltpu.SemaphoreType.DMA((4,)),
            pltpu.SemaphoreType.DMA((4, 2, 7)),
            pltpu.SemaphoreType.DMA((4,)),
            pltpu.SemaphoreType.DMA((20,)),
            pltpu.SemaphoreType.DMA((2,)),
            pltpu.SemaphoreType.DMA((2, 2, 3)),
            pltpu.SemaphoreType.DMA((2,)),
            pltpu.SemaphoreType.DMA((2, 2, 8)),
            pltpu.SemaphoreType.DMA((2, 2)),
        ],
        compiler_params=pltpu.CompilerParams(
            collective_id=0, has_side_effects=True, vmem_limit_bytes=67_000_000
        ),
    )(tokens, mixer_output, en, eg, ev, ed, ep, mg, ln, lg, lv, ld, lp)


def solution(mesh):
    placed = (
        P(("rep", "fs", "tp"), None),
        P(("rep", "fs", "tp"), None),
        P(),
        P("fs", "tp"),
        P("fs", "tp"),
        P("tp", "fs"),
        P(),
        P(),
        P(),
        P("fs", "tp"),
        P("fs", "tp"),
        P("tp", "fs"),
        P(),
    )
    return jax.shard_map(
        on_device,
        mesh=mesh,
        in_specs=placed,
        out_specs=P(("rep", "fs", "tp"), None),
        check_vma=False,
    )
```

```python
import functools

import jax
import jax.numpy as jnp
from jax import lax
from jax.experimental import pallas as pl
from jax.experimental.pallas import tpu as pltpu
from jax.sharding import PartitionSpec as P

MESH = pl.DeviceIdType.MESH
EPS = 1e-06
BF = jnp.bfloat16
F32 = jnp.float32


ORDER = (
    ("en", 0), ("en", 1), ("ao", 0, 1, 0), ("ao", 0, 0, 0), ("ao", 0, 0, 1), ("ao", 0, 0, 2), ("ao", 0, 0, 3),
    ("ao", 0, 1, 1), ("af", 0, 1, 0), ("y", 0, 0), ("af", 0, 0, 0), ("af", 0, 0, 1), ("x", 0, 1), ("y", 0, 1),
    ("ao", 0, 1, 2), ("ao", 0, 1, 3), ("af", 0, 1, 1), ("y", 0, 2), ("ae", 0, 0), ("x", 0, 3), ("y", 0, 3),
    ("y", 0, 4), ("ae", 0, 1), ("g1", 0), ("g1", 1), ("x", 0, 5), ("y", 0, 5), ("g2", 1), ("y", 0, 6), ("x", 0, 6),
    ("g2", 0), ("y", 1, 0), ("x", 1, 1), ("he", 1), ("y", 1, 1), ("he", 0), ("y", 1, 2), ("d", 0, 0, 0),
    ("d", 0, 0, 1), ("d", 0, 1, 1), ("y", 1, 3), ("d", 0, 1, 0), ("d", 0, 1, 2), ("x", 1, 3), ("y", 1, 4),
    ("d", 0, 0, 2), ("c", 0, 0, (0, 0)), ("y", 1, 5), ("c", 0, 0, (0, 1)), ("c", 0, 1, (0, 1)), ("d", 0, 0, 3),
    ("c", 0, 1, (0, 0)), ("x", 1, 5), ("d", 0, 1, 3), ("c", 0, 1, (-1, 0)), ("c", 0, 1, (1, 0)), ("y", 1, 6),
    ("c", 0, 0, (-1, 0)), ("x", 1, 6), ("d", 0, 0, 4), ("c", 0, 0, (1, 0)), ("d", 0, 0, 5), ("d", 0, 1, 4),
    ("c", 0, 0, (2, 0)), ("y", 2, 0), ("c", 0, 1, (2, 0)), ("d", 0, 1, 5), ("c", 0, 0, (-1, 1)),
    ("c", 0, 0, (1, 1)), ("y", 2, 1), ("c", 0, 0, (2, 1)), ("x", 2, 1), ("c", 0, 1, (-1, 1)), ("c", 0, 1, (1, 1)),
    ("c", 0, 1, (2, 1)), ("y", 2, 2), ("f", 0, 0), ("ao", 1, 0, 0), ("ao", 1, 0, 1), ("ao", 1, 0, 2),
    ("ao", 1, 0, 3), ("f", 0, 1), ("y", 2, 3), ("x", 2, 3), ("ao", 1, 1, 0), ("af", 1, 0, 0), ("y", 2, 4),
    ("af", 1, 0, 1), ("ao", 1, 1, 1), ("y", 2, 5), ("x", 2, 5), ("ao", 1, 1, 2), ("af", 1, 1, 0), ("ao", 1, 1, 3),
    ("y", 2, 6), ("ae", 1, 0), ("gl", 0), ("x", 2, 6), ("y", 3, 0), ("af", 1, 1, 1), ("y", 3, 1), ("x", 3, 1),
    ("hl", 0), ("d", 1, 0, 0), ("y", 3, 2), ("d", 1, 0, 1), ("y", 3, 3), ("ae", 1, 1), ("gl", 1), ("d", 1, 0, 2),
    ("x", 3, 3), ("y", 3, 4), ("c", 1, 0, (0, 0)), ("hl", 1), ("d", 1, 1, 0), ("d", 1, 1, 1), ("d", 1, 1, 2),
    ("c", 1, 0, (0, 1)), ("y", 3, 5), ("x", 3, 5), ("c", 1, 0, (-1, 0)), ("c", 1, 0, (1, 0)), ("d", 1, 1, 3),
    ("d", 1, 0, 3), ("d", 1, 0, 4), ("c", 1, 1, (0, 0)), ("x", 3, 6), ("y", 3, 6), ("c", 1, 1, (0, 1)),
    ("c", 1, 1, (-1, 0)), ("c", 1, 1, (1, 0)), ("d", 1, 0, 5), ("d", 1, 1, 5), ("c", 1, 1, (2, 0)), ("d", 1, 1, 4),
    ("c", 1, 0, (2, 0)), ("c", 1, 0, (-1, 1)), ("c", 1, 0, (1, 1)), ("c", 1, 0, (2, 1)), ("c", 1, 1, (2, 1)),
    ("c", 1, 1, (-1, 1)), ("c", 1, 1, (1, 1)), ("f", 1, 0), ("f", 1, 1),
)
OWN_Y_AT = 4
OWN_X_AT = 4


def kernel(
    tok, mix, en, eg, ev, ed, ep, mg, ln, lg, lv, ld, lp,
    out,
    gbuf, vbuf, dbuf, xbuf, acc, hbuf, tokv, mixv, mixed, gains,
    rs1, rr1, rs2, rr2, keep, br, pbuf,
    loc_sem, w_send, w_recv, p_send, p_recv, ag_send, ag_recv, rs_send, rs1_recv, rs2_recv,
):
    rep = lax.axis_index("rep")
    fs = lax.axis_index("fs")
    z = lax.axis_index("tp")
    c = lax.rem(fs, 2)
    xl = lax.rem(fs // 2, 2)
    y = fs // 4
    x = rep * 2 + xl

    def mod4(v):
        return lax.rem(v + 8, 4)

    def dev(dx=0, dy=0, dz=0, dc=0):
        nx = mod4(x + dx)
        ny = mod4(y + dy)
        nc = c if dc == 0 else 1 - c
        return (nx // 2, (ny * 2 + lax.rem(nx, 2)) * 2 + nc, mod4(z + dz))

    y_dev = {1: dev(dy=1), -1: dev(dy=-1)}
    x_dev = {1: dev(dx=1), -1: dev(dx=-1)}
    z_dev = {1: dev(dz=1), -1: dev(dz=-1)}
    partner = dev(dc=1)
    everyone = [y_dev[1], y_dev[-1], x_dev[1], x_dev[-1], z_dev[1], z_dev[-1], partner]
    zp, zm, zo = mod4(z + 1), mod4(z - 1), mod4(z + 2)

    def blk_of(dy, dp):
        return mod4(y + dy) * 2 + (xl if dp == 0 else 1 - xl)

    blocks = {(dy, dp): blk_of(dy, dp) for dy in (0, 1, -1, 2) for dp in (0, 1)}

    def unit(r, content, core):
        dy, dp, st, s = content
        blk = blocks[(dy, dp)]
        layer = r // 2
        if r % 2 == 0:
            buf = gbuf if st == 0 else vbuf
            row = pl.multiple_of(blk * 256 + core * 128 + s * 64, 64)
            return buf.at[layer, pl.ds(row, 64), :]
        return dbuf.at[layer, blk, core, pl.ds(st * 640 + s * 320, 320), :]

    def unit_id(content):
        dy, dp, st, s = content
        return (((dy % 4) * 2 + dp) * 2 + st) * 2 + s

    def send(src, dst, send_sem, recv_sem, target):
        pltpu.make_async_remote_copy(src, dst, send_sem, recv_sem, device_id=target, device_id_type=MESH).start()

    def await_bytes(ref, sem):
        pltpu.make_async_copy(ref, ref, sem).wait()

    def units(r, n):
        return gbuf.at[0, pl.ds(0, n * (64 if r % 2 == 0 else 32)), :]

    def tee(sign):
        return 0 if sign > 0 else 1

    def y_recv_content(sign, k):
        t = tee(sign)
        return [(-sign, 0, t, 0), (-sign, 0, t, 1), (-sign, 0, 1 - t, 0), (-sign, 0, 1 - t, 1), (2, 0, t, 0),
                (2, 0, t, 1), (2, 1, t, 1)][k]

    def y_send_content(sign, k):
        t = tee(sign)
        return [(0, 0, t, 0), (0, 0, t, 1), (0, 0, 1 - t, 0), (0, 0, 1 - t, 1), (-sign, 0, t, 0),
                (-sign, 0, t, 1), (-sign, 1, t, 1)][k]

    def x_content(sign, k, dp):
        t = tee(sign)
        return [(0, dp, t, 0), (0, dp, t, 1), (-sign, dp, t, 0), (-sign, dp, t, 1), (sign, dp, t, 0),
                (sign, dp, t, 1), (2, dp, t, 0)][k]

    have = set()
    partner_have = set()

    def group_of(r, content):
        dy, dp, st, s = content
        if r % 2 == 0:
            return (0 if r == 0 else 19) + (0 if dy in (0, -1 if st == 0 else 1) else 2 if dy == 2 else 1)
        return 3 + (r // 2) * 8 + (dy % 4) * 2 + dp

    def send_y(r, sign, k):
        content = y_send_content(sign, k)
        assert (r, content) in have
        ref = unit(r, content, c)
        send(ref, ref, w_send.at[r], w_recv.at[r, k], y_dev[sign])

    def send_x(r, sign, k):
        content = x_content(sign, k, 0)
        assert (r, content) in have
        ref = unit(r, content, c)
        send(ref, ref, w_send.at[r], w_recv.at[r, 7 + k // 2], x_dev[sign])

    def send_partner(r, content):
        ref = unit(r, content, c)
        send(ref, ref, p_send.at[r], p_recv.at[group_of(r, content)], partner)

    every = [(dy, dp, st, s) for dy in (0, 1, -1, 2) for dp in (0, 1) for st in (0, 1) for s in (0, 1)]

    def need(r, group):
        members = [content for content in every if group_of(r, content) == group]
        assert all((r, content) in have for content in members), (r, group)
        if group not in partner_have:
            partner_have.add(group)
            await_bytes(units(r, len(members)), p_recv.at[group])

    def own_y(r):
        wait_local(r)
        for sign in (1, -1):
            for k in (0, 1, 2, 3):
                send_y(r, sign, k)

    def own_x(r):
        for sign in (1, -1):
            send_x(r, sign, 0)
            send_x(r, sign, 1)

    def own_partner(r):
        for st in (0, 1):
            for s in (0, 1):
                send_partner(r, (0, 0, st, s))

    def y_event(r, j):
        await_bytes(units(r, 2), w_recv.at[r, j])
        for sign in (1, -1):
            have.add((r, y_recv_content(sign, j)))
        for sign in (1, -1):
            if j in (2, 3):
                send_x(r, -sign, j + 2)
            elif j < 5:
                send_x(r, sign, j + 2)
            if j < 2:
                send_y(r, sign, j + 4)
        if r < 3 and j == OWN_Y_AT:
            own_y(r + 1)
        if r < 3 and j == OWN_X_AT:
            own_x(r + 1)
        for sign in (1, -1):
            send_partner(r, y_recv_content(sign, j))
        if r < 3 and j == OWN_Y_AT:
            own_partner(r + 1)

    def x_event(r, j):
        ks = (6,) if j == 6 else (j - 1, j)
        await_bytes(units(r, 2 * len(ks)), w_recv.at[r, 7 + ks[0] // 2])
        for sign in (1, -1):
            for k in ks:
                have.add((r, x_content(sign, k, 1)))
            if j == 3:
                send_y(r, sign, 6)
        for k in ks:
            for sign in (1, -1):
                send_partner(r, x_content(sign, k, 1))

    own = pl.multiple_of(blocks[(0, 0)] * 256 + c * 128, 128)
    weights = {
        0: [(eg, gbuf.at[0, pl.ds(own, 128), :]), (ev, vbuf.at[0, pl.ds(own, 128), :])],
        1: [(ed, dbuf.at[0, blocks[(0, 0)], c])],
        2: [(lg, gbuf.at[1, pl.ds(own, 128), :]), (lv, vbuf.at[1, pl.ds(own, 128), :])],
        3: [(ld, dbuf.at[1, blocks[(0, 0)], c])],
    }
    norms = [(g, gains.at[i]) for i, g in enumerate((en, ep, mg, ln, lp))]
    for i, pairs in enumerate((weights[0], [(tok, tokv)], norms, weights[1], weights[2], weights[3], [(mix, mixv)])):
        for src, dst in pairs:
            pltpu.make_async_copy(src, dst, loc_sem.at[i]).start()

    def wait_local(r):
        await_bytes(units(r, 4), loc_sem.at[(0, 3, 4, 5)[r]])
        for st in (0, 1):
            for s in (0, 1):
                have.add((r, (0, 0, st, s)))

    barrier = pltpu.get_barrier_semaphore()
    for other in everyone:
        pl.semaphore_signal(barrier, inc=1, device_id=other, device_id_type=MESH)
    pl.semaphore_wait(barrier, len(everyone))

    def x_rows(layer, h, zz, u, n=16):
        row = pl.multiple_of(h * 256 + zz * 64 + u * 16, 16)
        return xbuf.at[layer, pl.ds(row, n), :]

    def ag_own(layer, h, u):
        for sign in (1, -1):
            v = u if sign > 0 else (u + 2) % 4
            ref = x_rows(layer, h, z, v)
            send(ref, ref, ag_send.at[layer], ag_recv.at[h, min(u, 2)], z_dev[sign])

    def ag_forward(layer, h, u):
        await_bytes(xbuf.at[0, pl.ds(0, 32), :], ag_recv.at[h, u])
        for sign in (1, -1):
            v = u if sign > 0 else u + 2
            ref = x_rows(layer, h, zm if sign > 0 else zp, v)
            send(ref, ref, ag_send.at[layer], ag_recv.at[h, 2], z_dev[sign])

    def ag_finish(layer, h):
        await_bytes(xbuf.at[0, pl.ds(0, 128), :], ag_recv.at[h, 2])

    def rms(v, gain):
        return v * lax.rsqrt(jnp.mean(v * v, axis=-1, keepdims=True) + EPS) * gain

    def early_norm(h):
        for i in range(4):
            v = rms(tokv[h * 64 + i * 16 : h * 64 + i * 16 + 16, :].astype(F32), gains[0])
            x_rows(0, h, z, i)[...] = v.astype(BF)

    def dot_rows(st, rows, dy, cols, layer=0):
        base = pl.multiple_of(mod4(y + dy) * 512, 512)
        w = gbuf if st == 0 else vbuf
        return jnp.dot(xbuf[layer, rows, pl.ds(base, 512)], w[layer, pl.ds(base, 512), cols], preferred_element_type=F32)

    whole = slice(0, 512)

    def tile(n):
        return slice(n * 256, n * 256 + 256)

    def gemm1(st):
        need(0, 0)
        for n in range(5):
            acc[st, :, tile(n)] = dot_rows(st, whole, 0, tile(n)) + dot_rows(st, whole, -1 if st == 0 else 1, tile(n))

    def silu_mul(g, v):
        return (g * (1.0 / (1.0 + jnp.exp(-g))) * v).astype(BF)

    def gemm2(st):
        need(0, 1)
        for n in range(5):
            acc[st, :, tile(n)] += dot_rows(st, whole, 1 if st == 0 else -1, tile(n))

    def gemm1_later(h):
        need(2, 19)
        need(2, 20)
        rows = slice(h * 256, h * 256 + 256)
        for n in range(5):
            for st in (0, 1):
                parts = [dot_rows(st, rows, dy, tile(n), 1) for dy in (0, -1, 1)]
                acc[st, rows, tile(n)] = parts[0] + parts[1] + parts[2]

    def hidden(layer, h):
        need(2 * layer, 19 * layer + 2)
        rows = slice(h * 256, h * 256 + 256)
        for n in range(5):
            g = acc[0, rows, tile(n)] + dot_rows(0, rows, 2, tile(n), layer)
            v = acc[1, rows, tile(n)] + dot_rows(1, rows, 2, tile(n), layer)
            hbuf[rows, tile(n)] = silu_mul(g, v)

    def hidden_early(h):
        hidden(0, h)

    def hidden_later(h):
        hidden(1, h)

    chunks = ((0, 0), (0, 1), (-1, 0), (1, 0), (2, 0), (-1, 1), (1, 1), (2, 1))

    groups = (((0, 0),), ((0, 1),), ((-1, 0), (1, 0)), ((2, 0),), ((-1, 1), (1, 1)), ((2, 1),))

    def down(layer, h, i):
        r = 2 * layer + 1

        def rows(zz, half):
            return pl.ds(pl.multiple_of(zz * 64 + half * 32, 32), 32)

        for dy, dp in groups[i]:
            need(r, group_of(r, (dy, dp, 0, 0)))
        for k, chunk in enumerate(groups[i]):
            blk = blocks[chunk]
            w = jnp.concatenate([dbuf[layer, blk, 0], dbuf[layer, blk, 1]], axis=1)
            pbuf[k] = jnp.dot(hbuf[h * 256 : h * 256 + 256, :], w, preferred_element_type=F32)
        for k, chunk in enumerate(groups[i]):
            j = chunks.index(chunk)
            rs1[layer, h, j, 0, 0:32, :] = pbuf[k, rows(zo, 0), :].astype(BF)
            rs1[layer, h, j, 0, 32:64, :] = pbuf[k, rows(zp, 1), :].astype(BF)
            rs1[layer, h, j, 1, 0:32, :] = pbuf[k, rows(zm, 0), :].astype(BF)
            rs1[layer, h, j, 1, 32:64, :] = pbuf[k, rows(zo, 1), :].astype(BF)
            keep[h, j, 0] = pbuf[k, rows(zp, 0), :]
            keep[h, j, 1] = pbuf[k, rows(zm, 1), :]
            cols = pl.ds(pl.multiple_of(blocks[chunk] * 256, 256), 256)
            br[h * 64 : h * 64 + 64, cols] = pbuf[k, pl.ds(pl.multiple_of(z * 64, 64), 64), :]
        for chunk in groups[i]:
            j = chunks.index(chunk)
            for sign in (1, -1):
                lane = tee(sign)
                send(rs1.at[layer, h, j, lane], rr1.at[layer, h, j, lane], rs_send.at[0], rs1_recv.at[h, j], z_dev[sign])

    def combine(layer, h, chunk):
        j = chunks.index(chunk)
        await_bytes(rr1.at[layer, h, j], rs1_recv.at[h, j])
        for sign in (1, -1):
            lane = tee(sign)
            half = slice(0, 32) if sign > 0 else slice(32, 64)
            rs2[layer, h, j, lane] = (rr1[layer, h, j, lane, half, :].astype(F32) + keep[h, j, lane]).astype(BF)
        for sign in (1, -1):
            lane = tee(sign)
            send(rs2.at[layer, h, j, lane], rr2.at[layer, h, j, lane], rs_send.at[1], rs2_recv.at[h], z_dev[sign])
        cols = pl.ds(pl.multiple_of(blocks[chunk] * 256, 256), 256)
        br[h * 64 : h * 64 + 32, cols] += rr1[layer, h, j, 1, 0:32, :].astype(F32)
        br[h * 64 + 32 : h * 64 + 64, cols] += rr1[layer, h, j, 0, 32:64, :].astype(F32)

    def finish(layer, h):
        await_bytes(rr2.at[layer, h], rs2_recv.at[h])
        for j, chunk in enumerate(chunks):
            cols = pl.ds(pl.multiple_of(blocks[chunk] * 256, 256), 256)
            br[h * 64 : h * 64 + 32, cols] += rr2[layer, h, j, 0].astype(F32)
            br[h * 64 + 32 : h * 64 + 64, cols] += rr2[layer, h, j, 1].astype(F32)
        for i in range(4):
            rows = slice(h * 64 + i * 16, h * 64 + i * 16 + 16)
            branch = br[rows, :]
            if layer == 0:
                m = tokv[rows, :].astype(F32) + 0.5 * rms(branch, gains[1]) + rms(mixv[rows, :].astype(F32), gains[2])
                m = m.astype(BF)
                mixed[rows, :] = m
                x_rows(1, h, z, i)[...] = rms(m.astype(F32), gains[3]).astype(BF)
            else:
                out[rows, :] = (mixed[rows, :].astype(F32) + 0.5 * rms(branch, gains[4])).astype(BF)

    wait_local(0)
    for sign in (1, -1):
        send_y(0, sign, 0)
        send_x(0, sign, 0)
        send_y(0, sign, 1)
        send_x(0, sign, 1)
        send_y(0, sign, 2)
        send_y(0, sign, 3)
    own_partner(0)
    await_bytes(tokv, loc_sem.at[1])
    await_bytes(gains, loc_sem.at[2])
    await_bytes(mixv, loc_sem.at[6])
    tasks = dict(
        y=y_event, x=x_event, en=early_norm, ao=ag_own, af=ag_forward, ae=ag_finish, g1=gemm1, g2=gemm2, gl=gemm1_later,
        he=hidden_early, hl=hidden_later, d=down, c=combine, f=finish,
    )
    for name, *args in ORDER:
        fn = tasks[name]
        fn(*args)

    for r in range(4):
        await_bytes(units(r, 28), w_send.at[r])
        await_bytes(units(r, 32), p_send.at[r])
    for layer in (0, 1):
        await_bytes(xbuf.at[0, pl.ds(0, 384), :], ag_send.at[layer])
    await_bytes(rs1, rs_send.at[0])
    await_bytes(rs2, rs_send.at[1])


def on_device(tokens, mixer_output, en, eg, ev, ed, ep, mg, ln, lg, lv, ld, lp):
    gains = [g.reshape(1, 2048) for g in (en, ep, mg, ln, lp)]
    en, ep, mg, ln, lp = gains
    return pl.pallas_call(
        kernel,
        out_shape=jax.ShapeDtypeStruct((128, 2048), BF),
        in_specs=[pl.BlockSpec(memory_space=pl.ANY)] * 13,
        out_specs=pl.BlockSpec(memory_space=pltpu.VMEM),
        scratch_shapes=[
            pltpu.VMEM((2, 2048, 1280), BF),
            pltpu.VMEM((2, 2048, 1280), BF),
            pltpu.VMEM((2, 8, 2, 1280, 128), BF),
            pltpu.VMEM((2, 512, 2048), BF),
            pltpu.VMEM((2, 512, 1280), F32),
            pltpu.VMEM((512, 1280), BF),
            pltpu.VMEM((128, 2048), BF),
            pltpu.VMEM((128, 2048), BF),
            pltpu.VMEM((128, 2048), BF),
            pltpu.VMEM((5, 1, 2048), F32),
            pltpu.VMEM((2, 2, 8, 2, 64, 256), BF),
            pltpu.VMEM((2, 2, 8, 2, 64, 256), BF),
            pltpu.VMEM((2, 2, 8, 2, 32, 256), BF),
            pltpu.VMEM((2, 2, 8, 2, 32, 256), BF),
            pltpu.VMEM((2, 8, 2, 32, 256), F32),
            pltpu.VMEM((128, 2048), F32),
            pltpu.VMEM((2, 256, 256), F32),
            pltpu.SemaphoreType.DMA((7,)),
            pltpu.SemaphoreType.DMA((4,)),
            pltpu.SemaphoreType.DMA((4, 11)),
            pltpu.SemaphoreType.DMA((4,)),
            pltpu.SemaphoreType.DMA((22,)),
            pltpu.SemaphoreType.DMA((2,)),
            pltpu.SemaphoreType.DMA((2, 3)),
            pltpu.SemaphoreType.DMA((2,)),
            pltpu.SemaphoreType.DMA((2, 8)),
            pltpu.SemaphoreType.DMA((2,)),
        ],
        compiler_params=pltpu.CompilerParams(
            collective_id=0, has_side_effects=True, vmem_limit_bytes=67_000_000
        ),
    )(tokens, mixer_output, en, eg, ev, ed, ep, mg, ln, lg, lv, ld, lp)


def solution(mesh):
    placed = (
        P(("rep", "fs", "tp"), None),
        P(("rep", "fs", "tp"), None),
        P(),
        P("fs", "tp"),
        P("fs", "tp"),
        P("tp", "fs"),
        P(),
        P(),
        P(),
        P("fs", "tp"),
        P("fs", "tp"),
        P("tp", "fs"),
        P(),
    )
    return jax.shard_map(
        on_device,
        mesh=mesh,
        in_specs=placed,
        out_specs=P(("rep", "fs", "tp"), None),
        check_vma=False,
    )
```

```python
import functools

import jax
import jax.numpy as jnp
from jax import lax
from jax.experimental import pallas as pl
from jax.experimental.pallas import tpu as pltpu
from jax.sharding import PartitionSpec as P

MESH = pl.DeviceIdType.MESH
EPS = 1e-06
BF = jnp.bfloat16
F32 = jnp.float32


ORDER = (
    ("en", 0), ("en", 1), ("ao", 0, 1, 0), ("ao", 0, 0, 0), ("y", 0, 0), ("ao", 0, 1, 1), ("ao", 0, 0, 1),
    ("x", 0, 1), ("ao", 0, 0, 2), ("af", 0, 1, 0), ("af", 0, 0, 0), ("y", 0, 1), ("y", 0, 2), ("ao", 0, 0, 3),
    ("ao", 0, 1, 2), ("af", 0, 0, 1), ("y", 0, 3), ("ao", 0, 1, 3), ("x", 0, 3), ("af", 0, 1, 1), ("y", 0, 4),
    ("y", 0, 5), ("x", 0, 5), ("ae", 0, 0), ("ae", 0, 1), ("g1", 0), ("g1", 1), ("y", 0, 6), ("x", 0, 6),
    ("g2", 1), ("y", 1, 0), ("g2", 0), ("y", 1, 1), ("x", 1, 1), ("he", 0), ("he", 1), ("y", 1, 2), ("d", 0, 0, 1),
    ("d", 0, 1, 1), ("y", 1, 3), ("d", 0, 1, 0), ("x", 1, 3), ("d", 0, 0, 0), ("y", 1, 4), ("d", 0, 0, 2),
    ("y", 1, 5), ("c", 0, 0, (0, 1)), ("d", 0, 1, 2), ("x", 1, 5), ("d", 0, 0, 3), ("d", 0, 1, 3),
    ("c", 0, 0, (0, 0)), ("y", 1, 6), ("x", 1, 6), ("c", 0, 0, (-1, 0)), ("d", 0, 0, 4), ("d", 0, 0, 5),
    ("d", 0, 1, 4), ("c", 0, 0, (1, 0)), ("d", 0, 1, 5), ("y", 2, 0), ("c", 0, 0, (-1, 1)), ("c", 0, 0, (2, 0)),
    ("c", 0, 0, (1, 1)), ("c", 0, 0, (2, 1)), ("c", 0, 1, (0, 0)), ("y", 2, 1), ("c", 0, 1, (2, 0)),
    ("c", 0, 1, (-1, 0)), ("c", 0, 1, (-1, 1)), ("c", 0, 1, (0, 1)), ("c", 0, 1, (1, 0)), ("c", 0, 1, (1, 1)),
    ("c", 0, 1, (2, 1)), ("y", 2, 2), ("f", 0, 0), ("ao", 1, 0, 0), ("ao", 1, 0, 1), ("f", 0, 1), ("ao", 1, 1, 0),
    ("x", 2, 1), ("ao", 1, 0, 2), ("ao", 1, 0, 3), ("y", 2, 3), ("x", 2, 3), ("af", 1, 0, 1), ("y", 2, 4),
    ("af", 1, 0, 0), ("ao", 1, 1, 1), ("af", 1, 1, 0), ("y", 2, 5), ("x", 2, 5), ("ao", 1, 1, 2), ("ae", 1, 0),
    ("y", 2, 6), ("x", 2, 6), ("ao", 1, 1, 3), ("gl", 0, 1), ("af", 1, 1, 1), ("gl", 0, 0), ("y", 3, 0),
    ("x", 3, 1), ("hl", 0), ("y", 3, 1), ("d", 1, 0, 0), ("y", 3, 2), ("d", 1, 0, 1), ("y", 3, 3), ("ae", 1, 1),
    ("gl", 1, 1), ("gl", 1, 0), ("d", 1, 0, 2), ("x", 3, 3), ("c", 1, 0, (0, 1)), ("y", 3, 4), ("c", 1, 0, (0, 0)),
    ("y", 3, 5), ("hl", 1), ("d", 1, 1, 1), ("d", 1, 1, 0), ("d", 1, 1, 3), ("x", 3, 5), ("d", 1, 0, 3),
    ("c", 1, 0, (-1, 0)), ("d", 1, 1, 2), ("y", 3, 6), ("x", 3, 6), ("d", 1, 1, 4), ("d", 1, 0, 5),
    ("c", 1, 0, (1, 0)), ("d", 1, 1, 5), ("c", 1, 1, (0, 1)), ("d", 1, 0, 4), ("c", 1, 1, (1, 0)),
    ("c", 1, 1, (-1, 0)), ("c", 1, 1, (1, 1)), ("c", 1, 0, (2, 1)), ("c", 1, 1, (-1, 1)), ("c", 1, 1, (2, 0)),
    ("c", 1, 1, (2, 1)), ("c", 1, 1, (0, 0)), ("c", 1, 0, (-1, 1)), ("c", 1, 0, (2, 0)), ("c", 1, 0, (1, 1)),
    ("f", 1, 1), ("f", 1, 0),
)
OWN_Y_AT = 4
OWN_X_AT = 5


def kernel(
    tok, mix, en, eg, ev, ed, ep, mg, ln, lg, lv, ld, lp,
    out,
    gbuf, vbuf, dbuf, xbuf, acc, hbuf, tokv, mixv, mixed, gains,
    rs1, rr1, rs2, rr2, keep, br, pbuf, outv,
    loc_sem, w_send, w_recv, p_send, p_recv, ag_send, ag_recv, rs_send, rs1_recv, rs2_recv, out_sem,
):
    rep = lax.axis_index("rep")
    fs = lax.axis_index("fs")
    z = lax.axis_index("tp")
    c = lax.rem(fs, 2)
    xl = lax.rem(fs // 2, 2)
    y = fs // 4
    x = rep * 2 + xl

    def mod4(v):
        return lax.rem(v + 8, 4)

    def dev(dx=0, dy=0, dz=0, dc=0):
        nx = mod4(x + dx)
        ny = mod4(y + dy)
        nc = c if dc == 0 else 1 - c
        return (nx // 2, (ny * 2 + lax.rem(nx, 2)) * 2 + nc, mod4(z + dz))

    y_dev = {1: dev(dy=1), -1: dev(dy=-1)}
    x_dev = {1: dev(dx=1), -1: dev(dx=-1)}
    z_dev = {1: dev(dz=1), -1: dev(dz=-1)}
    partner = dev(dc=1)
    everyone = [y_dev[1], y_dev[-1], x_dev[1], x_dev[-1], z_dev[1], z_dev[-1], partner]
    zp, zm, zo = mod4(z + 1), mod4(z - 1), mod4(z + 2)

    def blk_of(dy, dp):
        return mod4(y + dy) * 2 + (xl if dp == 0 else 1 - xl)

    blocks = {(dy, dp): blk_of(dy, dp) for dy in (0, 1, -1, 2) for dp in (0, 1)}

    def unit(r, content, core):
        dy, dp, st, s = content
        blk = blocks[(dy, dp)]
        layer = r // 2
        if r % 2 == 0:
            buf = gbuf if st == 0 else vbuf
            row = pl.multiple_of(blk * 256 + core * 128 + s * 64, 64)
            return buf.at[layer, pl.ds(row, 64), :]
        return dbuf.at[layer, blk, core, pl.ds(st * 640 + s * 320, 320), :]

    def unit_id(content):
        dy, dp, st, s = content
        return (((dy % 4) * 2 + dp) * 2 + st) * 2 + s

    def send(src, dst, send_sem, recv_sem, target):
        pltpu.make_async_remote_copy(src, dst, send_sem, recv_sem, device_id=target, device_id_type=MESH).start()

    def await_bytes(ref, sem):
        pltpu.make_async_copy(ref, ref, sem).wait()

    def units(r, n):
        return gbuf.at[0, pl.ds(0, n * (64 if r % 2 == 0 else 32)), :]

    def tee(sign):
        return 0 if sign > 0 else 1

    def y_recv_content(sign, k):
        t = tee(sign)
        return [(-sign, 0, t, 0), (-sign, 0, t, 1), (-sign, 0, 1 - t, 0), (-sign, 0, 1 - t, 1), (2, 0, t, 0),
                (2, 0, t, 1), (2, 1, t, 1)][k]

    def y_send_content(sign, k):
        t = tee(sign)
        return [(0, 0, t, 0), (0, 0, t, 1), (0, 0, 1 - t, 0), (0, 0, 1 - t, 1), (-sign, 0, t, 0),
                (-sign, 0, t, 1), (-sign, 1, t, 1)][k]

    def x_content(sign, k, dp):
        t = tee(sign)
        return [(0, dp, t, 0), (0, dp, t, 1), (-sign, dp, t, 0), (-sign, dp, t, 1), (sign, dp, t, 0),
                (sign, dp, t, 1), (2, dp, t, 0)][k]

    have = set()
    partner_have = set()

    def group_of(r, content):
        dy, dp, st, s = content
        if r % 2 == 0:
            return (0 if r == 0 else 19) + (0 if dy in (0, -1 if st == 0 else 1) else 2 if dy == 2 else 1)
        return 3 + (r // 2) * 8 + (dy % 4) * 2 + dp

    def send_y(r, sign, k):
        content = y_send_content(sign, k)
        assert (r, content) in have
        ref = unit(r, content, c)
        send(ref, ref, w_send.at[r], w_recv.at[r, k], y_dev[sign])

    def send_x(r, sign, k):
        content = x_content(sign, k, 0)
        assert (r, content) in have
        ref = unit(r, content, c)
        send(ref, ref, w_send.at[r], w_recv.at[r, 7 + k // 2], x_dev[sign])

    def send_partner(r, content):
        ref = unit(r, content, c)
        send(ref, ref, p_send.at[r], p_recv.at[group_of(r, content)], partner)

    every = [(dy, dp, st, s) for dy in (0, 1, -1, 2) for dp in (0, 1) for st in (0, 1) for s in (0, 1)]

    def need(r, group):
        members = [content for content in every if group_of(r, content) == group]
        assert all((r, content) in have for content in members), (r, group)
        if group not in partner_have:
            partner_have.add(group)
            await_bytes(units(r, len(members)), p_recv.at[group])

    def own_y(r):
        wait_local(r)
        for sign in (1, -1):
            for k in (0, 1, 2, 3):
                send_y(r, sign, k)

    def own_x(r):
        for sign in (1, -1):
            send_x(r, sign, 0)
            send_x(r, sign, 1)

    def own_partner(r):
        for st in (0, 1):
            for s in (0, 1):
                send_partner(r, (0, 0, st, s))

    def y_event(r, j):
        await_bytes(units(r, 2), w_recv.at[r, j])
        for sign in (1, -1):
            have.add((r, y_recv_content(sign, j)))
        for sign in (1, -1):
            if j in (2, 3):
                send_x(r, -sign, j + 2)
            elif j < 5:
                send_x(r, sign, j + 2)
            if j < 2:
                send_y(r, sign, j + 4)
        if r < 3 and j == OWN_Y_AT:
            own_y(r + 1)
        if r < 3 and j == OWN_X_AT:
            own_x(r + 1)
        for sign in (1, -1):
            send_partner(r, y_recv_content(sign, j))
        if r < 3 and j == OWN_Y_AT:
            own_partner(r + 1)

    def x_event(r, j):
        ks = (6,) if j == 6 else (j - 1, j)
        await_bytes(units(r, 2 * len(ks)), w_recv.at[r, 7 + ks[0] // 2])
        for sign in (1, -1):
            for k in ks:
                have.add((r, x_content(sign, k, 1)))
            if j == 3:
                send_y(r, sign, 6)
        for k in ks:
            for sign in (1, -1):
                send_partner(r, x_content(sign, k, 1))

    own = pl.multiple_of(blocks[(0, 0)] * 256 + c * 128, 128)
    weights = {
        0: [(eg, gbuf.at[0, pl.ds(own, 128), :]), (ev, vbuf.at[0, pl.ds(own, 128), :])],
        1: [(ed, dbuf.at[0, blocks[(0, 0)], c])],
        2: [(lg, gbuf.at[1, pl.ds(own, 128), :]), (lv, vbuf.at[1, pl.ds(own, 128), :])],
        3: [(ld, dbuf.at[1, blocks[(0, 0)], c])],
    }
    norms = [(g, gains.at[i]) for i, g in enumerate((en, ep, mg, ln, lp))]
    for i, pairs in enumerate((weights[0], [(tok, tokv)], norms, weights[1], weights[2], weights[3], [(mix, mixv)])):
        for src, dst in pairs:
            pltpu.make_async_copy(src, dst, loc_sem.at[i]).start()

    def wait_local(r):
        await_bytes(units(r, 4), loc_sem.at[(0, 3, 4, 5)[r]])
        for st in (0, 1):
            for s in (0, 1):
                have.add((r, (0, 0, st, s)))

    barrier = pltpu.get_barrier_semaphore()
    for other in everyone:
        pl.semaphore_signal(barrier, inc=1, device_id=other, device_id_type=MESH)
    pl.semaphore_wait(barrier, len(everyone))

    def x_rows(layer, h, zz, u, n=16):
        row = pl.multiple_of(h * 256 + zz * 64 + u * 16, 16)
        return xbuf.at[layer, pl.ds(row, n), :]

    def ag_own(layer, h, u):
        for sign in (1, -1):
            v = u if sign > 0 else (u + 2) % 4
            ref = x_rows(layer, h, z, v)
            send(ref, ref, ag_send.at[layer], ag_recv.at[h, min(u, 2)], z_dev[sign])

    def ag_forward(layer, h, u):
        await_bytes(xbuf.at[0, pl.ds(0, 32), :], ag_recv.at[h, u])
        for sign in (1, -1):
            v = u if sign > 0 else u + 2
            ref = x_rows(layer, h, zm if sign > 0 else zp, v)
            send(ref, ref, ag_send.at[layer], ag_recv.at[h, 2], z_dev[sign])

    def ag_finish(layer, h):
        await_bytes(xbuf.at[0, pl.ds(0, 128), :], ag_recv.at[h, 2])

    def rms(v, gain):
        return v * lax.rsqrt(jnp.mean(v * v, axis=-1, keepdims=True) + EPS) * gain

    def early_norm(h):
        for i in range(4):
            v = rms(tokv[h * 64 + i * 16 : h * 64 + i * 16 + 16, :].astype(F32), gains[0])
            x_rows(0, h, z, i)[...] = v.astype(BF)

    def dot_rows(st, rows, dy, cols, layer=0):
        base = pl.multiple_of(mod4(y + dy) * 512, 512)
        w = gbuf if st == 0 else vbuf
        return jnp.dot(xbuf[layer, rows, pl.ds(base, 512)], w[layer, pl.ds(base, 512), cols], preferred_element_type=F32)

    whole = slice(0, 512)

    def tile(n):
        return slice(n * 256, n * 256 + 256)

    def gemm1(st):
        need(0, 0)
        for n in range(5):
            acc[st, :, tile(n)] = dot_rows(st, whole, 0, tile(n)) + dot_rows(st, whole, -1 if st == 0 else 1, tile(n))

    def silu_mul(g, v):
        return (g * (1.0 / (1.0 + jnp.exp(-g))) * v).astype(BF)

    def gemm2(st):
        need(0, 1)
        for n in range(5):
            acc[st, :, tile(n)] += dot_rows(st, whole, 1 if st == 0 else -1, tile(n))

    def gemm1_later(h, part):
        need(2, 19)
        need(2, 20)
        rows = slice(h * 256, h * 256 + 256)
        for n in ((0, 1, 2), (3, 4))[part]:
            for st in (0, 1):
                parts = [dot_rows(st, rows, dy, tile(n), 1) for dy in (0, -1, 1)]
                acc[st, rows, tile(n)] = parts[0] + parts[1] + parts[2]

    def hidden(layer, h):
        need(2 * layer, 19 * layer + 2)
        rows = slice(h * 256, h * 256 + 256)
        for n in range(5):
            g = acc[0, rows, tile(n)] + dot_rows(0, rows, 2, tile(n), layer)
            v = acc[1, rows, tile(n)] + dot_rows(1, rows, 2, tile(n), layer)
            hbuf[rows, tile(n)] = silu_mul(g, v)

    def hidden_early(h):
        hidden(0, h)

    def hidden_later(h):
        hidden(1, h)

    chunks = ((0, 0), (0, 1), (-1, 0), (1, 0), (2, 0), (-1, 1), (1, 1), (2, 1))

    groups = (((0, 0),), ((0, 1),), ((-1, 0), (1, 0)), ((2, 0),), ((-1, 1), (1, 1)), ((2, 1),))

    def down(layer, h, i):
        r = 2 * layer + 1

        def rows(zz, half):
            return pl.ds(pl.multiple_of(zz * 64 + half * 32, 32), 32)

        for dy, dp in groups[i]:
            need(r, group_of(r, (dy, dp, 0, 0)))
        for k, chunk in enumerate(groups[i]):
            blk = blocks[chunk]
            w = jnp.concatenate([dbuf[layer, blk, 0], dbuf[layer, blk, 1]], axis=1)
            pbuf[k] = jnp.dot(hbuf[h * 256 : h * 256 + 256, :], w, preferred_element_type=F32)
        for k, chunk in enumerate(groups[i]):
            j = chunks.index(chunk)
            rs1[layer, h, j, 0, 0:32, :] = pbuf[k, rows(zo, 0), :].astype(BF)
            rs1[layer, h, j, 0, 32:64, :] = pbuf[k, rows(zp, 1), :].astype(BF)
            rs1[layer, h, j, 1, 0:32, :] = pbuf[k, rows(zm, 0), :].astype(BF)
            rs1[layer, h, j, 1, 32:64, :] = pbuf[k, rows(zo, 1), :].astype(BF)
            keep[h, j, 0] = pbuf[k, rows(zp, 0), :]
            keep[h, j, 1] = pbuf[k, rows(zm, 1), :]
            cols = pl.ds(pl.multiple_of(blocks[chunk] * 256, 256), 256)
            br[h * 64 : h * 64 + 64, cols] = pbuf[k, pl.ds(pl.multiple_of(z * 64, 64), 64), :]
        for chunk in groups[i]:
            j = chunks.index(chunk)
            for sign in (1, -1):
                lane = tee(sign)
                send(rs1.at[layer, h, j, lane], rr1.at[layer, h, j, lane], rs_send.at[0], rs1_recv.at[h, j], z_dev[sign])

    def combine(layer, h, chunk):
        j = chunks.index(chunk)
        await_bytes(rr1.at[layer, h, j], rs1_recv.at[h, j])
        for sign in (1, -1):
            lane = tee(sign)
            half = slice(0, 32) if sign > 0 else slice(32, 64)
            rs2[layer, h, j, lane] = (rr1[layer, h, j, lane, half, :].astype(F32) + keep[h, j, lane]).astype(BF)
        for sign in (1, -1):
            lane = tee(sign)
            send(rs2.at[layer, h, j, lane], rr2.at[layer, h, j, lane], rs_send.at[1], rs2_recv.at[h], z_dev[sign])
        cols = pl.ds(pl.multiple_of(blocks[chunk] * 256, 256), 256)
        br[h * 64 : h * 64 + 32, cols] += rr1[layer, h, j, 1, 0:32, :].astype(F32)
        br[h * 64 + 32 : h * 64 + 64, cols] += rr1[layer, h, j, 0, 32:64, :].astype(F32)

    def finish(layer, h):
        await_bytes(rr2.at[layer, h], rs2_recv.at[h])
        for j, chunk in enumerate(chunks):
            cols = pl.ds(pl.multiple_of(blocks[chunk] * 256, 256), 256)
            br[h * 64 : h * 64 + 32, cols] += rr2[layer, h, j, 0].astype(F32)
            br[h * 64 + 32 : h * 64 + 64, cols] += rr2[layer, h, j, 1].astype(F32)
        for i in range(4):
            rows = slice(h * 64 + i * 16, h * 64 + i * 16 + 16)
            branch = br[rows, :]
            if layer == 0:
                m = tokv[rows, :].astype(F32) + 0.5 * rms(branch, gains[1]) + rms(mixv[rows, :].astype(F32), gains[2])
                m = m.astype(BF)
                mixed[rows, :] = m
                x_rows(1, h, z, i)[...] = rms(m.astype(F32), gains[3]).astype(BF)
            else:
                outv[rows, :] = (mixed[rows, :].astype(F32) + 0.5 * rms(branch, gains[4])).astype(BF)
        if layer == 1:
            half = pl.ds(h * 64, 64)
            pltpu.make_async_copy(outv.at[half], out.at[half], out_sem.at[h]).start()

    wait_local(0)
    for sign in (1, -1):
        send_y(0, sign, 0)
        send_x(0, sign, 0)
        send_y(0, sign, 1)
        send_x(0, sign, 1)
        send_y(0, sign, 2)
        send_y(0, sign, 3)
    own_partner(0)
    await_bytes(tokv, loc_sem.at[1])
    await_bytes(gains, loc_sem.at[2])
    await_bytes(mixv, loc_sem.at[6])
    tasks = dict(
        y=y_event, x=x_event, en=early_norm, ao=ag_own, af=ag_forward, ae=ag_finish, g1=gemm1, g2=gemm2, gl=gemm1_later,
        he=hidden_early, hl=hidden_later, d=down, c=combine, f=finish,
    )
    for name, *args in ORDER:
        fn = tasks[name]
        fn(*args)

    for r in range(4):
        await_bytes(units(r, 28), w_send.at[r])
        await_bytes(units(r, 32), p_send.at[r])
    for layer in (0, 1):
        await_bytes(xbuf.at[0, pl.ds(0, 384), :], ag_send.at[layer])
    for h in (0, 1):
        half = pl.ds(h * 64, 64)
        pltpu.make_async_copy(outv.at[half], out.at[half], out_sem.at[h]).wait()
    await_bytes(rs1, rs_send.at[0])
    await_bytes(rs2, rs_send.at[1])


PIECES = 4


def settle(source, target, buf, in_sem, out_sem):
    rows = 128 // PIECES
    parts = [pl.ds(i * rows, rows) for i in range(PIECES)]
    arrive = [pltpu.make_async_copy(source.at[p], buf.at[p], in_sem.at[i]) for i, p in enumerate(parts)]
    leave = [pltpu.make_async_copy(buf.at[p], target.at[p], out_sem.at[i]) for i, p in enumerate(parts)]
    for copy in arrive:
        copy.start()
    for i in range(PIECES):
        arrive[i].wait()
        leave[i].start()
    for copy in leave:
        copy.wait()


def on_device(tokens, mixer_output, en, eg, ev, ed, ep, mg, ln, lg, lv, ld, lp):
    gains = [g.reshape(1, 2048) for g in (en, ep, mg, ln, lp)]
    en, ep, mg, ln, lp = gains
    result = pl.pallas_call(
        kernel,
        out_shape=jax.ShapeDtypeStruct((128, 2048), BF),
        in_specs=[pl.BlockSpec(memory_space=pl.ANY)] * 13,
        out_specs=pl.BlockSpec(memory_space=pl.ANY),
        scratch_shapes=[
            pltpu.VMEM((2, 2048, 1280), BF),
            pltpu.VMEM((2, 2048, 1280), BF),
            pltpu.VMEM((2, 8, 2, 1280, 128), BF),
            pltpu.VMEM((2, 512, 2048), BF),
            pltpu.VMEM((2, 512, 1280), F32),
            pltpu.VMEM((512, 1280), BF),
            pltpu.VMEM((128, 2048), BF),
            pltpu.VMEM((128, 2048), BF),
            pltpu.VMEM((128, 2048), BF),
            pltpu.VMEM((5, 1, 2048), F32),
            pltpu.VMEM((2, 2, 8, 2, 64, 256), BF),
            pltpu.VMEM((2, 2, 8, 2, 64, 256), BF),
            pltpu.VMEM((2, 2, 8, 2, 32, 256), BF),
            pltpu.VMEM((2, 2, 8, 2, 32, 256), BF),
            pltpu.VMEM((2, 8, 2, 32, 256), F32),
            pltpu.VMEM((128, 2048), F32),
            pltpu.VMEM((2, 256, 256), F32),
            pltpu.VMEM((128, 2048), BF),
            pltpu.SemaphoreType.DMA((7,)),
            pltpu.SemaphoreType.DMA((4,)),
            pltpu.SemaphoreType.DMA((4, 11)),
            pltpu.SemaphoreType.DMA((4,)),
            pltpu.SemaphoreType.DMA((22,)),
            pltpu.SemaphoreType.DMA((2,)),
            pltpu.SemaphoreType.DMA((2, 3)),
            pltpu.SemaphoreType.DMA((2,)),
            pltpu.SemaphoreType.DMA((2, 8)),
            pltpu.SemaphoreType.DMA((2,)),
            pltpu.SemaphoreType.DMA((2,)),
        ],
        compiler_params=pltpu.CompilerParams(
            collective_id=0, has_side_effects=True, vmem_limit_bytes=67_000_000
        ),
    )(tokens, mixer_output, en, eg, ev, ed, ep, mg, ln, lg, lv, ld, lp)
    return pl.pallas_call(
        settle,
        out_shape=jax.ShapeDtypeStruct((128, 2048), BF),
        in_specs=[pl.BlockSpec(memory_space=pl.ANY)],
        out_specs=pl.BlockSpec(memory_space=pl.ANY),
        scratch_shapes=[
            pltpu.VMEM((128, 2048), BF), pltpu.SemaphoreType.DMA((PIECES,)), pltpu.SemaphoreType.DMA((PIECES,))
        ],
    )(result)


def solution(mesh):
    placed = (
        P(("rep", "fs", "tp"), None),
        P(("rep", "fs", "tp"), None),
        P(),
        P("fs", "tp"),
        P("fs", "tp"),
        P("tp", "fs"),
        P(),
        P(),
        P(),
        P("fs", "tp"),
        P("fs", "tp"),
        P("tp", "fs"),
        P(),
    )
    return jax.shard_map(
        on_device,
        mesh=mesh,
        in_specs=placed,
        out_specs=P(("rep", "fs", "tp"), None),
        check_vma=False,
    )
```

```python
import functools

import jax
import jax.numpy as jnp
from jax import lax
from jax.experimental import pallas as pl
from jax.experimental.pallas import tpu as pltpu
from jax.sharding import PartitionSpec as P

MESH = pl.DeviceIdType.MESH
EPS = 1e-06
BF = jnp.bfloat16
F32 = jnp.float32


ORDER = (
    ("en", 0), ("en", 1), ("ao", 0, 1, 0), ("ao", 0, 0, 0), ("y", 0, 0), ("ao", 0, 1, 1), ("ao", 0, 0, 1),
    ("x", 0, 1), ("ao", 0, 0, 2), ("af", 0, 1, 0), ("af", 0, 0, 0), ("y", 0, 1), ("y", 0, 2), ("ao", 0, 0, 3),
    ("ao", 0, 1, 2), ("af", 0, 0, 1), ("y", 0, 3), ("ao", 0, 1, 3), ("x", 0, 3), ("af", 0, 1, 1), ("y", 0, 4),
    ("y", 0, 5), ("x", 0, 5), ("ae", 0, 0), ("ae", 0, 1), ("g1", 0), ("g1", 1), ("y", 0, 6), ("x", 0, 6),
    ("g2", 1), ("y", 1, 0), ("g2", 0), ("y", 1, 1), ("x", 1, 1), ("he", 0), ("he", 1), ("y", 1, 2), ("d", 0, 0, 1),
    ("d", 0, 1, 1), ("y", 1, 3), ("d", 0, 1, 0), ("x", 1, 3), ("d", 0, 0, 0), ("y", 1, 4), ("d", 0, 0, 2),
    ("y", 1, 5), ("c", 0, 0, (0, 1)), ("d", 0, 1, 2), ("x", 1, 5), ("d", 0, 0, 3), ("d", 0, 1, 3),
    ("c", 0, 0, (0, 0)), ("y", 1, 6), ("x", 1, 6), ("c", 0, 0, (-1, 0)), ("d", 0, 0, 4), ("d", 0, 0, 5),
    ("d", 0, 1, 4), ("c", 0, 0, (1, 0)), ("d", 0, 1, 5), ("y", 2, 0), ("c", 0, 0, (-1, 1)), ("c", 0, 0, (2, 0)),
    ("c", 0, 0, (1, 1)), ("c", 0, 0, (2, 1)), ("c", 0, 1, (0, 0)), ("y", 2, 1), ("c", 0, 1, (2, 0)),
    ("c", 0, 1, (-1, 0)), ("c", 0, 1, (-1, 1)), ("c", 0, 1, (0, 1)), ("c", 0, 1, (1, 0)), ("c", 0, 1, (1, 1)),
    ("c", 0, 1, (2, 1)), ("y", 2, 2), ("f", 0, 0), ("ao", 1, 0, 0), ("ao", 1, 0, 1), ("f", 0, 1), ("ao", 1, 1, 0),
    ("x", 2, 1), ("ao", 1, 0, 2), ("ao", 1, 0, 3), ("y", 2, 3), ("x", 2, 3), ("af", 1, 0, 1), ("y", 2, 4),
    ("af", 1, 0, 0), ("ao", 1, 1, 1), ("af", 1, 1, 0), ("y", 2, 5), ("x", 2, 5), ("ao", 1, 1, 2), ("ae", 1, 0),
    ("y", 2, 6), ("x", 2, 6), ("ao", 1, 1, 3), ("gl", 0, 1), ("af", 1, 1, 1), ("gl", 0, 0), ("y", 3, 0),
    ("x", 3, 1), ("hl", 0), ("y", 3, 1), ("d", 1, 0, 0), ("y", 3, 2), ("d", 1, 0, 1), ("y", 3, 3), ("ae", 1, 1),
    ("gl", 1, 1), ("gl", 1, 0), ("d", 1, 0, 2), ("x", 3, 3), ("c", 1, 0, (0, 1)), ("y", 3, 4), ("c", 1, 0, (0, 0)),
    ("y", 3, 5), ("hl", 1), ("d", 1, 1, 1), ("d", 1, 1, 0), ("d", 1, 1, 3), ("x", 3, 5), ("d", 1, 0, 3),
    ("c", 1, 0, (-1, 0)), ("d", 1, 1, 2), ("y", 3, 6), ("x", 3, 6), ("d", 1, 1, 4), ("d", 1, 0, 5),
    ("c", 1, 0, (1, 0)), ("d", 1, 1, 5), ("c", 1, 1, (0, 1)), ("d", 1, 0, 4), ("c", 1, 1, (1, 0)),
    ("c", 1, 1, (-1, 0)), ("c", 1, 1, (1, 1)), ("c", 1, 0, (2, 1)), ("c", 1, 1, (-1, 1)), ("c", 1, 1, (2, 0)),
    ("c", 1, 1, (2, 1)), ("c", 1, 1, (0, 0)), ("c", 1, 0, (-1, 1)), ("c", 1, 0, (2, 0)), ("c", 1, 0, (1, 1)),
    ("f", 1, 1), ("f", 1, 0),
)
OWN_Y_AT = 4
OWN_X_AT = 5


def kernel(
    tok, mix, en, eg, ev, ed, ep, mg, ln, lg, lv, ld, lp,
    out,
    gbuf, vbuf, dbuf, xbuf, acc, hbuf, tokv, mixv, mixed, gains,
    rs1, rr1, rs2, rr2, keep, br, pbuf,
    loc_sem, w_send, w_recv, p_send, p_recv, ag_send, ag_recv, rs_send, rs1_recv, rs2_recv,
):
    rep = lax.axis_index("rep")
    fs = lax.axis_index("fs")
    z = lax.axis_index("tp")
    c = lax.rem(fs, 2)
    xl = lax.rem(fs // 2, 2)
    y = fs // 4
    x = rep * 2 + xl

    def mod4(v):
        return lax.rem(v + 8, 4)

    def dev(dx=0, dy=0, dz=0, dc=0):
        nx = mod4(x + dx)
        ny = mod4(y + dy)
        nc = c if dc == 0 else 1 - c
        return (nx // 2, (ny * 2 + lax.rem(nx, 2)) * 2 + nc, mod4(z + dz))

    y_dev = {1: dev(dy=1), -1: dev(dy=-1)}
    x_dev = {1: dev(dx=1), -1: dev(dx=-1)}
    z_dev = {1: dev(dz=1), -1: dev(dz=-1)}
    partner = dev(dc=1)
    everyone = [y_dev[1], y_dev[-1], x_dev[1], x_dev[-1], z_dev[1], z_dev[-1], partner]
    zp, zm, zo = mod4(z + 1), mod4(z - 1), mod4(z + 2)

    def blk_of(dy, dp):
        return mod4(y + dy) * 2 + (xl if dp == 0 else 1 - xl)

    blocks = {(dy, dp): blk_of(dy, dp) for dy in (0, 1, -1, 2) for dp in (0, 1)}

    def unit(r, content, core):
        dy, dp, st, s = content
        blk = blocks[(dy, dp)]
        layer = r // 2
        if r % 2 == 0:
            buf = gbuf if st == 0 else vbuf
            row = pl.multiple_of(blk * 256 + core * 128 + s * 64, 64)
            return buf.at[layer, pl.ds(row, 64), :]
        return dbuf.at[layer, blk, core, pl.ds(st * 640 + s * 320, 320), :]

    def unit_id(content):
        dy, dp, st, s = content
        return (((dy % 4) * 2 + dp) * 2 + st) * 2 + s

    def send(src, dst, send_sem, recv_sem, target):
        pltpu.make_async_remote_copy(src, dst, send_sem, recv_sem, device_id=target, device_id_type=MESH).start()

    def await_bytes(ref, sem):
        pltpu.make_async_copy(ref, ref, sem).wait()

    def units(r, n):
        return gbuf.at[0, pl.ds(0, n * (64 if r % 2 == 0 else 32)), :]

    def tee(sign):
        return 0 if sign > 0 else 1

    def y_recv_content(sign, k):
        t = tee(sign)
        return [(-sign, 0, t, 0), (-sign, 0, t, 1), (-sign, 0, 1 - t, 0), (-sign, 0, 1 - t, 1), (2, 0, t, 0),
                (2, 0, t, 1), (2, 1, t, 1)][k]

    def y_send_content(sign, k):
        t = tee(sign)
        return [(0, 0, t, 0), (0, 0, t, 1), (0, 0, 1 - t, 0), (0, 0, 1 - t, 1), (-sign, 0, t, 0),
                (-sign, 0, t, 1), (-sign, 1, t, 1)][k]

    def x_content(sign, k, dp):
        t = tee(sign)
        return [(0, dp, t, 0), (0, dp, t, 1), (-sign, dp, t, 0), (-sign, dp, t, 1), (sign, dp, t, 0),
                (sign, dp, t, 1), (2, dp, t, 0)][k]

    have = set()
    partner_have = set()

    def group_of(r, content):
        dy, dp, st, s = content
        if r % 2 == 0:
            return (0 if r == 0 else 19) + (0 if dy in (0, -1 if st == 0 else 1) else 2 if dy == 2 else 1)
        return 3 + (r // 2) * 8 + (dy % 4) * 2 + dp

    def send_y(r, sign, k):
        content = y_send_content(sign, k)
        assert (r, content) in have
        ref = unit(r, content, c)
        send(ref, ref, w_send.at[r], w_recv.at[r, k], y_dev[sign])

    def send_x(r, sign, k):
        content = x_content(sign, k, 0)
        assert (r, content) in have
        ref = unit(r, content, c)
        send(ref, ref, w_send.at[r], w_recv.at[r, 7 + k // 2], x_dev[sign])

    def send_partner(r, content):
        ref = unit(r, content, c)
        send(ref, ref, p_send.at[r], p_recv.at[group_of(r, content)], partner)

    every = [(dy, dp, st, s) for dy in (0, 1, -1, 2) for dp in (0, 1) for st in (0, 1) for s in (0, 1)]

    def need(r, group):
        members = [content for content in every if group_of(r, content) == group]
        assert all((r, content) in have for content in members), (r, group)
        if group not in partner_have:
            partner_have.add(group)
            await_bytes(units(r, len(members)), p_recv.at[group])

    def own_y(r):
        wait_local(r)
        for sign in (1, -1):
            for k in (0, 1, 2, 3):
                send_y(r, sign, k)

    def own_x(r):
        for sign in (1, -1):
            send_x(r, sign, 0)
            send_x(r, sign, 1)

    def own_partner(r):
        for st in (0, 1):
            for s in (0, 1):
                send_partner(r, (0, 0, st, s))

    def y_event(r, j):
        await_bytes(units(r, 2), w_recv.at[r, j])
        for sign in (1, -1):
            have.add((r, y_recv_content(sign, j)))
        for sign in (1, -1):
            if j in (2, 3):
                send_x(r, -sign, j + 2)
            elif j < 5:
                send_x(r, sign, j + 2)
            if j < 2:
                send_y(r, sign, j + 4)
        if r < 3 and j == OWN_Y_AT:
            own_y(r + 1)
        if r < 3 and j == OWN_X_AT:
            own_x(r + 1)
        for sign in (1, -1):
            send_partner(r, y_recv_content(sign, j))
        if r < 3 and j == OWN_Y_AT:
            own_partner(r + 1)

    def x_event(r, j):
        ks = (6,) if j == 6 else (j - 1, j)
        await_bytes(units(r, 2 * len(ks)), w_recv.at[r, 7 + ks[0] // 2])
        for sign in (1, -1):
            for k in ks:
                have.add((r, x_content(sign, k, 1)))
            if j == 3:
                send_y(r, sign, 6)
        for k in ks:
            for sign in (1, -1):
                send_partner(r, x_content(sign, k, 1))

    own = pl.multiple_of(blocks[(0, 0)] * 256 + c * 128, 128)
    weights = {
        0: [(eg, gbuf.at[0, pl.ds(own, 128), :]), (ev, vbuf.at[0, pl.ds(own, 128), :])],
        1: [(ed, dbuf.at[0, blocks[(0, 0)], c])],
        2: [(lg, gbuf.at[1, pl.ds(own, 128), :]), (lv, vbuf.at[1, pl.ds(own, 128), :])],
        3: [(ld, dbuf.at[1, blocks[(0, 0)], c])],
    }
    norms = [(g, gains.at[i]) for i, g in enumerate((en, ep, mg, ln, lp))]
    for i, pairs in enumerate((weights[0], [(tok, tokv)], norms, weights[1], weights[2], weights[3], [(mix, mixv)])):
        for src, dst in pairs:
            pltpu.make_async_copy(src, dst, loc_sem.at[i]).start()

    def wait_local(r):
        await_bytes(units(r, 4), loc_sem.at[(0, 3, 4, 5)[r]])
        for st in (0, 1):
            for s in (0, 1):
                have.add((r, (0, 0, st, s)))

    barrier = pltpu.get_barrier_semaphore()
    for other in everyone:
        pl.semaphore_signal(barrier, inc=1, device_id=other, device_id_type=MESH)
    pl.semaphore_wait(barrier, len(everyone))

    def x_rows(layer, h, zz, u, n=16):
        row = pl.multiple_of(h * 256 + zz * 64 + u * 16, 16)
        return xbuf.at[layer, pl.ds(row, n), :]

    def ag_own(layer, h, u):
        for sign in (1, -1):
            v = u if sign > 0 else (u + 2) % 4
            ref = x_rows(layer, h, z, v)
            send(ref, ref, ag_send.at[layer], ag_recv.at[h, min(u, 2)], z_dev[sign])

    def ag_forward(layer, h, u):
        await_bytes(xbuf.at[0, pl.ds(0, 32), :], ag_recv.at[h, u])
        for sign in (1, -1):
            v = u if sign > 0 else u + 2
            ref = x_rows(layer, h, zm if sign > 0 else zp, v)
            send(ref, ref, ag_send.at[layer], ag_recv.at[h, 2], z_dev[sign])

    def ag_finish(layer, h):
        await_bytes(xbuf.at[0, pl.ds(0, 128), :], ag_recv.at[h, 2])

    def rms(v, gain):
        return v * lax.rsqrt(jnp.mean(v * v, axis=-1, keepdims=True) + EPS) * gain

    def early_norm(h):
        for i in range(4):
            v = rms(tokv[h * 64 + i * 16 : h * 64 + i * 16 + 16, :].astype(F32), gains[0])
            x_rows(0, h, z, i)[...] = v.astype(BF)

    def dot_rows(st, rows, dy, cols, layer=0):
        base = pl.multiple_of(mod4(y + dy) * 512, 512)
        w = gbuf if st == 0 else vbuf
        return jnp.dot(xbuf[layer, rows, pl.ds(base, 512)], w[layer, pl.ds(base, 512), cols], preferred_element_type=F32)

    whole = slice(0, 512)

    def tile(n):
        return slice(n * 256, n * 256 + 256)

    def gemm1(st):
        need(0, 0)
        for n in range(5):
            acc[st, :, tile(n)] = dot_rows(st, whole, 0, tile(n)) + dot_rows(st, whole, -1 if st == 0 else 1, tile(n))

    def silu_mul(g, v):
        return (g * (1.0 / (1.0 + jnp.exp(-g))) * v).astype(BF)

    def gemm2(st):
        need(0, 1)
        for n in range(5):
            acc[st, :, tile(n)] += dot_rows(st, whole, 1 if st == 0 else -1, tile(n))

    def gemm1_later(h, part):
        need(2, 19)
        need(2, 20)
        rows = slice(h * 256, h * 256 + 256)
        for n in ((0, 1, 2), (3, 4))[part]:
            for st in (0, 1):
                parts = [dot_rows(st, rows, dy, tile(n), 1) for dy in (0, -1, 1)]
                acc[st, rows, tile(n)] = parts[0] + parts[1] + parts[2]

    def hidden(layer, h):
        need(2 * layer, 19 * layer + 2)
        rows = slice(h * 256, h * 256 + 256)
        for n in range(5):
            g = acc[0, rows, tile(n)] + dot_rows(0, rows, 2, tile(n), layer)
            v = acc[1, rows, tile(n)] + dot_rows(1, rows, 2, tile(n), layer)
            hbuf[rows, tile(n)] = silu_mul(g, v)

    def hidden_early(h):
        hidden(0, h)

    def hidden_later(h):
        hidden(1, h)

    chunks = ((0, 0), (0, 1), (-1, 0), (1, 0), (2, 0), (-1, 1), (1, 1), (2, 1))

    groups = (((0, 0),), ((0, 1),), ((-1, 0), (1, 0)), ((2, 0),), ((-1, 1), (1, 1)), ((2, 1),))

    def down(layer, h, i):
        r = 2 * layer + 1

        def rows(zz, half):
            return pl.ds(pl.multiple_of(zz * 64 + half * 32, 32), 32)

        for dy, dp in groups[i]:
            need(r, group_of(r, (dy, dp, 0, 0)))
        for k, chunk in enumerate(groups[i]):
            blk = blocks[chunk]
            w = jnp.concatenate([dbuf[layer, blk, 0], dbuf[layer, blk, 1]], axis=1)
            pbuf[k] = jnp.dot(hbuf[h * 256 : h * 256 + 256, :], w, preferred_element_type=F32)
        for k, chunk in enumerate(groups[i]):
            j = chunks.index(chunk)
            rs1[layer, h, j, 0, 0:32, :] = pbuf[k, rows(zo, 0), :].astype(BF)
            rs1[layer, h, j, 0, 32:64, :] = pbuf[k, rows(zp, 1), :].astype(BF)
            rs1[layer, h, j, 1, 0:32, :] = pbuf[k, rows(zm, 0), :].astype(BF)
            rs1[layer, h, j, 1, 32:64, :] = pbuf[k, rows(zo, 1), :].astype(BF)
            keep[h, j, 0] = pbuf[k, rows(zp, 0), :]
            keep[h, j, 1] = pbuf[k, rows(zm, 1), :]
            cols = pl.ds(pl.multiple_of(blocks[chunk] * 256, 256), 256)
            br[h * 64 : h * 64 + 64, cols] = pbuf[k, pl.ds(pl.multiple_of(z * 64, 64), 64), :]
        for chunk in groups[i]:
            j = chunks.index(chunk)
            for sign in (1, -1):
                lane = tee(sign)
                send(rs1.at[layer, h, j, lane], rr1.at[layer, h, j, lane], rs_send.at[0], rs1_recv.at[h, j], z_dev[sign])

    def combine(layer, h, chunk):
        j = chunks.index(chunk)
        await_bytes(rr1.at[layer, h, j], rs1_recv.at[h, j])
        for sign in (1, -1):
            lane = tee(sign)
            half = slice(0, 32) if sign > 0 else slice(32, 64)
            rs2[layer, h, j, lane] = (rr1[layer, h, j, lane, half, :].astype(F32) + keep[h, j, lane]).astype(BF)
        for sign in (1, -1):
            lane = tee(sign)
            send(rs2.at[layer, h, j, lane], rr2.at[layer, h, j, lane], rs_send.at[1], rs2_recv.at[h], z_dev[sign])
        cols = pl.ds(pl.multiple_of(blocks[chunk] * 256, 256), 256)
        br[h * 64 : h * 64 + 32, cols] += rr1[layer, h, j, 1, 0:32, :].astype(F32)
        br[h * 64 + 32 : h * 64 + 64, cols] += rr1[layer, h, j, 0, 32:64, :].astype(F32)

    def finish(layer, h):
        await_bytes(rr2.at[layer, h], rs2_recv.at[h])
        for j, chunk in enumerate(chunks):
            cols = pl.ds(pl.multiple_of(blocks[chunk] * 256, 256), 256)
            br[h * 64 : h * 64 + 32, cols] += rr2[layer, h, j, 0].astype(F32)
            br[h * 64 + 32 : h * 64 + 64, cols] += rr2[layer, h, j, 1].astype(F32)
        for i in range(4):
            rows = slice(h * 64 + i * 16, h * 64 + i * 16 + 16)
            branch = br[rows, :]
            if layer == 0:
                m = tokv[rows, :].astype(F32) + 0.5 * rms(branch, gains[1]) + rms(mixv[rows, :].astype(F32), gains[2])
                m = m.astype(BF)
                mixed[rows, :] = m
                x_rows(1, h, z, i)[...] = rms(m.astype(F32), gains[3]).astype(BF)
            else:
                out[rows, :] = (mixed[rows, :].astype(F32) + 0.5 * rms(branch, gains[4])).astype(BF)

    wait_local(0)
    for sign in (1, -1):
        send_y(0, sign, 0)
        send_x(0, sign, 0)
        send_y(0, sign, 1)
        send_x(0, sign, 1)
        send_y(0, sign, 2)
        send_y(0, sign, 3)
    own_partner(0)
    await_bytes(tokv, loc_sem.at[1])
    await_bytes(gains, loc_sem.at[2])
    await_bytes(mixv, loc_sem.at[6])
    tasks = dict(
        y=y_event, x=x_event, en=early_norm, ao=ag_own, af=ag_forward, ae=ag_finish, g1=gemm1, g2=gemm2, gl=gemm1_later,
        he=hidden_early, hl=hidden_later, d=down, c=combine, f=finish,
    )
    for name, *args in ORDER:
        fn = tasks[name]
        fn(*args)

    for r in range(4):
        await_bytes(units(r, 28), w_send.at[r])
        await_bytes(units(r, 32), p_send.at[r])
    for layer in (0, 1):
        await_bytes(xbuf.at[0, pl.ds(0, 384), :], ag_send.at[layer])
    await_bytes(rs1, rs_send.at[0])
    await_bytes(rs2, rs_send.at[1])


def on_device(tokens, mixer_output, en, eg, ev, ed, ep, mg, ln, lg, lv, ld, lp):
    gains = [g.reshape(1, 2048) for g in (en, ep, mg, ln, lp)]
    en, ep, mg, ln, lp = gains
    return pl.pallas_call(
        kernel,
        out_shape=pltpu.VMEM((128, 2048), BF),
        in_specs=[pl.BlockSpec(memory_space=pl.ANY)] * 13,
        out_specs=pl.BlockSpec(memory_space=pltpu.VMEM),
        scratch_shapes=[
            pltpu.VMEM((2, 2048, 1280), BF),
            pltpu.VMEM((2, 2048, 1280), BF),
            pltpu.VMEM((2, 8, 2, 1280, 128), BF),
            pltpu.VMEM((2, 512, 2048), BF),
            pltpu.VMEM((2, 512, 1280), F32),
            pltpu.VMEM((512, 1280), BF),
            pltpu.VMEM((128, 2048), BF),
            pltpu.VMEM((128, 2048), BF),
            pltpu.VMEM((128, 2048), BF),
            pltpu.VMEM((5, 1, 2048), F32),
            pltpu.VMEM((2, 2, 8, 2, 64, 256), BF),
            pltpu.VMEM((2, 2, 8, 2, 64, 256), BF),
            pltpu.VMEM((2, 2, 8, 2, 32, 256), BF),
            pltpu.VMEM((2, 2, 8, 2, 32, 256), BF),
            pltpu.VMEM((2, 8, 2, 32, 256), F32),
            pltpu.VMEM((128, 2048), F32),
            pltpu.VMEM((2, 256, 256), F32),
            pltpu.SemaphoreType.DMA((7,)),
            pltpu.SemaphoreType.DMA((4,)),
            pltpu.SemaphoreType.DMA((4, 11)),
            pltpu.SemaphoreType.DMA((4,)),
            pltpu.SemaphoreType.DMA((22,)),
            pltpu.SemaphoreType.DMA((2,)),
            pltpu.SemaphoreType.DMA((2, 3)),
            pltpu.SemaphoreType.DMA((2,)),
            pltpu.SemaphoreType.DMA((2, 8)),
            pltpu.SemaphoreType.DMA((2,)),
        ],
        compiler_params=pltpu.CompilerParams(
            collective_id=0, has_side_effects=True, vmem_limit_bytes=60_000_000
        ),
    )(tokens, mixer_output, en, eg, ev, ed, ep, mg, ln, lg, lv, ld, lp)


def solution(mesh):
    placed = (
        P(("rep", "fs", "tp"), None),
        P(("rep", "fs", "tp"), None),
        P(),
        P("fs", "tp"),
        P("fs", "tp"),
        P("tp", "fs"),
        P(),
        P(),
        P(),
        P("fs", "tp"),
        P("fs", "tp"),
        P("tp", "fs"),
        P(),
    )
    return jax.shard_map(
        on_device,
        mesh=mesh,
        in_specs=placed,
        out_specs=P(("rep", "fs", "tp"), None),
        check_vma=False,
    )
```

```python
import functools

import jax
import jax.numpy as jnp
from jax import lax
from jax.experimental import pallas as pl
from jax.experimental.pallas import tpu as pltpu
from jax.sharding import PartitionSpec as P

MESH = pl.DeviceIdType.MESH
EPS = 1e-06
BF = jnp.bfloat16
F32 = jnp.float32


ORDER = (
    ("en", 0), ("en", 1), ("ao", 0, 1, 0), ("ao", 0, 0, 0), ("y", 0, 0), ("ao", 0, 1, 1), ("ao", 0, 0, 1),
    ("x", 0, 1), ("ao", 0, 0, 2), ("af", 0, 1, 0), ("af", 0, 0, 0), ("y", 0, 1), ("y", 0, 2), ("ao", 0, 0, 3),
    ("ao", 0, 1, 2), ("af", 0, 0, 1), ("y", 0, 3), ("ao", 0, 1, 3), ("x", 0, 3), ("af", 0, 1, 1), ("y", 0, 4),
    ("y", 0, 5), ("x", 0, 5), ("ae", 0, 0), ("ae", 0, 1), ("g1", 0), ("g1", 1), ("y", 0, 6), ("x", 0, 6),
    ("g2", 1), ("y", 1, 0), ("g2", 0), ("y", 1, 1), ("x", 1, 1), ("he", 0), ("he", 1), ("y", 1, 2), ("d", 0, 0, 1),
    ("d", 0, 1, 1), ("y", 1, 3), ("d", 0, 1, 0), ("x", 1, 3), ("d", 0, 0, 0), ("y", 1, 4), ("d", 0, 0, 2),
    ("y", 1, 5), ("c", 0, 0, (0, 1)), ("d", 0, 1, 2), ("x", 1, 5), ("d", 0, 0, 3), ("d", 0, 1, 3),
    ("c", 0, 0, (0, 0)), ("y", 1, 6), ("x", 1, 6), ("c", 0, 0, (-1, 0)), ("d", 0, 0, 4), ("d", 0, 0, 5),
    ("d", 0, 1, 4), ("c", 0, 0, (1, 0)), ("d", 0, 1, 5), ("y", 2, 0), ("c", 0, 0, (-1, 1)), ("c", 0, 0, (2, 0)),
    ("c", 0, 0, (1, 1)), ("c", 0, 0, (2, 1)), ("c", 0, 1, (0, 0)), ("y", 2, 1), ("c", 0, 1, (2, 0)),
    ("c", 0, 1, (-1, 0)), ("c", 0, 1, (-1, 1)), ("c", 0, 1, (0, 1)), ("c", 0, 1, (1, 0)), ("c", 0, 1, (1, 1)),
    ("c", 0, 1, (2, 1)), ("y", 2, 2), ("f", 0, 0), ("ao", 1, 0, 0), ("ao", 1, 0, 1), ("f", 0, 1), ("ao", 1, 1, 0),
    ("x", 2, 1), ("ao", 1, 0, 2), ("ao", 1, 0, 3), ("y", 2, 3), ("x", 2, 3), ("af", 1, 0, 1), ("y", 2, 4),
    ("af", 1, 0, 0), ("ao", 1, 1, 1), ("af", 1, 1, 0), ("y", 2, 5), ("x", 2, 5), ("ao", 1, 1, 2), ("ae", 1, 0),
    ("y", 2, 6), ("x", 2, 6), ("ao", 1, 1, 3), ("gl", 0, 1), ("af", 1, 1, 1), ("gl", 0, 0), ("y", 3, 0),
    ("x", 3, 1), ("hl", 0), ("y", 3, 1), ("d", 1, 0, 0), ("y", 3, 2), ("d", 1, 0, 1), ("y", 3, 3), ("ae", 1, 1),
    ("gl", 1, 1), ("gl", 1, 0), ("d", 1, 0, 2), ("x", 3, 3), ("c", 1, 0, (0, 1)), ("y", 3, 4), ("c", 1, 0, (0, 0)),
    ("y", 3, 5), ("hl", 1), ("d", 1, 1, 1), ("d", 1, 1, 0), ("d", 1, 1, 3), ("x", 3, 5), ("d", 1, 0, 3),
    ("c", 1, 0, (-1, 0)), ("d", 1, 1, 2), ("y", 3, 6), ("x", 3, 6), ("d", 1, 1, 4), ("d", 1, 0, 5),
    ("c", 1, 0, (1, 0)), ("d", 1, 1, 5), ("c", 1, 1, (0, 1)), ("d", 1, 0, 4), ("c", 1, 1, (1, 0)),
    ("c", 1, 1, (-1, 0)), ("c", 1, 1, (1, 1)), ("c", 1, 0, (2, 1)), ("c", 1, 1, (-1, 1)), ("c", 1, 1, (2, 0)),
    ("c", 1, 1, (2, 1)), ("c", 1, 1, (0, 0)), ("c", 1, 0, (-1, 1)), ("c", 1, 0, (2, 0)), ("c", 1, 0, (1, 1)),
    ("f", 1, 1), ("f", 1, 0),
)
OWN_Y_AT = 4
OWN_X_AT = 5


def kernel(
    tok, mix, en, eg, ev, ed, ep, mg, ln, lg, lv, ld, lp,
    out,
    gbuf, vbuf, dbuf, xbuf, acc, hbuf, tokv, mixv, mixed, gains,
    rs1, rr1, rs2, rr2, keep, br, pbuf,
    loc_sem, w_send, w_recv, p_send, p_recv, ag_send, ag_recv, rs_send, rs1_recv, rs2_recv,
):
    rep = lax.axis_index("rep")
    fs = lax.axis_index("fs")
    z = lax.axis_index("tp")
    c = lax.rem(fs, 2)
    xl = lax.rem(fs // 2, 2)
    y = fs // 4
    x = rep * 2 + xl

    def mod4(v):
        return lax.rem(v + 8, 4)

    def dev(dx=0, dy=0, dz=0, dc=0):
        nx = mod4(x + dx)
        ny = mod4(y + dy)
        nc = c if dc == 0 else 1 - c
        return (nx // 2, (ny * 2 + lax.rem(nx, 2)) * 2 + nc, mod4(z + dz))

    y_dev = {1: dev(dy=1), -1: dev(dy=-1)}
    x_dev = {1: dev(dx=1), -1: dev(dx=-1)}
    z_dev = {1: dev(dz=1), -1: dev(dz=-1)}
    partner = dev(dc=1)
    everyone = [y_dev[1], y_dev[-1], x_dev[1], x_dev[-1], z_dev[1], z_dev[-1], partner]
    zp, zm, zo = mod4(z + 1), mod4(z - 1), mod4(z + 2)

    def blk_of(dy, dp):
        return mod4(y + dy) * 2 + (xl if dp == 0 else 1 - xl)

    blocks = {(dy, dp): blk_of(dy, dp) for dy in (0, 1, -1, 2) for dp in (0, 1)}

    def unit(r, content, core):
        dy, dp, st, s = content
        blk = blocks[(dy, dp)]
        layer = r // 2
        if r % 2 == 0:
            buf = gbuf if st == 0 else vbuf
            row = pl.multiple_of(blk * 256 + core * 128 + s * 64, 64)
            return buf.at[layer, pl.ds(row, 64), :]
        return dbuf.at[layer, blk, core, pl.ds(st * 640 + s * 320, 320), :]

    def unit_id(content):
        dy, dp, st, s = content
        return (((dy % 4) * 2 + dp) * 2 + st) * 2 + s

    def send(src, dst, send_sem, recv_sem, target):
        pltpu.make_async_remote_copy(src, dst, send_sem, recv_sem, device_id=target, device_id_type=MESH).start()

    def await_bytes(ref, sem):
        pltpu.make_async_copy(ref, ref, sem).wait()

    def units(r, n):
        return gbuf.at[0, pl.ds(0, n * (64 if r % 2 == 0 else 32)), :]

    def tee(sign):
        return 0 if sign > 0 else 1

    def y_recv_content(sign, k):
        t = tee(sign)
        return [(-sign, 0, t, 0), (-sign, 0, t, 1), (-sign, 0, 1 - t, 0), (-sign, 0, 1 - t, 1), (2, 0, t, 0),
                (2, 0, t, 1), (2, 1, t, 1)][k]

    def y_send_content(sign, k):
        t = tee(sign)
        return [(0, 0, t, 0), (0, 0, t, 1), (0, 0, 1 - t, 0), (0, 0, 1 - t, 1), (-sign, 0, t, 0),
                (-sign, 0, t, 1), (-sign, 1, t, 1)][k]

    def x_content(sign, k, dp):
        t = tee(sign)
        return [(0, dp, t, 0), (0, dp, t, 1), (-sign, dp, t, 0), (-sign, dp, t, 1), (sign, dp, t, 0),
                (sign, dp, t, 1), (2, dp, t, 0)][k]

    have = set()
    partner_have = set()

    def group_of(r, content):
        dy, dp, st, s = content
        if r % 2 == 0:
            return (0 if r == 0 else 19) + (0 if dy in (0, -1 if st == 0 else 1) else 2 if dy == 2 else 1)
        return 3 + (r // 2) * 8 + (dy % 4) * 2 + dp

    def send_y(r, sign, k):
        content = y_send_content(sign, k)
        assert (r, content) in have
        ref = unit(r, content, c)
        send(ref, ref, w_send.at[r], w_recv.at[r, k], y_dev[sign])

    def send_x(r, sign, k):
        content = x_content(sign, k, 0)
        assert (r, content) in have
        ref = unit(r, content, c)
        send(ref, ref, w_send.at[r], w_recv.at[r, 7 + k // 2], x_dev[sign])

    def send_partner(r, content):
        ref = unit(r, content, c)
        send(ref, ref, p_send.at[r], p_recv.at[group_of(r, content)], partner)

    every = [(dy, dp, st, s) for dy in (0, 1, -1, 2) for dp in (0, 1) for st in (0, 1) for s in (0, 1)]

    def need(r, group):
        members = [content for content in every if group_of(r, content) == group]
        assert all((r, content) in have for content in members), (r, group)
        if group not in partner_have:
            partner_have.add(group)
            await_bytes(units(r, len(members)), p_recv.at[group])

    def own_y(r):
        wait_local(r)
        for sign in (1, -1):
            for k in (0, 1, 2, 3):
                send_y(r, sign, k)

    def own_x(r):
        for sign in (1, -1):
            send_x(r, sign, 0)
            send_x(r, sign, 1)

    def own_partner(r):
        for st in (0, 1):
            for s in (0, 1):
                send_partner(r, (0, 0, st, s))

    def y_event(r, j):
        await_bytes(units(r, 2), w_recv.at[r, j])
        for sign in (1, -1):
            have.add((r, y_recv_content(sign, j)))
        for sign in (1, -1):
            if j in (2, 3):
                send_x(r, -sign, j + 2)
            elif j < 5:
                send_x(r, sign, j + 2)
            if j < 2:
                send_y(r, sign, j + 4)
        if r < 3 and j == OWN_Y_AT:
            own_y(r + 1)
        if r < 3 and j == OWN_X_AT:
            own_x(r + 1)
        for sign in (1, -1):
            send_partner(r, y_recv_content(sign, j))
        if r < 3 and j == OWN_Y_AT:
            own_partner(r + 1)

    def x_event(r, j):
        ks = (6,) if j == 6 else (j - 1, j)
        await_bytes(units(r, 2 * len(ks)), w_recv.at[r, 7 + ks[0] // 2])
        for sign in (1, -1):
            for k in ks:
                have.add((r, x_content(sign, k, 1)))
            if j == 3:
                send_y(r, sign, 6)
        for k in ks:
            for sign in (1, -1):
                send_partner(r, x_content(sign, k, 1))

    own = pl.multiple_of(blocks[(0, 0)] * 256 + c * 128, 128)
    weights = {
        0: [(eg, gbuf.at[0, pl.ds(own, 128), :]), (ev, vbuf.at[0, pl.ds(own, 128), :])],
        1: [(ed, dbuf.at[0, blocks[(0, 0)], c])],
        2: [(lg, gbuf.at[1, pl.ds(own, 128), :]), (lv, vbuf.at[1, pl.ds(own, 128), :])],
        3: [(ld, dbuf.at[1, blocks[(0, 0)], c])],
    }
    norms = [(g, gains.at[i]) for i, g in enumerate((en, ep, mg, ln, lp))]
    for i, pairs in enumerate((weights[0], [(tok, tokv)], norms, weights[1], weights[2], weights[3], [(mix, mixv)])):
        for src, dst in pairs:
            pltpu.make_async_copy(src, dst, loc_sem.at[i]).start()
        if i == 0:
            barrier = pltpu.get_barrier_semaphore()
            for other in everyone:
                pl.semaphore_signal(barrier, inc=1, device_id=other, device_id_type=MESH)

    def wait_local(r):
        await_bytes(units(r, 4), loc_sem.at[(0, 3, 4, 5)[r]])
        for st in (0, 1):
            for s in (0, 1):
                have.add((r, (0, 0, st, s)))

    pl.semaphore_wait(barrier, len(everyone))

    def x_rows(layer, h, zz, u, n=16):
        row = pl.multiple_of(h * 256 + zz * 64 + u * 16, 16)
        return xbuf.at[layer, pl.ds(row, n), :]

    def ag_own(layer, h, u):
        for sign in (1, -1):
            v = u if sign > 0 else (u + 2) % 4
            ref = x_rows(layer, h, z, v)
            send(ref, ref, ag_send.at[layer], ag_recv.at[h, min(u, 2)], z_dev[sign])

    def ag_forward(layer, h, u):
        await_bytes(xbuf.at[0, pl.ds(0, 32), :], ag_recv.at[h, u])
        for sign in (1, -1):
            v = u if sign > 0 else u + 2
            ref = x_rows(layer, h, zm if sign > 0 else zp, v)
            send(ref, ref, ag_send.at[layer], ag_recv.at[h, 2], z_dev[sign])

    def ag_finish(layer, h):
        await_bytes(xbuf.at[0, pl.ds(0, 128), :], ag_recv.at[h, 2])

    def rms(v, gain):
        return v * lax.rsqrt(jnp.mean(v * v, axis=-1, keepdims=True) + EPS) * gain

    def early_norm(h):
        for i in range(4):
            v = rms(tokv[h * 64 + i * 16 : h * 64 + i * 16 + 16, :].astype(F32), gains[0])
            x_rows(0, h, z, i)[...] = v.astype(BF)

    def dot_rows(st, rows, dy, cols, layer=0):
        base = pl.multiple_of(mod4(y + dy) * 512, 512)
        w = gbuf if st == 0 else vbuf
        return jnp.dot(xbuf[layer, rows, pl.ds(base, 512)], w[layer, pl.ds(base, 512), cols], preferred_element_type=F32)

    whole = slice(0, 512)

    def tile(n):
        return slice(n * 256, n * 256 + 256)

    def gemm1(st):
        need(0, 0)
        for n in range(5):
            acc[st, :, tile(n)] = dot_rows(st, whole, 0, tile(n)) + dot_rows(st, whole, -1 if st == 0 else 1, tile(n))

    def silu_mul(g, v):
        return (g * (1.0 / (1.0 + jnp.exp(-g))) * v).astype(BF)

    def gemm2(st):
        need(0, 1)
        for n in range(5):
            acc[st, :, tile(n)] += dot_rows(st, whole, 1 if st == 0 else -1, tile(n))

    def gemm1_later(h, part):
        need(2, 19)
        need(2, 20)
        rows = slice(h * 256, h * 256 + 256)
        for n in ((0, 1, 2), (3, 4))[part]:
            for st in (0, 1):
                parts = [dot_rows(st, rows, dy, tile(n), 1) for dy in (0, -1, 1)]
                acc[st, rows, tile(n)] = parts[0] + parts[1] + parts[2]

    def hidden(layer, h):
        need(2 * layer, 19 * layer + 2)
        rows = slice(h * 256, h * 256 + 256)
        for n in range(5):
            g = acc[0, rows, tile(n)] + dot_rows(0, rows, 2, tile(n), layer)
            v = acc[1, rows, tile(n)] + dot_rows(1, rows, 2, tile(n), layer)
            hbuf[rows, tile(n)] = silu_mul(g, v)

    def hidden_early(h):
        hidden(0, h)

    def hidden_later(h):
        hidden(1, h)

    chunks = ((0, 0), (0, 1), (-1, 0), (1, 0), (2, 0), (-1, 1), (1, 1), (2, 1))

    groups = (((0, 0),), ((0, 1),), ((-1, 0), (1, 0)), ((2, 0),), ((-1, 1), (1, 1)), ((2, 1),))

    def down(layer, h, i):
        r = 2 * layer + 1

        def rows(zz, half):
            return pl.ds(pl.multiple_of(zz * 64 + half * 32, 32), 32)

        for dy, dp in groups[i]:
            need(r, group_of(r, (dy, dp, 0, 0)))
        for k, chunk in enumerate(groups[i]):
            blk = blocks[chunk]
            w = jnp.concatenate([dbuf[layer, blk, 0], dbuf[layer, blk, 1]], axis=1)
            pbuf[k] = jnp.dot(hbuf[h * 256 : h * 256 + 256, :], w, preferred_element_type=F32)
        for k, chunk in enumerate(groups[i]):
            j = chunks.index(chunk)
            rs1[layer, h, j, 0, 0:32, :] = pbuf[k, rows(zo, 0), :].astype(BF)
            rs1[layer, h, j, 0, 32:64, :] = pbuf[k, rows(zp, 1), :].astype(BF)
            rs1[layer, h, j, 1, 0:32, :] = pbuf[k, rows(zm, 0), :].astype(BF)
            rs1[layer, h, j, 1, 32:64, :] = pbuf[k, rows(zo, 1), :].astype(BF)
            keep[h, j, 0] = pbuf[k, rows(zp, 0), :]
            keep[h, j, 1] = pbuf[k, rows(zm, 1), :]
            cols = pl.ds(pl.multiple_of(blocks[chunk] * 256, 256), 256)
            br[h * 64 : h * 64 + 64, cols] = pbuf[k, pl.ds(pl.multiple_of(z * 64, 64), 64), :]
        for chunk in groups[i]:
            j = chunks.index(chunk)
            for sign in (1, -1):
                lane = tee(sign)
                send(rs1.at[layer, h, j, lane], rr1.at[layer, h, j, lane], rs_send.at[0], rs1_recv.at[h, j], z_dev[sign])

    def combine(layer, h, chunk):
        j = chunks.index(chunk)
        await_bytes(rr1.at[layer, h, j], rs1_recv.at[h, j])
        for sign in (1, -1):
            lane = tee(sign)
            half = slice(0, 32) if sign > 0 else slice(32, 64)
            rs2[layer, h, j, lane] = (rr1[layer, h, j, lane, half, :].astype(F32) + keep[h, j, lane]).astype(BF)
        for sign in (1, -1):
            lane = tee(sign)
            send(rs2.at[layer, h, j, lane], rr2.at[layer, h, j, lane], rs_send.at[1], rs2_recv.at[h], z_dev[sign])
        cols = pl.ds(pl.multiple_of(blocks[chunk] * 256, 256), 256)
        br[h * 64 : h * 64 + 32, cols] += rr1[layer, h, j, 1, 0:32, :].astype(F32)
        br[h * 64 + 32 : h * 64 + 64, cols] += rr1[layer, h, j, 0, 32:64, :].astype(F32)

    def finish(layer, h):
        await_bytes(rr2.at[layer, h], rs2_recv.at[h])
        for j, chunk in enumerate(chunks):
            cols = pl.ds(pl.multiple_of(blocks[chunk] * 256, 256), 256)
            br[h * 64 : h * 64 + 32, cols] += rr2[layer, h, j, 0].astype(F32)
            br[h * 64 + 32 : h * 64 + 64, cols] += rr2[layer, h, j, 1].astype(F32)
        for i in range(4):
            rows = slice(h * 64 + i * 16, h * 64 + i * 16 + 16)
            branch = br[rows, :]
            if layer == 0:
                m = tokv[rows, :].astype(F32) + 0.5 * rms(branch, gains[1]) + rms(mixv[rows, :].astype(F32), gains[2])
                m = m.astype(BF)
                mixed[rows, :] = m
                x_rows(1, h, z, i)[...] = rms(m.astype(F32), gains[3]).astype(BF)
            else:
                out[rows, :] = (mixed[rows, :].astype(F32) + 0.5 * rms(branch, gains[4])).astype(BF)

    wait_local(0)
    for sign in (1, -1):
        send_y(0, sign, 0)
        send_x(0, sign, 0)
        send_y(0, sign, 1)
        send_x(0, sign, 1)
        send_y(0, sign, 2)
        send_y(0, sign, 3)
    own_partner(0)
    await_bytes(tokv, loc_sem.at[1])
    await_bytes(gains, loc_sem.at[2])
    await_bytes(mixv, loc_sem.at[6])
    tasks = dict(
        y=y_event, x=x_event, en=early_norm, ao=ag_own, af=ag_forward, ae=ag_finish, g1=gemm1, g2=gemm2, gl=gemm1_later,
        he=hidden_early, hl=hidden_later, d=down, c=combine, f=finish,
    )
    for name, *args in ORDER:
        fn = tasks[name]
        fn(*args)

    for r in range(4):
        await_bytes(units(r, 28), w_send.at[r])
        await_bytes(units(r, 32), p_send.at[r])
    for layer in (0, 1):
        await_bytes(xbuf.at[0, pl.ds(0, 384), :], ag_send.at[layer])
    await_bytes(rs1, rs_send.at[0])
    await_bytes(rs2, rs_send.at[1])


def on_device(tokens, mixer_output, en, eg, ev, ed, ep, mg, ln, lg, lv, ld, lp):
    gains = [g.reshape(1, 2048) for g in (en, ep, mg, ln, lp)]
    en, ep, mg, ln, lp = gains
    return pl.pallas_call(
        kernel,
        out_shape=pltpu.VMEM((128, 2048), BF),
        in_specs=[pl.BlockSpec(memory_space=pl.ANY)] * 13,
        out_specs=pl.BlockSpec(memory_space=pltpu.VMEM),
        scratch_shapes=[
            pltpu.VMEM((2, 2048, 1280), BF),
            pltpu.VMEM((2, 2048, 1280), BF),
            pltpu.VMEM((2, 8, 2, 1280, 128), BF),
            pltpu.VMEM((2, 512, 2048), BF),
            pltpu.VMEM((2, 512, 1280), F32),
            pltpu.VMEM((512, 1280), BF),
            pltpu.VMEM((128, 2048), BF),
            pltpu.VMEM((128, 2048), BF),
            pltpu.VMEM((128, 2048), BF),
            pltpu.VMEM((5, 1, 2048), F32),
            pltpu.VMEM((2, 2, 8, 2, 64, 256), BF),
            pltpu.VMEM((2, 2, 8, 2, 64, 256), BF),
            pltpu.VMEM((2, 2, 8, 2, 32, 256), BF),
            pltpu.VMEM((2, 2, 8, 2, 32, 256), BF),
            pltpu.VMEM((2, 8, 2, 32, 256), F32),
            pltpu.VMEM((128, 2048), F32),
            pltpu.VMEM((2, 256, 256), F32),
            pltpu.SemaphoreType.DMA((7,)),
            pltpu.SemaphoreType.DMA((4,)),
            pltpu.SemaphoreType.DMA((4, 11)),
            pltpu.SemaphoreType.DMA((4,)),
            pltpu.SemaphoreType.DMA((22,)),
            pltpu.SemaphoreType.DMA((2,)),
            pltpu.SemaphoreType.DMA((2, 3)),
            pltpu.SemaphoreType.DMA((2,)),
            pltpu.SemaphoreType.DMA((2, 8)),
            pltpu.SemaphoreType.DMA((2,)),
        ],
        compiler_params=pltpu.CompilerParams(
            collective_id=0, has_side_effects=True, vmem_limit_bytes=60_000_000
        ),
    )(tokens, mixer_output, en, eg, ev, ed, ep, mg, ln, lg, lv, ld, lp)


def solution(mesh):
    placed = (
        P(("rep", "fs", "tp"), None),
        P(("rep", "fs", "tp"), None),
        P(),
        P("fs", "tp"),
        P("fs", "tp"),
        P("tp", "fs"),
        P(),
        P(),
        P(),
        P("fs", "tp"),
        P("fs", "tp"),
        P("tp", "fs"),
        P(),
    )
    return jax.shard_map(
        on_device,
        mesh=mesh,
        in_specs=placed,
        out_specs=P(("rep", "fs", "tp"), None),
        check_vma=False,
    )
```

```python
import functools

import jax
import jax.numpy as jnp
from jax import lax
from jax.experimental import pallas as pl
from jax.experimental.pallas import tpu as pltpu
from jax.sharding import PartitionSpec as P

MESH = pl.DeviceIdType.MESH
EPS = 1e-06
BF = jnp.bfloat16
F32 = jnp.float32


ORDER = (
    ("en", 0), ("en", 1), ("ao", 0, 1, 0), ("ao", 0, 0, 0), ("y", 0, 0), ("ao", 0, 1, 1), ("ao", 0, 0, 1),
    ("x", 0, 1), ("ao", 0, 0, 2), ("af", 0, 1, 0), ("af", 0, 0, 0), ("y", 0, 1), ("y", 0, 2), ("ao", 0, 0, 3),
    ("ao", 0, 1, 2), ("af", 0, 0, 1), ("y", 0, 3), ("ao", 0, 1, 3), ("x", 0, 3), ("af", 0, 1, 1), ("y", 0, 4),
    ("y", 0, 5), ("x", 0, 5), ("ae", 0, 0), ("ae", 0, 1), ("g1", 0), ("g1", 1), ("y", 0, 6), ("x", 0, 6),
    ("g2", 1), ("y", 1, 0), ("g2", 0), ("y", 1, 1), ("x", 1, 1), ("he", 0), ("he", 1), ("y", 1, 2), ("d", 0, 0, 1),
    ("d", 0, 1, 1), ("y", 1, 3), ("d", 0, 1, 0), ("x", 1, 3), ("d", 0, 0, 0), ("y", 1, 4), ("d", 0, 0, 2),
    ("y", 1, 5), ("c", 0, 0, (0, 1)), ("d", 0, 1, 2), ("x", 1, 5), ("d", 0, 0, 3), ("d", 0, 1, 3),
    ("c", 0, 0, (0, 0)), ("y", 1, 6), ("x", 1, 6), ("c", 0, 0, (-1, 0)), ("d", 0, 0, 4), ("d", 0, 0, 5),
    ("d", 0, 1, 4), ("c", 0, 0, (1, 0)), ("d", 0, 1, 5), ("y", 2, 0), ("c", 0, 0, (-1, 1)), ("c", 0, 0, (2, 0)),
    ("c", 0, 0, (1, 1)), ("c", 0, 0, (2, 1)), ("c", 0, 1, (0, 0)), ("y", 2, 1), ("c", 0, 1, (2, 0)),
    ("c", 0, 1, (-1, 0)), ("c", 0, 1, (-1, 1)), ("c", 0, 1, (0, 1)), ("c", 0, 1, (1, 0)), ("c", 0, 1, (1, 1)),
    ("c", 0, 1, (2, 1)), ("y", 2, 2), ("f", 0, 0), ("ao", 1, 0, 0), ("ao", 1, 0, 1), ("f", 0, 1), ("ao", 1, 1, 0),
    ("x", 2, 1), ("ao", 1, 0, 2), ("ao", 1, 0, 3), ("y", 2, 3), ("x", 2, 3), ("af", 1, 0, 1), ("y", 2, 4),
    ("af", 1, 0, 0), ("ao", 1, 1, 1), ("af", 1, 1, 0), ("y", 2, 5), ("x", 2, 5), ("ao", 1, 1, 2), ("ae", 1, 0),
    ("y", 2, 6), ("x", 2, 6), ("ao", 1, 1, 3), ("gl", 0, 1), ("af", 1, 1, 1), ("gl", 0, 0), ("y", 3, 0),
    ("x", 3, 1), ("hl", 0), ("y", 3, 1), ("d", 1, 0, 0), ("y", 3, 2), ("d", 1, 0, 1), ("y", 3, 3), ("ae", 1, 1),
    ("gl", 1, 1), ("gl", 1, 0), ("d", 1, 0, 2), ("x", 3, 3), ("c", 1, 0, (0, 1)), ("y", 3, 4), ("c", 1, 0, (0, 0)),
    ("y", 3, 5), ("hl", 1), ("d", 1, 1, 1), ("d", 1, 1, 0), ("d", 1, 1, 3), ("x", 3, 5), ("d", 1, 0, 3),
    ("c", 1, 0, (-1, 0)), ("d", 1, 1, 2), ("y", 3, 6), ("x", 3, 6), ("d", 1, 1, 4), ("d", 1, 0, 5),
    ("c", 1, 0, (1, 0)), ("d", 1, 1, 5), ("c", 1, 1, (0, 1)), ("d", 1, 0, 4), ("c", 1, 1, (1, 0)),
    ("c", 1, 1, (-1, 0)), ("c", 1, 1, (1, 1)), ("c", 1, 0, (2, 1)), ("c", 1, 1, (-1, 1)), ("c", 1, 1, (2, 0)),
    ("c", 1, 1, (2, 1)), ("c", 1, 1, (0, 0)), ("c", 1, 0, (-1, 1)), ("c", 1, 0, (2, 0)), ("c", 1, 0, (1, 1)),
    ("f", 1, 1), ("f", 1, 0),
)
OWN_Y_AT = 4
OWN_X_AT = 4


def kernel(
    tok, mix, en, eg, ev, ed, ep, mg, ln, lg, lv, ld, lp,
    out,
    gbuf, vbuf, dbuf, xbuf, acc, hbuf, tokv, mixv, mixed, gains,
    rs1, rr1, rs2, rr2, keep, br, pbuf,
    loc_sem, w_send, w_recv, p_send, p_recv, ag_send, ag_recv, rs_send, rs1_recv, rs2_recv,
):
    rep = lax.axis_index("rep")
    fs = lax.axis_index("fs")
    z = lax.axis_index("tp")
    c = lax.rem(fs, 2)
    xl = lax.rem(fs // 2, 2)
    y = fs // 4
    x = rep * 2 + xl

    def mod4(v):
        return lax.rem(v + 8, 4)

    def dev(dx=0, dy=0, dz=0, dc=0):
        nx = mod4(x + dx)
        ny = mod4(y + dy)
        nc = c if dc == 0 else 1 - c
        return (nx // 2, (ny * 2 + lax.rem(nx, 2)) * 2 + nc, mod4(z + dz))

    y_dev = {1: dev(dy=1), -1: dev(dy=-1)}
    x_dev = {1: dev(dx=1), -1: dev(dx=-1)}
    z_dev = {1: dev(dz=1), -1: dev(dz=-1)}
    partner = dev(dc=1)
    everyone = [y_dev[1], y_dev[-1], x_dev[1], x_dev[-1], z_dev[1], z_dev[-1], partner]
    zp, zm, zo = mod4(z + 1), mod4(z - 1), mod4(z + 2)

    def blk_of(dy, dp):
        return mod4(y + dy) * 2 + (xl if dp == 0 else 1 - xl)

    blocks = {(dy, dp): blk_of(dy, dp) for dy in (0, 1, -1, 2) for dp in (0, 1)}

    def unit(r, content, core):
        dy, dp, st, s = content
        blk = blocks[(dy, dp)]
        layer = r // 2
        if r % 2 == 0:
            buf = gbuf if st == 0 else vbuf
            row = pl.multiple_of(blk * 256 + core * 128 + s * 64, 64)
            return buf.at[layer, pl.ds(row, 64), :]
        return dbuf.at[layer, blk, core, pl.ds(st * 640 + s * 320, 320), :]

    def unit_id(content):
        dy, dp, st, s = content
        return (((dy % 4) * 2 + dp) * 2 + st) * 2 + s

    def send(src, dst, send_sem, recv_sem, target):
        pltpu.make_async_remote_copy(src, dst, send_sem, recv_sem, device_id=target, device_id_type=MESH).start()

    def await_bytes(ref, sem):
        pltpu.make_async_copy(ref, ref, sem).wait()

    def units(r, n):
        return gbuf.at[0, pl.ds(0, n * (64 if r % 2 == 0 else 32)), :]

    def tee(sign):
        return 0 if sign > 0 else 1

    def y_recv_content(sign, k):
        t = tee(sign)
        return [(-sign, 0, t, 0), (-sign, 0, t, 1), (-sign, 0, 1 - t, 0), (-sign, 0, 1 - t, 1), (2, 0, t, 0),
                (2, 0, t, 1), (2, 1, t, 1)][k]

    def y_send_content(sign, k):
        t = tee(sign)
        return [(0, 0, t, 0), (0, 0, t, 1), (0, 0, 1 - t, 0), (0, 0, 1 - t, 1), (-sign, 0, t, 0),
                (-sign, 0, t, 1), (-sign, 1, t, 1)][k]

    def x_content(sign, k, dp):
        t = tee(sign)
        return [(0, dp, t, 0), (0, dp, t, 1), (-sign, dp, t, 0), (-sign, dp, t, 1), (sign, dp, t, 0),
                (sign, dp, t, 1), (2, dp, t, 0)][k]

    have = set()
    partner_have = set()

    def group_of(r, content):
        dy, dp, st, s = content
        if r % 2 == 0:
            return (0 if r == 0 else 19) + (0 if dy in (0, -1 if st == 0 else 1) else 2 if dy == 2 else 1)
        return 3 + (r // 2) * 8 + (dy % 4) * 2 + dp

    def send_y(r, sign, k):
        content = y_send_content(sign, k)
        assert (r, content) in have
        ref = unit(r, content, c)
        send(ref, ref, w_send.at[r], w_recv.at[r, k], y_dev[sign])

    def send_x(r, sign, k):
        content = x_content(sign, k, 0)
        assert (r, content) in have
        ref = unit(r, content, c)
        send(ref, ref, w_send.at[r], w_recv.at[r, 7 + k // 2], x_dev[sign])

    def send_partner(r, content):
        ref = unit(r, content, c)
        send(ref, ref, p_send.at[r], p_recv.at[group_of(r, content)], partner)

    every = [(dy, dp, st, s) for dy in (0, 1, -1, 2) for dp in (0, 1) for st in (0, 1) for s in (0, 1)]

    def need(r, group):
        members = [content for content in every if group_of(r, content) == group]
        assert all((r, content) in have for content in members), (r, group)
        if group not in partner_have:
            partner_have.add(group)
            await_bytes(units(r, len(members)), p_recv.at[group])

    def own_y(r):
        wait_local(r)
        for sign in (1, -1):
            for k in (0, 1, 2, 3):
                send_y(r, sign, k)

    def own_x(r):
        for sign in (1, -1):
            send_x(r, sign, 0)
            send_x(r, sign, 1)

    def own_partner(r):
        for st in (0, 1):
            for s in (0, 1):
                send_partner(r, (0, 0, st, s))

    def y_event(r, j):
        await_bytes(units(r, 2), w_recv.at[r, j])
        for sign in (1, -1):
            have.add((r, y_recv_content(sign, j)))
        for sign in (1, -1):
            if j in (2, 3):
                send_x(r, -sign, j + 2)
            elif j < 5:
                send_x(r, sign, j + 2)
            if j < 2:
                send_y(r, sign, j + 4)
        if r < 3 and j == OWN_Y_AT:
            own_y(r + 1)
        if r < 3 and j == OWN_X_AT:
            own_x(r + 1)
        for sign in (1, -1):
            send_partner(r, y_recv_content(sign, j))
        if r < 3 and j == OWN_Y_AT:
            own_partner(r + 1)

    def x_event(r, j):
        ks = (6,) if j == 6 else (j - 1, j)
        await_bytes(units(r, 2 * len(ks)), w_recv.at[r, 7 + ks[0] // 2])
        for sign in (1, -1):
            for k in ks:
                have.add((r, x_content(sign, k, 1)))
            if j == 3:
                send_y(r, sign, 6)
        for k in ks:
            for sign in (1, -1):
                send_partner(r, x_content(sign, k, 1))

    own = pl.multiple_of(blocks[(0, 0)] * 256 + c * 128, 128)
    weights = {
        0: [(eg, gbuf.at[0, pl.ds(own, 128), :]), (ev, vbuf.at[0, pl.ds(own, 128), :])],
        1: [(ed, dbuf.at[0, blocks[(0, 0)], c])],
        2: [(lg, gbuf.at[1, pl.ds(own, 128), :]), (lv, vbuf.at[1, pl.ds(own, 128), :])],
        3: [(ld, dbuf.at[1, blocks[(0, 0)], c])],
    }
    norms = [(g, gains.at[i]) for i, g in enumerate((en, ep, mg, ln, lp))]
    for i, pairs in enumerate((weights[0], [(tok, tokv)], norms, weights[1], weights[2], weights[3], [(mix, mixv)])):
        for src, dst in pairs:
            pltpu.make_async_copy(src, dst, loc_sem.at[i]).start()

    def wait_local(r):
        await_bytes(units(r, 4), loc_sem.at[(0, 3, 4, 5)[r]])
        for st in (0, 1):
            for s in (0, 1):
                have.add((r, (0, 0, st, s)))

    barrier = pltpu.get_barrier_semaphore()
    for other in everyone:
        pl.semaphore_signal(barrier, inc=1, device_id=other, device_id_type=MESH)
    pl.semaphore_wait(barrier, len(everyone))

    def x_rows(layer, h, zz, u, n=16):
        row = pl.multiple_of(h * 256 + zz * 64 + u * 16, 16)
        return xbuf.at[layer, pl.ds(row, n), :]

    def ag_own(layer, h, u):
        for sign in (1, -1):
            v = u if sign > 0 else (u + 2) % 4
            ref = x_rows(layer, h, z, v)
            send(ref, ref, ag_send.at[layer], ag_recv.at[h, min(u, 2)], z_dev[sign])

    def ag_forward(layer, h, u):
        await_bytes(xbuf.at[0, pl.ds(0, 32), :], ag_recv.at[h, u])
        for sign in (1, -1):
            v = u if sign > 0 else u + 2
            ref = x_rows(layer, h, zm if sign > 0 else zp, v)
            send(ref, ref, ag_send.at[layer], ag_recv.at[h, 2], z_dev[sign])

    def ag_finish(layer, h):
        await_bytes(xbuf.at[0, pl.ds(0, 128), :], ag_recv.at[h, 2])

    def rms(v, gain):
        return v * lax.rsqrt(jnp.mean(v * v, axis=-1, keepdims=True) + EPS) * gain

    def early_norm(h):
        for i in range(4):
            v = rms(tokv[h * 64 + i * 16 : h * 64 + i * 16 + 16, :].astype(F32), gains[0])
            x_rows(0, h, z, i)[...] = v.astype(BF)

    def dot_rows(st, rows, dy, cols, layer=0):
        base = pl.multiple_of(mod4(y + dy) * 512, 512)
        w = gbuf if st == 0 else vbuf
        return jnp.dot(xbuf[layer, rows, pl.ds(base, 512)], w[layer, pl.ds(base, 512), cols], preferred_element_type=F32)

    whole = slice(0, 512)

    def tile(n):
        return slice(n * 256, n * 256 + 256)

    def gemm1(st):
        need(0, 0)
        for n in range(5):
            acc[st, :, tile(n)] = dot_rows(st, whole, 0, tile(n)) + dot_rows(st, whole, -1 if st == 0 else 1, tile(n))

    def silu_mul(g, v):
        return (g * (1.0 / (1.0 + jnp.exp(-g))) * v).astype(BF)

    def gemm2(st):
        need(0, 1)
        for n in range(5):
            acc[st, :, tile(n)] += dot_rows(st, whole, 1 if st == 0 else -1, tile(n))

    def gemm1_later(h, part):
        need(2, 19)
        need(2, 20)
        rows = slice(h * 256, h * 256 + 256)
        for n in ((0, 1, 2), (3, 4))[part]:
            for st in (0, 1):
                parts = [dot_rows(st, rows, dy, tile(n), 1) for dy in (0, -1, 1)]
                acc[st, rows, tile(n)] = parts[0] + parts[1] + parts[2]

    def hidden(layer, h):
        need(2 * layer, 19 * layer + 2)
        rows = slice(h * 256, h * 256 + 256)
        for n in range(5):
            g = acc[0, rows, tile(n)] + dot_rows(0, rows, 2, tile(n), layer)
            v = acc[1, rows, tile(n)] + dot_rows(1, rows, 2, tile(n), layer)
            hbuf[rows, tile(n)] = silu_mul(g, v)

    def hidden_early(h):
        hidden(0, h)

    def hidden_later(h):
        hidden(1, h)

    chunks = ((0, 0), (0, 1), (-1, 0), (1, 0), (2, 0), (-1, 1), (1, 1), (2, 1))

    groups = (((0, 0),), ((0, 1),), ((-1, 0), (1, 0)), ((2, 0),), ((-1, 1), (1, 1)), ((2, 1),))

    def down(layer, h, i):
        r = 2 * layer + 1

        def rows(zz, half):
            return pl.ds(pl.multiple_of(zz * 64 + half * 32, 32), 32)

        for dy, dp in groups[i]:
            need(r, group_of(r, (dy, dp, 0, 0)))
        for k, chunk in enumerate(groups[i]):
            blk = blocks[chunk]
            w = jnp.concatenate([dbuf[layer, blk, 0], dbuf[layer, blk, 1]], axis=1)
            pbuf[k] = jnp.dot(hbuf[h * 256 : h * 256 + 256, :], w, preferred_element_type=F32)
        for k, chunk in enumerate(groups[i]):
            j = chunks.index(chunk)
            rs1[layer, h, j, 0, 0:32, :] = pbuf[k, rows(zo, 0), :].astype(BF)
            rs1[layer, h, j, 0, 32:64, :] = pbuf[k, rows(zp, 1), :].astype(BF)
            rs1[layer, h, j, 1, 0:32, :] = pbuf[k, rows(zm, 0), :].astype(BF)
            rs1[layer, h, j, 1, 32:64, :] = pbuf[k, rows(zo, 1), :].astype(BF)
            keep[h, j, 0] = pbuf[k, rows(zp, 0), :]
            keep[h, j, 1] = pbuf[k, rows(zm, 1), :]
            cols = pl.ds(pl.multiple_of(blocks[chunk] * 256, 256), 256)
            br[h * 64 : h * 64 + 64, cols] = pbuf[k, pl.ds(pl.multiple_of(z * 64, 64), 64), :]
        for chunk in groups[i]:
            j = chunks.index(chunk)
            for sign in (1, -1):
                lane = tee(sign)
                send(rs1.at[layer, h, j, lane], rr1.at[layer, h, j, lane], rs_send.at[0], rs1_recv.at[h, j], z_dev[sign])

    def combine(layer, h, chunk):
        j = chunks.index(chunk)
        await_bytes(rr1.at[layer, h, j], rs1_recv.at[h, j])
        for sign in (1, -1):
            lane = tee(sign)
            half = slice(0, 32) if sign > 0 else slice(32, 64)
            rs2[layer, h, j, lane] = (rr1[layer, h, j, lane, half, :].astype(F32) + keep[h, j, lane]).astype(BF)
        for sign in (1, -1):
            lane = tee(sign)
            send(rs2.at[layer, h, j, lane], rr2.at[layer, h, j, lane], rs_send.at[1], rs2_recv.at[h], z_dev[sign])
        cols = pl.ds(pl.multiple_of(blocks[chunk] * 256, 256), 256)
        br[h * 64 : h * 64 + 32, cols] += rr1[layer, h, j, 1, 0:32, :].astype(F32)
        br[h * 64 + 32 : h * 64 + 64, cols] += rr1[layer, h, j, 0, 32:64, :].astype(F32)

    def finish(layer, h):
        await_bytes(rr2.at[layer, h], rs2_recv.at[h])
        for j, chunk in enumerate(chunks):
            cols = pl.ds(pl.multiple_of(blocks[chunk] * 256, 256), 256)
            br[h * 64 : h * 64 + 32, cols] += rr2[layer, h, j, 0].astype(F32)
            br[h * 64 + 32 : h * 64 + 64, cols] += rr2[layer, h, j, 1].astype(F32)
        for i in range(4):
            rows = slice(h * 64 + i * 16, h * 64 + i * 16 + 16)
            branch = br[rows, :]
            if layer == 0:
                m = tokv[rows, :].astype(F32) + 0.5 * rms(branch, gains[1]) + rms(mixv[rows, :].astype(F32), gains[2])
                m = m.astype(BF)
                mixed[rows, :] = m
                x_rows(1, h, z, i)[...] = rms(m.astype(F32), gains[3]).astype(BF)
            else:
                out[rows, :] = (mixed[rows, :].astype(F32) + 0.5 * rms(branch, gains[4])).astype(BF)

    wait_local(0)
    for sign in (1, -1):
        send_y(0, sign, 0)
        send_x(0, sign, 0)
        send_y(0, sign, 1)
        send_x(0, sign, 1)
        send_y(0, sign, 2)
        send_y(0, sign, 3)
    own_partner(0)
    await_bytes(tokv, loc_sem.at[1])
    await_bytes(gains, loc_sem.at[2])
    await_bytes(mixv, loc_sem.at[6])
    tasks = dict(
        y=y_event, x=x_event, en=early_norm, ao=ag_own, af=ag_forward, ae=ag_finish, g1=gemm1, g2=gemm2, gl=gemm1_later,
        he=hidden_early, hl=hidden_later, d=down, c=combine, f=finish,
    )
    for name, *args in ORDER:
        fn = tasks[name]
        fn(*args)

    for r in range(4):
        await_bytes(units(r, 28), w_send.at[r])
        await_bytes(units(r, 32), p_send.at[r])
    for layer in (0, 1):
        await_bytes(xbuf.at[0, pl.ds(0, 384), :], ag_send.at[layer])
    await_bytes(rs1, rs_send.at[0])
    await_bytes(rs2, rs_send.at[1])


def on_device(tokens, mixer_output, en, eg, ev, ed, ep, mg, ln, lg, lv, ld, lp):
    gains = [g.reshape(1, 2048) for g in (en, ep, mg, ln, lp)]
    en, ep, mg, ln, lp = gains
    return pl.pallas_call(
        kernel,
        out_shape=pltpu.VMEM((128, 2048), BF),
        in_specs=[pl.BlockSpec(memory_space=pl.ANY)] * 13,
        out_specs=pl.BlockSpec(memory_space=pltpu.VMEM),
        scratch_shapes=[
            pltpu.VMEM((2, 2048, 1280), BF),
            pltpu.VMEM((2, 2048, 1280), BF),
            pltpu.VMEM((2, 8, 2, 1280, 128), BF),
            pltpu.VMEM((2, 512, 2048), BF),
            pltpu.VMEM((2, 512, 1280), F32),
            pltpu.VMEM((512, 1280), BF),
            pltpu.VMEM((128, 2048), BF),
            pltpu.VMEM((128, 2048), BF),
            pltpu.VMEM((128, 2048), BF),
            pltpu.VMEM((5, 1, 2048), F32),
            pltpu.VMEM((2, 2, 8, 2, 64, 256), BF),
            pltpu.VMEM((2, 2, 8, 2, 64, 256), BF),
            pltpu.VMEM((2, 2, 8, 2, 32, 256), BF),
            pltpu.VMEM((2, 2, 8, 2, 32, 256), BF),
            pltpu.VMEM((2, 8, 2, 32, 256), F32),
            pltpu.VMEM((128, 2048), F32),
            pltpu.VMEM((2, 256, 256), F32),
            pltpu.SemaphoreType.DMA((7,)),
            pltpu.SemaphoreType.DMA((4,)),
            pltpu.SemaphoreType.DMA((4, 11)),
            pltpu.SemaphoreType.DMA((4,)),
            pltpu.SemaphoreType.DMA((22,)),
            pltpu.SemaphoreType.DMA((2,)),
            pltpu.SemaphoreType.DMA((2, 3)),
            pltpu.SemaphoreType.DMA((2,)),
            pltpu.SemaphoreType.DMA((2, 8)),
            pltpu.SemaphoreType.DMA((2,)),
        ],
        compiler_params=pltpu.CompilerParams(
            collective_id=0, has_side_effects=True, vmem_limit_bytes=60_000_000
        ),
    )(tokens, mixer_output, en, eg, ev, ed, ep, mg, ln, lg, lv, ld, lp)


def solution(mesh):
    placed = (
        P(("rep", "fs", "tp"), None),
        P(("rep", "fs", "tp"), None),
        P(),
        P("fs", "tp"),
        P("fs", "tp"),
        P("tp", "fs"),
        P(),
        P(),
        P(),
        P("fs", "tp"),
        P("fs", "tp"),
        P("tp", "fs"),
        P(),
    )
    return jax.shard_map(
        on_device,
        mesh=mesh,
        in_specs=placed,
        out_specs=P(("rep", "fs", "tp"), None),
        check_vma=False,
    )
```
